128 devices in a mesh: sp: 32 (over z, y, core), tp: 4 (over x).
Axes of the slice: x: 4, y: 4, z: 4, core: 2. Of those that a mesh axis runs over, the one named last changes fastest.
Arguments:
- tokens: bfloat16 [8192, 4096], P('sp', 'tp'), may hold values from -6 to 6
- input_norm_gain: float32 [4096], replicated, may hold values from 0.1 to 1.9
- query_weight: bfloat16 [4096, 2048], P('sp', 'tp'), may hold values from -0.09375 to 0.09375
- key_weight: bfloat16 [4096, 2048], P('sp', 'tp'), may hold values from -0.09375 to 0.09375
- value_weight: bfloat16 [4096, 2048], P('sp', 'tp'), may hold values from -0.09375 to 0.09375
- decay_first_map: bfloat16 [4096, 128], replicated, may hold values from -0.09375 to 0.09375
- decay_second_map: bfloat16 [128, 2048], P(None, 'tp'), may hold values from -0.5 to 0.5
- channel_decay_offset: float32 [2048], P('tp'), may hold values from -13 to -2
- position_decay_offset: float32 [8192], P('sp'), may hold values from -2 to 2
- extra_log_decay: float32 [8192, 32], P('sp', 'tp'), may hold values from -0.7 to 0
- rate_first_map: bfloat16 [4096, 128], replicated, may hold values from -0.09375 to 0.09375
- rate_second_map: bfloat16 [128, 2048], P(None, 'tp'), may hold values from -0.25 to 0.25
- channel_rate_offset: float32 [2048], P('tp'), may hold values from -10 to 1
- own_term_weight: float32 [2048], P('tp'), may hold values from -2 to 2
- head_norm_gain: float32 [2048], P('tp'), may hold values from 0.1 to 1.9
- starting_state: float32 [32, 64, 64], P('tp'), may hold values from -384 to 384
- outer_gate_weight: bfloat16 [4096, 2048], P('sp', 'tp'), may hold values from -0.09375 to 0.09375
- inner_gate_weight: bfloat16 [4096, 2048], P('sp', 'tp'), may hold values from -0.09375 to 0.09375
- signal_weight: bfloat16 [4096, 2048], P('sp', 'tp'), may hold values from -0.09375 to 0.09375
- convolution_taps: bfloat16 [3, 2048], P(None, 'tp'), may hold values from -3.5 to 3.5
- convolution_gain: float32 [2048], P('tp'), may hold values from 0.1 to 1.9
Outputs:
- linear_attention_output: bfloat16 [8192, 2048], P('sp', 'tp')
- out_conv: bfloat16 [8192, 2048], P('sp', 'tp')
The draws below stay inside these ranges and needn't reach their ends.
All inputs are finite; a program needn't handle non-finite values.
Results may differ from the reference program's by a relative error of at most 0.009.
Values may be sent and summed in bfloat16 or wider, within the bound.
A program may use at most 128 MiB of HBM per device.

```python
import math
import jax
import jax.numpy as jnp
from jax import lax

D = 4096
HEAD_COUNT = 32
HEAD_SIZE = 64
RANK = 128
TAPS = 3
BLOCK = 64
TOK_DEV = 256
MIXER_WIDTH = 2048
TOKEN_COUNT = 8192


def pick_slow(key):
    ranking = jax.random.permutation(jax.random.fold_in(key, 7), HEAD_COUNT)
    slow_count = HEAD_COUNT // 2
    return jnp.repeat(ranking < slow_count, HEAD_SIZE)


def draw_channel_decay_offset(key, part):
    slow_mask = pick_slow(key)
    jitter = jax.random.uniform(jax.random.fold_in(key, 21), (HEAD_COUNT * HEAD_SIZE,), jnp.float32, -0.5, 0.5)
    fast_values = jax.random.uniform(jax.random.fold_in(key, 22), (HEAD_COUNT * HEAD_SIZE,), jnp.float32, -3.5, -2.5)
    return jnp.where(slow_mask, -math.log(TOKEN_COUNT) - 1.0 + jitter, fast_values)


def draw_channel_rate_offset(key, part):
    slow_mask = pick_slow(key)
    jitter = jax.random.uniform(jax.random.fold_in(key, 23), (HEAD_COUNT * HEAD_SIZE,), jnp.float32, -0.5, 0.5)
    fast_values = jax.random.uniform(jax.random.fold_in(key, 24), (HEAD_COUNT * HEAD_SIZE,), jnp.float32, -1.0, 1.0)
    return jnp.where(slow_mask, math.log(8.0 / TOKEN_COUNT) + jitter, fast_values)


def draw_position_decay_offset(key, part):
    positions = jnp.arange(TOKEN_COUNT)
    per_block = jax.random.uniform(jax.random.fold_in(key, 31), (TOKEN_COUNT // BLOCK,), jnp.float32, -1.0, 1.0)
    per_device = jax.random.uniform(jax.random.fold_in(key, 32), (TOKEN_COUNT // TOK_DEV,), jnp.float32, -0.7, 0.7)
    return per_block[positions // BLOCK] + per_device[positions // TOK_DEV]


def draw_extra_log_decay(key, part):
    spots = jax.random.permutation(jax.random.fold_in(key, 41), TOKEN_COUNT)[:3]
    losses = jnp.log(jax.random.uniform(jax.random.fold_in(key, 42), (3, HEAD_COUNT), jnp.float32, 0.5, 0.8))
    markers = (jnp.arange(TOKEN_COUNT)[:, None] == spots[None, :]).astype(jnp.float32)
    return jnp.dot(markers, losses)


def draw_starting_state(key, part):
    spread = math.sqrt(TOKEN_COUNT)
    values = jnp.clip(jax.random.normal(jax.random.fold_in(key, 52), (HEAD_COUNT, HEAD_SIZE, HEAD_SIZE), jnp.float32), -6.0, 6.0) * 0.7
    return values * spread


def block_scale(own_key, extent, shards, least, high):
    factor_of, own = 1.0, jax.random.fold_in(own_key, 6)
    for position, shards_of in shards:
        draws = jnp.exp(jax.random.uniform(jax.random.fold_in(own, position), (shards_of,), jnp.float32, least / len(shards), high / len(shards)))
        factor_of = factor_of * jnp.repeat(draws, extent[position] // shards_of).reshape([-1 if axis == position else 1 for axis in range(len(extent))])
    return factor_of


def normal_values(rng, dims, width, most, cuts=(), held_as=jnp.bfloat16):
    result = jax.random.normal(rng, dims, jnp.float32) * width
    if len(cuts) > 0:
        result = block_scale(rng, dims, cuts, -0.22, 0.18) * result
    return jnp.clip(result, min=-most, max=most).astype(held_as)


def setup_inputs(seed: int = 0) -> dict:
    key_list = jax.random.split(jax.random.key(seed), 22)
    tokens = normal_values(key_list[0], (TOKEN_COUNT, D), 1.0, 6.0, ((0, 32), (1, 4)))
    input_norm_gain = jnp.clip(1.0 + 0.18 * jax.random.normal(key_list[1], (D,), jnp.float32), 0.1, 1.9)
    query_weight = normal_values(key_list[2], (D, MIXER_WIDTH), D ** -0.5, 0.09375, ((0, 32), (1, 4)))
    key_weight = normal_values(key_list[3], (D, MIXER_WIDTH), D ** -0.5, 0.09375, ((0, 32), (1, 4)))
    value_weight = normal_values(key_list[4], (D, MIXER_WIDTH), D ** -0.5, 0.09375, ((0, 32), (1, 4)))
    decay_first_map = normal_values(key_list[5], (D, RANK), D ** -0.5, 0.09375)
    decay_second_map = normal_values(key_list[6], (RANK, MIXER_WIDTH), RANK ** -0.5, 0.5, ((1, 4),))
    channel_decay_offset = draw_channel_decay_offset(jax.random.fold_in(key_list[21], 71), 0)
    position_decay_offset = draw_position_decay_offset(jax.random.fold_in(key_list[21], 71), 0)
    extra_log_decay = draw_extra_log_decay(jax.random.fold_in(key_list[21], 71), 0)
    rate_first_map = normal_values(key_list[10], (D, RANK), D ** -0.5, 0.09375)
    rate_second_map = normal_values(key_list[11], (RANK, MIXER_WIDTH), (4 * RANK) ** -0.5, 0.25, ((1, 4),))
    channel_rate_offset = draw_channel_rate_offset(jax.random.fold_in(key_list[21], 71), 0)
    own_term_weight = normal_values(key_list[13], (MIXER_WIDTH,), 0.125, 2.0, ((0, 4),), jnp.float32)
    head_norm_gain = jnp.clip(1.0 + 0.18 * jax.random.normal(key_list[14], (MIXER_WIDTH,), jnp.float32), 0.1, 1.9)
    starting_state = draw_starting_state(jax.random.fold_in(key_list[21], 71), 0)
    outer_gate_weight = normal_values(key_list[16], (D, MIXER_WIDTH), D ** -0.5, 0.09375, ((0, 32), (1, 4)))
    inner_gate_weight = normal_values(key_list[17], (D, MIXER_WIDTH), D ** -0.5, 0.09375, ((0, 32), (1, 4)))
    signal_weight = normal_values(key_list[18], (D, MIXER_WIDTH), D ** -0.5, 0.09375, ((0, 32), (1, 4)))
    convolution_taps = normal_values(key_list[19], (TAPS, MIXER_WIDTH), TAPS ** -0.5, 3.5, ((1, 4),))
    convolution_gain = jnp.clip(1.0 + 0.18 * jax.random.normal(key_list[20], (MIXER_WIDTH,), jnp.float32), 0.1, 1.9)
    return {"tokens": tokens, "input_norm_gain": input_norm_gain, "query_weight": query_weight, "key_weight": key_weight, "value_weight": value_weight, "decay_first_map": decay_first_map, "decay_second_map": decay_second_map, "channel_decay_offset": channel_decay_offset, "position_decay_offset": position_decay_offset, "extra_log_decay": extra_log_decay, "rate_first_map": rate_first_map, "rate_second_map": rate_second_map, "channel_rate_offset": channel_rate_offset, "own_term_weight": own_term_weight, "head_norm_gain": head_norm_gain, "starting_state": starting_state, "outer_gate_weight": outer_gate_weight, "inner_gate_weight": inner_gate_weight, "signal_weight": signal_weight, "convolution_taps": convolution_taps, "convolution_gain": convolution_gain}


DECAY_FACTOR = 0.606531
NORM_EPS = 1e-06
GROUP_EPS = 0.00064
KEY_EPS = 1e-06

def rounded(values):
    return lax.optimization_barrier(values.astype(jnp.bfloat16)).astype(jnp.float32)

def project(normed, weight):
    return rounded(jnp.dot(normed, weight, preferred_element_type=jnp.float32))

def recurrence(state, inputs):
    query, decay, keyed, valued, unit_key, rate = inputs
    removal = jnp.einsum('hvk,hk->hv', state, -unit_key, precision=lax.Precision.HIGHEST)
    state = state * decay[:, None, :] + removal[:, :, None] * (unit_key * rate)[:, None, :] + valued[:, :, None] * keyed[:, None, :]
    recalled = jnp.einsum('hvk,hk->hv', state, query, precision=lax.Precision.HIGHEST)
    return (state, recalled)

def reference(tokens, input_norm_gain, query_weight, key_weight, value_weight, decay_first_map, decay_second_map, channel_decay_offset, position_decay_offset, extra_log_decay, rate_first_map, rate_second_map, channel_rate_offset, own_term_weight, head_norm_gain, starting_state, outer_gate_weight, inner_gate_weight, signal_weight, convolution_taps, convolution_gain):
    wide = tokens.astype(jnp.float32)
    normed = (wide * lax.rsqrt(lax.optimization_barrier(jnp.mean(wide * wide, axis=1, keepdims=True)) + NORM_EPS) * input_norm_gain.astype(jnp.float32)).astype(jnp.bfloat16)
    query = project(normed, query_weight)
    keyed = project(normed, key_weight)
    valued = project(normed, value_weight)
    decay_low = jnp.tanh(jnp.dot(normed, decay_first_map, preferred_element_type=jnp.float32)).astype(jnp.bfloat16)
    decay_logits = channel_decay_offset + jnp.dot(decay_low, decay_second_map, preferred_element_type=jnp.float32) + position_decay_offset[:, None]
    decay_logarithm = -DECAY_FACTOR * jax.nn.sigmoid(decay_logits) + jnp.repeat(extra_log_decay, HEAD_SIZE, axis=1)
    rate_low = jnp.dot(normed, rate_first_map, preferred_element_type=jnp.float32).astype(jnp.bfloat16)
    rate = jax.nn.sigmoid(channel_rate_offset + jnp.dot(rate_low, rate_second_map, preferred_element_type=jnp.float32))
    head_shape = (TOKEN_COUNT, HEAD_COUNT, HEAD_SIZE)
    query_per_head = query.reshape(head_shape)
    key_per_head = keyed.reshape(head_shape)
    value_per_head = valued.reshape(head_shape)
    unit_key = key_per_head * lax.rsqrt(lax.optimization_barrier(jnp.sum(key_per_head * key_per_head, axis=2, keepdims=True)) + KEY_EPS)
    inputs = (query_per_head, jnp.exp(decay_logarithm).reshape(head_shape), key_per_head, value_per_head, unit_key, rate.reshape(head_shape))
    final_state, recalled = lax.scan(recurrence, starting_state, inputs)
    center = recalled - lax.optimization_barrier(jnp.mean(recalled, axis=2, keepdims=True))
    variance = lax.optimization_barrier(jnp.mean(center * center, axis=2, keepdims=True))
    input_normed = center * lax.rsqrt(variance + GROUP_EPS) * head_norm_gain.reshape(HEAD_COUNT, HEAD_SIZE)
    own_term = lax.optimization_barrier(jnp.sum(query_per_head * key_per_head * own_term_weight.reshape(HEAD_COUNT, HEAD_SIZE), axis=2, keepdims=True)) * value_per_head
    linear_attention_output = (input_normed + own_term).reshape(TOKEN_COUNT, MIXER_WIDTH).astype(jnp.bfloat16)
    outer = project(normed, outer_gate_weight)
    inner = project(normed, inner_gate_weight)
    signal = project(normed, signal_weight)
    mixed_in = rounded(inner * signal)
    padded = jnp.concatenate([jnp.zeros((2, MIXER_WIDTH), jnp.float32), mixed_in], axis=0)
    taps = convolution_taps.astype(jnp.float32)
    gated = outer * (taps[0] * padded[:-2] + taps[1] * padded[1:-1] + taps[2] * padded[2:])
    out_conv = (gated * lax.rsqrt(lax.optimization_barrier(jnp.mean(gated * gated, axis=1, keepdims=True)) + NORM_EPS) * convolution_gain).astype(jnp.bfloat16)
    return (linear_attention_output, out_conv)
```

```python
import jax
import jax.numpy as jnp
from jax import lax
from jax.experimental import pallas as pl
from jax.experimental.pallas import tpu as pltpu
from jax.sharding import Mesh
from jax.sharding import PartitionSpec as P

SP = ("sp_0", "sp_1", "sp_2")
MESH_IDS = pl.DeviceIdType.MESH
F32 = jnp.float32
BF16 = jnp.bfloat16

DECAY_FACTOR = 0.606531
NORM_EPS = 1e-06
GROUP_EPS = 0.00064
KEY_EPS = 1e-06

TOK = 256
HALO = 16
FEATS = 4096
BLK = 64
PAIRS = 4
OFFSETS = (0, -1, 1, 2)


def dot_nn(a, b):
    return lax.dot_general(a, b, (((1,), (0,)), ((), ())), preferred_element_type=F32)


def dot_nt(a, b):
    return lax.dot_general(a, b, (((1,), (1,)), ((), ())), preferred_element_type=F32)


def parts(a):
    high = a.astype(BF16)
    return high, (a - high.astype(F32)).astype(BF16)


def fine(dot, a, b):
    ah, al = parts(a)
    bh, bl = parts(b)
    return dot(ah, bh) + (dot(al, bh) + dot(ah, bl))


def exact_left(a, b):
    high, rest = parts(b)
    mid = (b - high.astype(F32) - rest.astype(F32)).astype(BF16)
    return dot_nn(a, high) + (dot_nn(a, rest) + dot_nn(a, mid))


def iota(shape, dim):
    return lax.broadcasted_iota(jnp.int32, shape, dim)


def same_head():
    return (iota((128, 128), 0) // 64) == (iota((128, 128), 1) // 64)


def diagonal_blocks(compact):
    return jnp.where(same_head(), jnp.concatenate([compact, compact], axis=0), 0.0)


def head_sums(values):
    ones = same_head().astype(F32).astype(BF16)
    high, rest = parts(values)
    return dot_nn(high, ones) + dot_nn(rest, ones)


def pair_local(q, k, v, decay, rate, cum):
    head = iota((TOK, 128), 1) // 64
    chunk_row = iota((TOK, 128), 0) // BLK
    row, col = iota((TOK, TOK), 0), iota((TOK, TOK), 1)
    within = (row // BLK) == (col // BLK)
    strict = within & (row > col)
    inclusive = within & (row >= col)
    unit = k * lax.rsqrt(head_sums(k * k) + KEY_EPS)
    grow = jnp.exp(-cum)
    a = -unit * jnp.exp(cum - decay)
    b = unit * rate
    r = q * jnp.exp(cum)
    a16, r16, v16 = a.astype(BF16), r.astype(BF16), v.astype(BF16)
    right = jnp.concatenate([(b * grow).astype(BF16), (k * grow).astype(BF16)], axis=0)
    zero = jnp.zeros((TOK, 128), BF16)
    probe = r
    free = jnp.zeros((TOK, 128), F32)
    solved = jnp.zeros((TOK, 256), F32)
    for h in range(2):
        mine = head == h
        a_h, r_h, v_h = (jnp.where(mine, t, zero) for t in (a16, r16, v16))
        top = dot_nt(a_h, right)
        power = jnp.where(strict, top[:, :TOK], 0.0).astype(BF16)
        writes = jnp.where(strict, top[:, TOK:], 0.0).astype(BF16)
        bottom = dot_nt(r_h, right)
        reads = jnp.where(inclusive, bottom[:, :TOK], 0.0).astype(BF16)
        key_reads = jnp.where(inclusive, bottom[:, TOK:], 0.0).astype(BF16)
        y = jnp.concatenate([jnp.where(mine, a, 0.0), dot_nn(writes, v_h)], axis=1)
        for level in range(6):
            y = y + dot_nn(power, y.astype(BF16))
            if level < 5:
                power = dot_nn(power, power).astype(BF16)
        read = dot_nn(reads, y.astype(BF16))
        probe = probe + read[:, :128]
        free = free + read[:, 128:] + dot_nn(key_reads, v_h)
        solved = solved + y
    lasts = [cum[BLK * (c + 1) - 1 : BLK * (c + 1), :] for c in range(TOK // BLK)]
    last = jnp.concatenate([jnp.broadcast_to(t, (BLK, 128)) for t in lasts], axis=0)
    fade = jnp.exp(last - cum)
    b_end, k_end = b * fade, k * fade
    in_chunk = [chunk_row == c for c in range(TOK // BLK)]
    b_wide = jnp.concatenate([jnp.where(m, b_end, 0.0) for m in in_chunk], axis=1)
    k_wide = jnp.concatenate([jnp.where(m, k_end, 0.0) for m in in_chunk], axis=1)
    maps = fine(dot_nn, solved.T, b_wide)
    gains = maps[128:] + fine(dot_nn, v.T, k_wide)
    eye = iota((128, 128), 0) == iota((128, 128), 1)
    state = chain = None
    recalled, probes = [], []
    for c in range(TOK // BLK):
        rows = slice(BLK * c, BLK * (c + 1))
        lanes = slice(128 * c, 128 * (c + 1))
        if c == 0:
            recalled.append(free[rows])
            probes.append(probe[rows])
        else:
            both = fine(dot_nt, probe[rows], jnp.concatenate([state, chain], axis=0))
            recalled.append(free[rows] + both[:, :128])
            probes.append(both[:, 128:])
        step = jnp.where(same_head(), maps[:128, lanes], 0.0)
        step = step + jnp.where(eye, jnp.broadcast_to(jnp.exp(lasts[c]), (128, 128)), 0.0)
        gain = jnp.where(same_head(), gains[:, lanes], 0.0)
        if c == 0:
            state, chain = gain, step
        else:
            both = fine(dot_nn, jnp.concatenate([state, chain], axis=0), step)
            state, chain = both[:128] + gain, both[128:]
    return (
        jnp.concatenate(recalled, axis=0),
        jnp.concatenate(probes, axis=0),
        state[:64] + state[64:],
        chain[:64] + chain[64:],
    )


def compose(earlier, later):
    both = fine(dot_nn, jnp.concatenate(earlier, axis=0), diagonal_blocks(later[0]))
    return both[:64], both[64:] + later[1]


def advance(state, later):
    return fine(dot_nn, state, diagonal_blocks(later[0])) + later[1]


def kernel(
    tokens,
    gain,
    wq,
    wk,
    wv,
    decay_first,
    decay_second,
    channel_decay,
    position_decay,
    extra_decay,
    rate_first,
    rate_second,
    channel_rate,
    own_weight,
    norm_gain,
    start_state,
    wo,
    wi,
    wsig,
    taps,
    conv_gain,
    lin_out,
    conv_out,
    gat_q,
    gat_c,
    raw,
    xn,
    low_d,
    low_r,
    acc,
    q_s,
    k_s,
    v_s,
    decay_s,
    rate_s,
    cum_s,
    rec_s,
    probe_s,
    st1,
    st2,
    st3,
    ent,
    sq_s,
    load_sem,
    tok_send,
    tok_recv,
    ici_send,
    ici_recv,
    d2d_send,
    d2d_recv,
    misc_send,
    misc_recv,
):
    z, y, c = (lax.axis_index(n) for n in SP)
    x = lax.axis_index("tp")

    def up(pos, offset):
        return lax.rem(pos + (offset + 4), 4)

    def at_x(o):
        return {"tp": up(x, o)}

    def at_y(o):
        return {"sp_1": up(y, o)}

    def at_z(o):
        return {"sp_0": up(z, o)}

    sibling = {"sp_2": 1 - c}
    rank = z * 8 + y * 2 + c
    after, before = lax.rem(rank + 1, 32), lax.rem(rank + 31, 32)

    def at_rank(r):
        return {"sp_0": r // 8, "sp_1": lax.rem(r // 2, 4), "sp_2": lax.rem(r, 2)}

    def push(src, dst, send, recv, device):
        copy = pltpu.make_async_remote_copy(
            src_ref=src,
            dst_ref=dst,
            send_sem=send,
            recv_sem=recv,
            device_id=device,
            device_id_type=MESH_IDS,
        )
        copy.start()
        return copy

    def arrived(region, recv):
        pltpu.make_async_copy(region, region, recv).wait()

    loads = [pltpu.make_async_copy(tokens, raw.at[x], load_sem.at[0])]
    for i, w in enumerate((wq, wk, wv)):
        loads.append(
            pltpu.make_async_copy(w, gat_q.at[rank, :, pl.ds(512 * i, 512)], load_sem.at[1 + i])
        )
    for i, w in enumerate((wo, wi, wsig)):
        loads.append(
            pltpu.make_async_copy(w, gat_c.at[rank, :, pl.ds(512 * i, 512)], load_sem.at[4 + i])
        )
    loads.append(pltpu.make_async_copy(decay_first, low_d, load_sem.at[7]))
    loads.append(pltpu.make_async_copy(rate_first, low_r, load_sem.at[8]))
    for load in loads:
        load.start()

    barrier = pltpu.get_barrier_semaphore()
    partners = [at_x(o) for o in OFFSETS[1:]] + [at_y(o) for o in OFFSETS[1:]]
    partners += [at_z(o) for o in OFFSETS[1:]] + [sibling, at_rank(after), at_rank(before)]
    for partner in partners:
        pl.semaphore_signal(barrier, inc=1, device_id=partner, device_id_type=MESH_IDS)
    pl.semaphore_wait(barrier, len(partners))

    loads[0].wait()
    tok_copies = [
        push(raw.at[x], raw.at[x], tok_send.at[0], tok_recv.at[0], at_x(1)),
        push(raw.at[x], raw.at[x], tok_send.at[1], tok_recv.at[1], at_x(-1)),
    ]

    def token_forward():
        left, right = up(x, -1), up(x, 1)
        arrived(raw.at[left], tok_recv.at[0])
        part = raw.at[left, pl.ds(0, 128)]
        tok_copies.append(push(part, part, tok_send.at[2], tok_recv.at[2], at_x(1)))
        arrived(raw.at[right], tok_recv.at[1])
        part = raw.at[right, pl.ds(128, 128)]
        tok_copies.append(push(part, part, tok_send.at[3], tok_recv.at[3], at_x(-1)))

    def token_rest():
        far = up(x, 2)
        arrived(raw.at[far, pl.ds(0, 128)], tok_recv.at[2])
        arrived(raw.at[far, pl.ds(128, 128)], tok_recv.at[3])

    class Gather:
        def __init__(self, which, buf):
            self.g, self.buf = which, buf

        def block(self, half, a, b, core):
            dy, dz = (a, b) if half == 0 else (b, a)
            return up(z, dz) * 8 + up(y, dy) * 2 + core

        def region(self, half, a, b, first, count, core=None):
            block = self.block(half, a, b, c if core is None else core)
            return self.buf.at[block, pl.ds(half * 64 + first, count)]

        def recv(self, half, index):
            return ici_recv.at[self.g * 40 + half * 20 + index]

        def send(self, half, along_a, direction, region, index):
            device = (at_y if (half == 0) == along_a else at_z)(direction)
            push(region, region, ici_send.at[self.g], self.recv(half, index), device)

        def share(self, half, ai, bi):
            region = self.region(half, OFFSETS[ai], OFFSETS[bi], 0, 64)
            sem = d2d_recv.at[self.g * 32 + half * 16 + ai * 4 + bi]
            push(region, region, d2d_send.at[self.g], sem, sibling)

        def spread(self, half, ai):
            region = self.region(half, OFFSETS[ai], 0, 0, 64)
            self.send(half, False, 1, region, 4 + 4 * ai)
            self.send(half, False, -1, region, 5 + 4 * ai)

        def start(self):
            for half in range(2):
                region = self.region(half, 0, 0, 0, 64)
                self.send(half, True, 1, region, 0)
                self.send(half, True, -1, region, 1)
            for half in range(2):
                self.spread(half, 0)
                self.share(half, 0, 0)

        def first_near(self, half, j):
            offset = (-1, 1)[j]
            arrived(self.region(half, offset, 0, 0, 64), self.recv(half, j))
            self.send(half, True, -offset, self.region(half, offset, 0, 32 * j, 32), 2 + j)
            self.spread(half, 1 + j)
            self.share(half, 1 + j, 0)

        def first_far(self, half):
            for j in range(2):
                arrived(self.region(half, 2, 0, 32 * j, 32), self.recv(half, 2 + j))
            self.spread(half, 3)
            self.share(half, 3, 0)

        def second_near(self, half, ai, j):
            offset = (-1, 1)[j]
            a = OFFSETS[ai]
            arrived(self.region(half, a, offset, 0, 64), self.recv(half, 4 + 4 * ai + j))
            part = self.region(half, a, offset, 32 * j, 32)
            self.send(half, False, -offset, part, 6 + 4 * ai + j)
            self.share(half, ai, 1 + j)

        def second_far(self, half, ai):
            for j in range(2):
                region = self.region(half, OFFSETS[ai], 2, 32 * j, 32)
                arrived(region, self.recv(half, 6 + 4 * ai + j))
            self.share(half, ai, 3)

        def shared(self, dy, dz):
            for half in range(2):
                a, b = (dy, dz) if half == 0 else (dz, dy)
                index = half * 16 + OFFSETS.index(a) * 4 + OFFSETS.index(b)
                region = self.region(half, a, b, 0, 64, 1 - c)
                arrived(region, d2d_recv.at[self.g * 32 + index])

        def steps(self):
            groups = []
            groups.append([lambda h=h, j=j: self.first_near(h, j) for j in (0, 1) for h in (0, 1)])
            groups.append(
                [lambda h=h, j=j: self.second_near(h, 0, j) for j in (0, 1) for h in (0, 1)]
            )
            groups.append([lambda h=h: self.first_far(h) for h in (0, 1)])
            groups.append(
                [
                    lambda h=h, j=j, a=a: self.second_near(h, a, j)
                    for a in (1, 2)
                    for j in (0, 1)
                    for h in (0, 1)
                ]
            )
            groups.append([lambda h=h: self.second_far(h, 0) for h in (0, 1)])
            groups.append(
                [lambda h=h, j=j: self.second_near(h, 3, j) for j in (0, 1) for h in (0, 1)]
            )
            groups.append([lambda h=h, a=a: self.second_far(h, a) for a in (1, 2, 3) for h in (0, 1)])
            return groups

        def finish(self):
            arrived(self.buf.at[pl.ds(0, 15)], ici_send.at[self.g])
            arrived(self.buf.at[pl.ds(0, 16)], d2d_send.at[self.g])

    def run(group):
        for step in group:
            step()

    near = [(dy, dz) for dy in (0, -1, 1) for dz in (0, -1, 1)]
    far = [(dy, dz) for dy in OFFSETS for dz in OFFSETS if 2 in (dy, dz)]

    def multiply(gather, chips, first_row, fresh):
        rows = TOK + HALO - first_row
        for n, (dy, dz) in enumerate(chips):
            gather.shared(dy, dz)
            chip = up(z, dz) * 4 + up(y, dy)
            left = xn[chip, pl.ds(first_row, rows)]
            right = gather.buf[pl.ds(chip * 2, 2)].reshape(256, 1536)
            part = dot_nn(left, right)
            if fresh and n == 0:
                acc[pl.ds(first_row, rows)] = part
            else:
                acc[pl.ds(first_row, rows)] += part

    gather_q, gather_c = Gather(0, gat_q), Gather(1, gat_c)
    for load in loads[1:4]:
        load.wait()
    gather_q.start()
    steps_q = gather_q.steps()
    run(steps_q[0])
    run(steps_q[1])
    token_forward()
    run(steps_q[2])
    run(steps_q[3][:4])
    token_rest()

    total = jnp.zeros((TOK, 1), F32)
    for i in range(4):
        wide = raw[i].astype(F32)
        total = total + jnp.sum(wide * wide, axis=1, keepdims=True)
    inverse = lax.rsqrt(total / FEATS + NORM_EPS)
    for i in range(4):
        for j in range(4):
            lanes = slice(256 * j, 256 * (j + 1))
            wide = raw[i, :, lanes].astype(F32) * inverse * gain[:, 1024 * i + 256 * j :][:, :256]
            xn[4 * i + j, pl.ds(HALO, TOK)] = wide.astype(BF16)
    run(steps_q[3][4:])
    run(steps_q[4])
    edge = pl.ds(TOK, HALO)
    halo_copy = push(
        xn.at[:, edge], xn.at[:, pl.ds(0, HALO)], misc_send.at[0], misc_recv.at[0], at_rank(after)
    )

    loads[7].wait()
    loads[8].wait()
    low = jnp.zeros((TOK, 256), F32)
    for i in range(16):
        rows = pl.ds(256 * i, 256)
        both = jnp.concatenate([low_d[rows], low_r[rows]], axis=1)
        low = low + dot_nn(xn[i, pl.ds(HALO, TOK)], both)
    decay_low = jnp.tanh(low[:, :128]).astype(BF16)
    rate_low = low[:, 128:].astype(BF16)
    by_position = jnp.broadcast_to(position_decay[...], (128, TOK)).T
    for p in range(PAIRS):
        lanes = slice(128 * p, 128 * (p + 1))
        logits = channel_decay[:, lanes] + dot_nn(decay_low, decay_second[:, lanes]) + by_position
        extra = jnp.where(
            iota((TOK, 128), 1) < 64,
            extra_decay[:, 2 * p : 2 * p + 1],
            extra_decay[:, 2 * p + 1 : 2 * p + 2],
        )
        decay_s[p] = -DECAY_FACTOR * jax.nn.sigmoid(logits) + extra
        rate_s[p] = jax.nn.sigmoid(
            channel_rate[:, lanes] + dot_nn(rate_low, rate_second[:, lanes])
        )
    row, col = iota((TOK, TOK), 0), iota((TOK, TOK), 1)
    summing = (((row // BLK) == (col // BLK)) & (row >= col)).astype(F32).astype(BF16)
    for p in range(PAIRS):
        cum_s[p] = exact_left(summing, decay_s[p])

    multiply(gather_q, near[:4], HALO, True)
    run(steps_q[5])
    for load in loads[4:7]:
        load.wait()
    gather_c.start()
    multiply(gather_q, near[4:], HALO, False)
    run(steps_q[6])
    multiply(gather_q, far, HALO, False)
    body = pl.ds(HALO, TOK)
    for p in range(PAIRS):
        for i, dst in enumerate((q_s, k_s, v_s)):
            rounded = acc[body, 512 * i + 128 * p : 512 * i + 128 * (p + 1)].astype(BF16)
            dst[p] = rounded.astype(F32)

    steps_c = gather_c.steps()
    during = {1: steps_c[0], 2: steps_c[1], 3: steps_c[2]}

    def one_pair(p, carry):
        for at, group in during.items():
            pl.when(p == at)(lambda group=group: run(group))
        recalled, probe, state, chain = pair_local(
            q_s[p], k_s[p], v_s[p], decay_s[p], rate_s[p], cum_s[p]
        )
        rec_s[p] = recalled
        probe_s[p] = probe
        st1[c, 2 * p] = chain.astype(BF16)
        st1[c, 2 * p + 1] = state.astype(BF16)
        return carry

    lax.fori_loop(0, PAIRS, one_pair, 0)

    copies = [push(st1.at[c], st1.at[c], misc_send.at[1], misc_recv.at[1], sibling)]
    run(steps_c[3])
    arrived(st1.at[1 - c], misc_recv.at[1])

    def held(ref, slot, p):
        return ref[slot, 2 * p].astype(F32), ref[slot, 2 * p + 1].astype(F32)

    for n in range(2):
        p = 2 * c + n
        chain, state = compose(held(st1, 0, p), held(st1, 1, p))
        st2[y, 2 * n] = chain.astype(BF16)
        st2[y, 2 * n + 1] = state.astype(BF16)
    for i, o in enumerate(OFFSETS[1:]):
        copies.append(push(st2.at[y], st2.at[y], misc_send.at[2 + i], misc_recv.at[2 + i], at_y(o)))
    run(steps_c[4])
    for i, o in enumerate(OFFSETS[1:]):
        arrived(st2.at[up(y, -o)], misc_recv.at[2 + i])
    ahead = []
    for n in range(2):
        total_map = held(st2, 0, n)
        eye = (iota((64, 128), 0) == lax.rem(iota((64, 128), 1), 64)).astype(F32)
        prefix = (eye, jnp.zeros((64, 128), F32))
        for k in range(1, 4):
            prefix = tuple(jnp.where(y >= k, new, old) for new, old in zip(total_map, prefix))
            total_map = compose(total_map, held(st2, k, n))
        ahead.append(prefix)
        st3[z, 2 * n] = total_map[0].astype(BF16)
        st3[z, 2 * n + 1] = total_map[1].astype(BF16)
    for i, o in enumerate(OFFSETS[1:]):
        copies.append(push(st3.at[z], st3.at[z], misc_send.at[5 + i], misc_recv.at[5 + i], at_z(o)))
    run(steps_c[5])
    for i, o in enumerate(OFFSETS[1:]):
        arrived(st3.at[up(z, -o)], misc_recv.at[5 + i])
    for n in range(2):
        p = 2 * c + n
        state = jnp.concatenate([start_state[2 * p], start_state[2 * p + 1]], axis=1)
        for k in range(3):
            state = jnp.where(z > k, advance(state, held(st3, k, n)), state)
        ent[p] = advance(state, ahead[n])
    copies.append(
        push(
            ent.at[pl.ds(2 * c, 2)],
            ent.at[pl.ds(2 * c, 2)],
            misc_send.at[8],
            misc_recv.at[8],
            sibling,
        )
    )
    arrived(xn.at[:, pl.ds(0, HALO)], misc_recv.at[0])
    halo = xn[:, pl.ds(0, HALO)]
    xn[:, pl.ds(0, HALO)] = jnp.where(rank == 0, jnp.zeros_like(halo), halo)
    multiply(gather_c, near, 0, True)
    arrived(ent.at[pl.ds(2 * (1 - c), 2)], misc_recv.at[8])
    for p in range(PAIRS):
        lanes = slice(128 * p, 128 * (p + 1))
        state = ent[p]
        state = jnp.where(c == 1, advance(state, held(st1, 0, p)), state)
        recalled = rec_s[p] + fine(dot_nt, probe_s[p], diagonal_blocks(state))
        center = recalled - head_sums(recalled) * (1.0 / 64)
        variance = head_sums(center * center) * (1.0 / 64)
        normed = center * lax.rsqrt(variance + GROUP_EPS) * norm_gain[:, lanes]
        own = head_sums(q_s[p] * k_s[p] * own_weight[:, lanes]) * v_s[p]
        lin_out[:, lanes] = (normed + own).astype(BF16)

    run(steps_c[6])
    multiply(gather_c, far, 0, False)
    squares = jnp.zeros((TOK, 128), F32)
    for p in range(PAIRS):
        lanes = slice(128 * p, 128 * (p + 1))
        outer, inner, signal = (
            acc[:, 512 * i + 128 * p : 512 * i + 128 * (p + 1)].astype(BF16).astype(F32)
            for i in range(3)
        )
        mixed = (inner * signal).astype(BF16).astype(F32)
        tap = taps[:, lanes].astype(F32)
        gated = outer[HALO:] * (
            tap[0:1] * pltpu.roll(mixed, 2, 0)[HALO:]
            + tap[1:2] * pltpu.roll(mixed, 1, 0)[HALO:]
            + tap[2:3] * mixed[HALO:]
        )
        q_s[p] = gated
        squares = squares + gated * gated
    column = jnp.broadcast_to(jnp.sum(squares, axis=1, keepdims=True), (TOK, 128))
    sq_s[x] = column.T[:8]
    for i, o in enumerate(OFFSETS[1:]):
        copies.append(push(sq_s.at[x], sq_s.at[x], misc_send.at[9 + i], misc_recv.at[9 + i], at_x(o)))
    gather_q.finish()
    gather_c.finish()
    for copy in tok_copies:
        copy.wait_send()
    halo_copy.wait_send()
    for i, o in enumerate(OFFSETS[1:]):
        arrived(sq_s.at[up(x, -o)], misc_recv.at[9 + i])
    summed = sq_s[0] + sq_s[1] + sq_s[2] + sq_s[3]
    column = jnp.concatenate([summed] * 16, axis=0).T
    scale = lax.rsqrt(column / 2048 + NORM_EPS)
    for p in range(PAIRS):
        lanes = slice(128 * p, 128 * (p + 1))
        conv_out[:, lanes] = (q_s[p] * scale * conv_gain[:, lanes]).astype(BF16)
    for copy in copies:
        copy.wait_send()


def shards(
    tokens,
    input_norm_gain,
    query_weight,
    key_weight,
    value_weight,
    decay_first_map,
    decay_second_map,
    channel_decay_offset,
    position_decay_offset,
    extra_log_decay,
    rate_first_map,
    rate_second_map,
    channel_rate_offset,
    own_term_weight,
    head_norm_gain,
    starting_state,
    outer_gate_weight,
    inner_gate_weight,
    signal_weight,
    convolution_taps,
    convolution_gain,
):
    far = pl.BlockSpec(memory_space=pl.ANY)
    near = pl.BlockSpec(memory_space=pltpu.VMEM)

    def line(v):
        return v.reshape(1, -1)

    pair = pltpu.VMEM((PAIRS, TOK, 128), F32)
    dma = pltpu.SemaphoreType.DMA
    out = jax.ShapeDtypeStruct((TOK, 512), BF16)
    return pl.pallas_call(
        kernel,
        name="mixer",
        out_shape=(out, out),
        in_specs=[far, near, far, far, far, far, near, near, near, near, far]
        + [near] * 5
        + [far, far, far, near, near],
        out_specs=(near, near),
        scratch_shapes=[
            pltpu.VMEM((32, 128, 1536), BF16),
            pltpu.VMEM((32, 128, 1536), BF16),
            pltpu.VMEM((4, TOK, 1024), BF16),
            pltpu.VMEM((16, TOK + HALO, 256), BF16),
            pltpu.VMEM((FEATS, 128), BF16),
            pltpu.VMEM((FEATS, 128), BF16),
            pltpu.VMEM((TOK + HALO, 1536), F32),
        ]
        + [pair] * 8
        + [
            pltpu.VMEM((2, 8, 64, 128), BF16),
            pltpu.VMEM((4, 4, 64, 128), BF16),
            pltpu.VMEM((4, 4, 64, 128), BF16),
            pltpu.VMEM((PAIRS, 64, 128), F32),
            pltpu.VMEM((4, 8, TOK), F32),
            dma((9,)),
            dma((4,)),
            dma((4,)),
            dma((2,)),
            dma((80,)),
            dma((2,)),
            dma((64,)),
            dma((12,)),
            dma((12,)),
        ],
        compiler_params=pltpu.CompilerParams(
            collective_id=0, has_side_effects=True, vmem_limit_bytes=60 * 1024 * 1024
        ),
    )(
        tokens,
        line(input_norm_gain),
        query_weight,
        key_weight,
        value_weight,
        decay_first_map,
        decay_second_map,
        line(channel_decay_offset),
        line(position_decay_offset),
        extra_log_decay,
        rate_first_map,
        rate_second_map,
        line(channel_rate_offset),
        line(own_term_weight),
        line(head_norm_gain),
        starting_state,
        outer_gate_weight,
        inner_gate_weight,
        signal_weight,
        convolution_taps,
        line(convolution_gain),
    )


def solution(mesh):
    torus = Mesh(mesh.devices.reshape(4, 4, 2, mesh.shape["tp"]), (*SP, "tp"))
    return jax.shard_map(
        shards,
        mesh=torus,
        in_specs=(
            P(SP, "tp"),
            P(),
            P(SP, "tp"),
            P(SP, "tp"),
            P(SP, "tp"),
            P(),
            P(None, "tp"),
            P("tp"),
            P(SP),
            P(SP, "tp"),
            P(),
            P(None, "tp"),
            P("tp"),
            P("tp"),
            P("tp"),
            P("tp", None, None),
            P(SP, "tp"),
            P(SP, "tp"),
            P(SP, "tp"),
            P(None, "tp"),
            P("tp"),
        ),
        out_specs=(P(SP, "tp"), P(SP, "tp")),
        check_vma=False,
    )
```

```python
import jax
import jax.numpy as jnp
from jax import lax
from jax.experimental import pallas as pl
from jax.experimental.pallas import tpu as pltpu
from jax.sharding import Mesh
from jax.sharding import PartitionSpec as P

SP = ("sp_0", "sp_1", "sp_2")
MESH_IDS = pl.DeviceIdType.MESH
F32 = jnp.float32
BF16 = jnp.bfloat16

DECAY_FACTOR = 0.606531
NORM_EPS = 1e-06
GROUP_EPS = 0.00064
KEY_EPS = 1e-06

TOK = 256
HALO = 16
FEATS = 4096
BLK = 64
PAIRS = 4
OFFSETS = (0, -1, 1, 2)


def dot_nn(a, b):
    return lax.dot_general(a, b, (((1,), (0,)), ((), ())), preferred_element_type=F32)


def dot_nt(a, b):
    return lax.dot_general(a, b, (((1,), (1,)), ((), ())), preferred_element_type=F32)


def parts(a):
    high = a.astype(BF16)
    return high, (a - high.astype(F32)).astype(BF16)


def dot_tn(a, b):
    return lax.dot_general(a, b, (((0,), (0,)), ((), ())), preferred_element_type=F32)


def fine(dot, a, b):
    ah, al = parts(a)
    bh, bl = parts(b)
    a_dim = 0 if dot is dot_tn else 1
    b_dim = 1 if dot is dot_nt else 0
    return dot(
        jnp.concatenate([ah, al, ah], axis=a_dim), jnp.concatenate([bh, bh, bl], axis=b_dim)
    )


def exact_left(a, b):
    high, rest = parts(b)
    mid = (b - high.astype(F32) - rest.astype(F32)).astype(BF16)
    return dot_nn(a, high) + (dot_nn(a, rest) + dot_nn(a, mid))


def iota(shape, dim):
    return lax.broadcasted_iota(jnp.int32, shape, dim)


def same_head():
    return (iota((128, 128), 0) // 64) == (iota((128, 128), 1) // 64)


def diagonal_blocks(compact):
    return jnp.where(same_head(), jnp.concatenate([compact, compact], axis=0), 0.0)


def head_sums(values):
    ones = same_head().astype(F32).astype(BF16)
    high, rest = parts(values)
    return dot_nn(high, ones) + dot_nn(rest, ones)


def spread_heads(values):
    both = jnp.concatenate([values, values], axis=0)
    return jnp.where(same_head(), both, jnp.zeros_like(both))


def pair_local(q, k, v, decay, rate, cum):
    chunks = range(TOK // BLK)
    rows = [slice(BLK * n, BLK * (n + 1)) for n in chunks]
    later, earlier = iota((BLK, 128), 0), lax.rem(iota((BLK, 128), 1), BLK)
    strict, inclusive = later > earlier, later >= earlier
    unit = k * lax.rsqrt(head_sums(k * k) + KEY_EPS)
    grow = jnp.exp(-cum)
    a = -unit * jnp.exp(cum - decay)
    b = unit * rate
    r = q * jnp.exp(cum)
    a16, r16, v16 = a.astype(BF16), r.astype(BF16), v.astype(BF16)
    b16, k16 = (b * grow).astype(BF16), (k * grow).astype(BF16)
    grams = [
        dot_nt(
            jnp.concatenate([a16[t], r16[t]], axis=0),
            jnp.concatenate([spread_heads(b16[t]), spread_heads(k16[t])], axis=0),
        )
        for t in rows
    ]
    power = [jnp.where(strict, g[:BLK, :128], 0.0).astype(BF16) for g in grams]
    writes = [jnp.where(strict, g[:BLK, 128:], 0.0).astype(BF16) for g in grams]
    reads = [
        jnp.concatenate(
            [
                jnp.where(inclusive, g[BLK:, :128], 0.0).astype(BF16),
                jnp.where(inclusive, g[BLK:, 128:], 0.0).astype(BF16),
            ],
            axis=1,
        )
        for g in grams
    ]
    values = [spread_heads(v16[t]) for t in rows]
    keys_solved = [a[t] for t in rows]
    free_solved = [dot_nn(writes[n], values[n]) for n in chunks]
    for level in range(6):
        for n in chunks:
            right = [spread_heads(keys_solved[n].astype(BF16))]
            right.append(spread_heads(free_solved[n].astype(BF16)))
            if level < 5:
                right.append(spread_heads(power[n]))
            product = dot_nn(power[n], jnp.concatenate(right, axis=1))
            keys_solved[n] = keys_solved[n] + product[:, :128]
            free_solved[n] = free_solved[n] + product[:, 128:256]
            if level < 5:
                power[n] = product[:, 256:].astype(BF16)
    read = []
    for n in chunks:
        top = [spread_heads(keys_solved[n].astype(BF16)), spread_heads(free_solved[n].astype(BF16))]
        low = [jnp.zeros((128, 128), BF16), values[n]]
        right = jnp.concatenate([jnp.concatenate(t, axis=1) for t in (top, low)], axis=0)
        read.append(dot_nn(reads[n], right))
    eye = iota((128, 128), 0) == iota((128, 128), 1)
    steps, gains = [], []
    for n in chunks:
        last = cum[BLK * (n + 1) - 1 : BLK * (n + 1), :]
        fade = jnp.exp(last - cum[rows[n]])
        b_end, k_end = b[rows[n]] * fade, k[rows[n]] * fade
        solved = jnp.concatenate([keys_solved[n], free_solved[n]], axis=1)
        both = fine(dot_tn, solved, b_end)
        step = jnp.where(same_head(), both[:128], 0.0)
        steps.append(step + jnp.where(eye, jnp.broadcast_to(jnp.exp(last), (128, 128)), 0.0))
        gain = both[128:] + fine(dot_tn, v[rows[n]], k_end)
        gains.append(jnp.where(same_head(), gain, 0.0))
    state, chain = gains[0], steps[0]
    recalled, probes = [read[0][:, 128:]], [r[rows[0]] + read[0][:, :128]]
    for n in chunks[1:]:
        carried = jnp.concatenate([state, chain], axis=0)
        both = fine(dot_nt, r[rows[n]] + read[n][:, :128], carried)
        recalled.append(read[n][:, 128:] + both[:, :128])
        probes.append(both[:, 128:])
        both = fine(dot_nn, carried, steps[n])
        state, chain = both[:128] + gains[n], both[128:]
    return (
        jnp.concatenate(recalled, axis=0),
        jnp.concatenate(probes, axis=0),
        state[:64] + state[64:],
        chain[:64] + chain[64:],
    )


def compose(earlier, later):
    both = fine(dot_nn, jnp.concatenate(earlier, axis=0), diagonal_blocks(later[0]))
    return both[:64], both[64:] + later[1]


def advance(state, later):
    return fine(dot_nn, state, diagonal_blocks(later[0])) + later[1]


def kernel(
    tokens,
    gain,
    wq,
    wk,
    wv,
    decay_first,
    decay_second,
    channel_decay,
    position_decay,
    extra_decay,
    rate_first,
    rate_second,
    channel_rate,
    own_weight,
    norm_gain,
    start_state,
    wo,
    wi,
    wsig,
    taps,
    conv_gain,
    lin_out,
    conv_out,
    gat_q,
    gat_c,
    raw,
    xn,
    low_d,
    low_r,
    acc,
    q_s,
    k_s,
    v_s,
    decay_s,
    rate_s,
    cum_s,
    rec_s,
    probe_s,
    st1,
    st2,
    st3,
    pre,
    ent,
    sq_s,
    load_sem,
    tok_send,
    tok_recv,
    ici_send,
    ici_recv,
    d2d_send,
    d2d_recv,
    misc_send,
    misc_recv,
):
    z, y, c = (lax.axis_index(n) for n in SP)
    x = lax.axis_index("tp")

    def up(pos, offset):
        return lax.rem(pos + (offset + 4), 4)

    def at_x(o):
        return {"tp": up(x, o)}

    def at_y(o):
        return {"sp_1": up(y, o), "sp_2": 1 - c}

    def at_z(o):
        return {"sp_0": up(z, o), "sp_2": 1 - c}

    def along(o):
        return {"sp_0": up(z, (1 - c) * o), "sp_1": up(y, c * o)}

    sibling = {"sp_2": 1 - c}
    rank = z * 8 + y * 2 + c
    after, before = lax.rem(rank + 1, 32), lax.rem(rank + 31, 32)

    def at_rank(r):
        return {"sp_0": r // 8, "sp_1": lax.rem(r // 2, 4), "sp_2": lax.rem(r, 2)}

    def push(src, dst, send, recv, device):
        copy = pltpu.make_async_remote_copy(
            src_ref=src,
            dst_ref=dst,
            send_sem=send,
            recv_sem=recv,
            device_id=device,
            device_id_type=MESH_IDS,
        )
        copy.start()
        return copy

    def arrived(region, recv):
        pltpu.make_async_copy(region, region, recv).wait()

    loads = [pltpu.make_async_copy(tokens, raw.at[x], load_sem.at[0])]
    for n, (buf, weights) in enumerate(((gat_q, (wq, wk, wv)), (gat_c, (wo, wi, wsig)))):
        for i, (w, first, count, half, at) in enumerate(
            (
                (weights[0], 0, 512, 0, 0),
                (weights[1], 0, 256, 0, 512),
                (weights[1], 256, 256, 1, 0),
                (weights[2], 0, 512, 1, 256),
            )
        ):
            src, dst = w.at[:, pl.ds(first, count)], buf.at[half, rank, :, pl.ds(at, count)]
            loads.append(pltpu.make_async_copy(src, dst, load_sem.at[1 + 4 * n + i]))
    loads.append(pltpu.make_async_copy(decay_first, low_d, load_sem.at[9]))
    loads.append(pltpu.make_async_copy(rate_first, low_r, load_sem.at[10]))
    for load in loads:
        load.start()

    barrier = pltpu.get_barrier_semaphore()
    partners = [f(o) for f in (at_x, at_y, at_z) for o in OFFSETS[1:]] + [along(1), along(-1)]
    partners += [sibling, at_rank(after), at_rank(before)]
    for partner in partners:
        pl.semaphore_signal(barrier, inc=1, device_id=partner, device_id_type=MESH_IDS)
    pl.semaphore_wait(barrier, len(partners))

    loads[0].wait()
    tok_copies = [
        push(raw.at[x], raw.at[x], tok_send.at[0], tok_recv.at[0], at_x(1)),
        push(raw.at[x], raw.at[x], tok_send.at[1], tok_recv.at[1], at_x(-1)),
    ]

    def token_forward():
        left, right = up(x, -1), up(x, 1)
        arrived(raw.at[left], tok_recv.at[0])
        part = raw.at[left, pl.ds(0, 128)]
        tok_copies.append(push(part, part, tok_send.at[2], tok_recv.at[2], at_x(1)))
        arrived(raw.at[right], tok_recv.at[1])
        part = raw.at[right, pl.ds(128, 128)]
        tok_copies.append(push(part, part, tok_send.at[3], tok_recv.at[3], at_x(-1)))

    def token_rest():
        far = up(x, 2)
        arrived(raw.at[far, pl.ds(0, 128)], tok_recv.at[2])
        arrived(raw.at[far, pl.ds(128, 128)], tok_recv.at[3])

    class Gather:
        def __init__(self, which, buf):
            self.g, self.buf = which, buf
            self.first, self.second = 1 - c, c

        def chip(self, ahead, across):
            zz = up(z, (1 - c) * ahead + c * across)
            return zz * 4 + up(y, c * ahead + (1 - c) * across)

        def piece(self, half, ahead, across, part=None):
            blocks = pl.ds(2 * self.chip(ahead, across), 2)
            if part is None:
                return self.buf.at[half, blocks]
            return self.buf.at[half, blocks, pl.ds(64 * part, 64)]

        def recv(self, index):
            return ici_recv.at[self.g * 22 + index]

        def shared(self, index):
            return d2d_recv.at[self.g * 17 + index]

        def send(self, region, direction, index):
            push(region, region, ici_send.at[self.g], self.recv(index), along(direction))

        def share(self, region, index):
            push(region, region, d2d_send.at[self.g], self.shared(index), sibling)

        def start(self):
            self.share(self.buf.at[self.second, rank], 0)
            self.share(self.buf.at[self.first, rank], 1)
            own = self.buf.at[self.first, rank]
            self.send(own, 1, 0)
            self.send(own, -1, 2)

        def start_sibling(self):
            other = rank + 1 - 2 * c
            region = self.buf.at[self.first, other]
            arrived(region, self.shared(0))
            self.send(region, 1, 1)
            self.send(region, -1, 3)
            arrived(self.buf.at[self.second, other], self.shared(1))
            self.spread(0)

        def spread(self, mi):
            region = self.piece(self.second, 0, OFFSETS[mi])
            self.send(region, 1, 6 + 4 * mi)
            self.send(region, -1, 7 + 4 * mi)

        def first_near(self, j):
            offset = (-1, 1)[j]
            for core in range(2):
                block = 2 * self.chip(offset, 0) + (c if core == 0 else 1 - c)
                arrived(self.buf.at[self.first, block], self.recv(2 * j + core))
            self.send(self.piece(self.first, offset, 0, j), -offset, 4 + j)
            self.share(self.piece(self.first, offset, 0), 2 + j)

        def first_far(self):
            for j in range(2):
                arrived(self.piece(self.first, 2, 0, j), self.recv(4 + j))
            self.share(self.piece(self.first, 2, 0), 4)

        def second_start(self, mi):
            arrived(self.piece(self.second, 0, OFFSETS[mi]), self.shared(1 + mi))
            self.spread(mi)

        def second_near(self, mi, j):
            offset = (-1, 1)[j]
            arrived(self.piece(self.second, offset, OFFSETS[mi]), self.recv(6 + 4 * mi + j))
            part = self.piece(self.second, offset, OFFSETS[mi], j)
            self.send(part, -offset, 8 + 4 * mi + j)
            self.share(self.piece(self.second, offset, OFFSETS[mi]), 5 + 3 * mi + j)

        def second_far(self, mi):
            for j in range(2):
                part = self.piece(self.second, 2, OFFSETS[mi], j)
                arrived(part, self.recv(8 + 4 * mi + j))
            self.share(self.piece(self.second, 2, OFFSETS[mi]), 7 + 3 * mi)

        def complete(self, ahead, across):
            if across != 0:
                index = 5 + 3 * OFFSETS.index(ahead) + OFFSETS.index(across) - 1
                arrived(self.piece(self.first, ahead, across), self.shared(index))

        def steps(self):
            def near(mi):
                return [lambda j=j: self.second_near(mi, j) for j in range(2)]

            return [
                [lambda: self.first_near(0), lambda: self.first_near(1)],
                [lambda: self.second_start(1), lambda: self.second_start(2)],
                near(0),
                [self.first_far],
                [lambda: self.second_start(3)],
                near(1),
                near(2),
                [lambda: self.second_far(0)],
                near(3),
                [lambda: self.second_far(1), lambda: self.second_far(2)],
                [lambda: self.second_far(3)],
            ]

        def finish(self):
            arrived(self.buf.at[0, pl.ds(0, 30)], ici_send.at[self.g])
            arrived(self.buf.at[0], d2d_send.at[self.g])

    def run(group):
        for step in group:
            step()

    near = [(a, b) for a in (0, -1, 1) for b in (0, -1, 1)]
    axis_far = [(2, 0), (0, 2)]
    side_far = [(-1, 2), (1, 2), (2, -1), (2, 1)]

    def multiply(gather, chips, first_row, fresh=False):
        rows = pl.ds(first_row, TOK + HALO - first_row)
        for n, (ahead, across) in enumerate(chips):
            gather.complete(ahead, across)
            chip = gather.chip(ahead, across)
            left = xn[chip, rows]
            for half in range(2):
                right = gather.buf[half, pl.ds(chip * 2, 2)].reshape(256, 768)
                part = dot_nn(left, right)
                if fresh and n == 0:
                    acc[half, rows] = part
                else:
                    acc[half, rows] += part

    def projection(i, p):
        at = 512 * i + 128 * p
        return at // 768, slice(at % 768, at % 768 + 128)

    gather_q, gather_c = Gather(0, gat_q), Gather(1, gat_c)
    for load in loads[1:5]:
        load.wait()
    gather_q.start()
    steps_q = gather_q.steps()
    gather_q.start_sibling()
    for n in range(3):
        run(steps_q[n])
    token_forward()
    for n in range(3, 6):
        run(steps_q[n])
    token_rest()

    total = jnp.zeros((TOK, 1), F32)
    for i in range(4):
        wide = raw[i].astype(F32)
        total = total + jnp.sum(wide * wide, axis=1, keepdims=True)
    inverse = lax.rsqrt(total / FEATS + NORM_EPS)
    for i in range(4):
        for j in range(4):
            lanes = slice(256 * j, 256 * (j + 1))
            wide = raw[i, :, lanes].astype(F32) * inverse * gain[:, 1024 * i + 256 * j :][:, :256]
            xn[4 * i + j, pl.ds(HALO, TOK)] = wide.astype(BF16)
    run(steps_q[6])
    run(steps_q[7])
    edge = pl.ds(TOK, HALO)
    halo_copy = push(
        xn.at[:, edge], xn.at[:, pl.ds(0, HALO)], misc_send.at[0], misc_recv.at[0], at_rank(after)
    )

    loads[9].wait()
    loads[10].wait()
    low = jnp.zeros((TOK, 256), F32)
    for i in range(16):
        rows = pl.ds(256 * i, 256)
        both = jnp.concatenate([low_d[rows], low_r[rows]], axis=1)
        low = low + dot_nn(xn[i, pl.ds(HALO, TOK)], both)
    decay_low = jnp.tanh(low[:, :128]).astype(BF16)
    rate_low = low[:, 128:].astype(BF16)
    by_position = jnp.broadcast_to(position_decay[...], (128, TOK)).T
    for p in range(PAIRS):
        lanes = slice(128 * p, 128 * (p + 1))
        logits = channel_decay[:, lanes] + dot_nn(decay_low, decay_second[:, lanes]) + by_position
        heads = [jnp.broadcast_to(extra_decay[h : h + 1], (64, TOK)) for h in (2 * p, 2 * p + 1)]
        extra = jnp.concatenate(heads, axis=0).T
        decay_s[p] = -DECAY_FACTOR * jax.nn.sigmoid(logits) + extra
        rate_s[p] = jax.nn.sigmoid(
            channel_rate[:, lanes] + dot_nn(rate_low, rate_second[:, lanes])
        )
    row, col = iota((TOK, TOK), 0), iota((TOK, TOK), 1)
    summing = (((row // BLK) == (col // BLK)) & (row >= col)).astype(F32).astype(BF16)
    for p in range(PAIRS):
        cum_s[p] = exact_left(summing, decay_s[p])

    multiply(gather_q, near, HALO, True)
    run(steps_q[8])
    multiply(gather_q, axis_far, HALO)
    run(steps_q[9])
    for load in loads[5:9]:
        load.wait()
    gather_c.start()
    multiply(gather_q, side_far, HALO)
    gather_c.start_sibling()
    run(steps_q[10])
    multiply(gather_q, [(2, 2)], HALO)
    body = pl.ds(HALO, TOK)
    for p in range(PAIRS):
        for i, dst in enumerate((q_s, k_s, v_s)):
            half, lanes = projection(i, p)
            dst[p] = acc[half, body, lanes].astype(BF16).astype(F32)

    steps_c = gather_c.steps()

    def held(ref, first, second):
        return ref[first, second, 0].astype(F32), ref[first, second, 1].astype(F32)

    def link(level, p, i):
        return misc_send.at[level + 3 * p + i], misc_recv.at[level + 3 * p + i]

    CORE, YAXIS, ZAXIS, BACK, SQUARES, TOTAL, PREFIX = 1, 16, 28, 40, 44, 47, 51

    def core_send(p):
        part = st1.at[p, c]
        push(part, part, misc_send.at[CORE + p], misc_recv.at[CORE + p], sibling)

    def y_send(p):
        arrived(st1.at[p, 1 - c], misc_recv.at[CORE + p])
        chain, state = compose(held(st1, p, 0), held(st1, p, 1))
        st2[p, y, 0] = chain.astype(BF16)
        st2[p, y, 1] = state.astype(BF16)

        @pl.when(c == 0)
        def _():
            part = st2.at[p, y]
            for i, o in enumerate(OFFSETS[1:]):
                push(part, part, *link(YAXIS, p, i), at_y(o))

    def z_send(p):
        for i, o in enumerate(OFFSETS[1:]):
            arrived(st2.at[p, up(y, -o)], link(YAXIS, p, i)[1])
        eye = (iota((64, 128), 0) == lax.rem(iota((64, 128), 1), 64)).astype(F32)
        prefix = (eye, jnp.zeros((64, 128), F32))
        total_map = held(st2, p, 0)
        for k in range(1, 4):
            prefix = tuple(jnp.where(y >= k, new, old) for new, old in zip(total_map, prefix))
            total_map = compose(total_map, held(st2, p, k))
        for i in range(2):
            pre[p, i] = prefix[i]
            st3[p, z, i] = total_map[i].astype(BF16)
        part = st3.at[p, z]
        for i, o in enumerate(OFFSETS[1:]):
            push(part, part, *link(ZAXIS, p, i), at_z(o))
        push(part, part, misc_send.at[TOTAL + p], misc_recv.at[TOTAL + p], sibling)
        push(pre.at[p], pre.at[p], misc_send.at[PREFIX + p], misc_recv.at[PREFIX + p], sibling)

    def back_send(p):
        for i, o in enumerate(OFFSETS[1:]):
            arrived(st3.at[p, up(z, -o)], link(ZAXIS, p, i)[1])
        arrived(st3.at[p, z], misc_recv.at[TOTAL + p])
        arrived(pre.at[p], misc_recv.at[PREFIX + p])
        state = jnp.concatenate([start_state[2 * p], start_state[2 * p + 1]], axis=1)
        for k in range(3):
            state = jnp.where(z > k, advance(state, held(st3, p, k)), state)
        ent[p] = advance(state, (pre[p, 0], pre[p, 1]))
        push(ent.at[p], ent.at[p], misc_send.at[BACK + p], misc_recv.at[BACK + p], sibling)

    during = {1: steps_c[0], 2: steps_c[1], 3: steps_c[2]}

    def one_pair(p, carry):
        for at, group in during.items():
            pl.when(p == at)(lambda group=group: run(group))
        recalled, probe, state, chain = pair_local(
            q_s[p], k_s[p], v_s[p], decay_s[p], rate_s[p], cum_s[p]
        )
        rec_s[p] = recalled
        probe_s[p] = probe
        st1[p, c, 0] = chain.astype(BF16)
        st1[p, c, 1] = state.astype(BF16)
        core_send(p)
        pl.when(p >= 1)(lambda: y_send(p - 1))
        pl.when((p >= 2) & (c == 1))(lambda: z_send(p - 2))
        return carry

    lax.fori_loop(0, PAIRS, one_pair, 0)
    y_send(3)

    def last_maps(p, carry):
        pl.when(c == 1)(lambda: z_send(p + 2))
        pl.when(c == 0)(lambda: back_send(p))
        return carry

    def last_states(p, carry):
        back_send(p)
        return carry

    lax.fori_loop(0, 1, last_maps, 0)
    run(steps_c[3])
    run(steps_c[4])
    lax.fori_loop(1, 2, last_maps, 0)
    run(steps_c[5])
    arrived(xn.at[:, pl.ds(0, HALO)], misc_recv.at[0])
    halo = xn[:, pl.ds(0, HALO)]
    xn[:, pl.ds(0, HALO)] = jnp.where(rank == 0, jnp.zeros_like(halo), halo)
    run(steps_c[6])

    @pl.when(c == 0)
    def _():
        lax.fori_loop(2, 4, last_states, 0)

    run(steps_c[7])

    def finish_pair(p, carry):
        pl.when(c == 1)(lambda: arrived(ent.at[p], misc_recv.at[BACK + p]))
        state = ent[p]
        state = jnp.where(c == 1, advance(state, held(st1, p, 0)), state)
        recalled = rec_s[p] + fine(dot_nt, probe_s[p], diagonal_blocks(state))
        center = recalled - head_sums(recalled) * (1.0 / 64)
        variance = head_sums(center * center) * (1.0 / 64)
        lanes = pl.ds(pl.multiple_of(128 * p, 128), 128)
        normed = center * lax.rsqrt(variance + GROUP_EPS) * norm_gain[:, lanes]
        own = head_sums(q_s[p] * k_s[p] * own_weight[:, lanes]) * v_s[p]
        lin_out[:, lanes] = (normed + own).astype(BF16)
        return carry

    multiply(gather_c, near, 0, True)
    run(steps_c[8])
    lax.fori_loop(0, PAIRS, finish_pair, 0)

    multiply(gather_c, axis_far, 0)
    run(steps_c[9])
    multiply(gather_c, side_far, 0)
    run(steps_c[10])
    multiply(gather_c, [(2, 2)], 0)
    squares = jnp.zeros((TOK, 128), F32)
    for p in range(PAIRS):
        lanes = slice(128 * p, 128 * (p + 1))
        sums = [acc[projection(i, p)[0], :, projection(i, p)[1]] for i in range(3)]
        outer, inner, signal = (t.astype(BF16).astype(F32) for t in sums)
        mixed = (inner * signal).astype(BF16).astype(F32)
        tap = taps[:, lanes].astype(F32)
        gated = outer[HALO:] * (
            tap[0:1] * pltpu.roll(mixed, 2, 0)[HALO:]
            + tap[1:2] * pltpu.roll(mixed, 1, 0)[HALO:]
            + tap[2:3] * mixed[HALO:]
        )
        q_s[p] = gated
        squares = squares + gated * gated
    column = jnp.broadcast_to(jnp.sum(squares, axis=1, keepdims=True), (TOK, 128))
    sq_s[x] = column.T[:8]
    for i, o in enumerate(OFFSETS[1:]):
        push(sq_s.at[x], sq_s.at[x], misc_send.at[SQUARES + i], misc_recv.at[SQUARES + i], at_x(o))
    gather_q.finish()
    gather_c.finish()
    for copy in tok_copies:
        copy.wait_send()
    halo_copy.wait_send()
    for i, o in enumerate(OFFSETS[1:]):
        arrived(sq_s.at[up(x, -o)], misc_recv.at[SQUARES + i])
    summed = sq_s[0] + sq_s[1] + sq_s[2] + sq_s[3]
    column = jnp.concatenate([summed] * 16, axis=0).T
    scale = lax.rsqrt(column / 2048 + NORM_EPS)
    for p in range(PAIRS):
        lanes = slice(128 * p, 128 * (p + 1))
        conv_out[:, lanes] = (q_s[p] * scale * conv_gain[:, lanes]).astype(BF16)
    for p in range(PAIRS):
        arrived(st1.at[p, c], misc_send.at[CORE + p])

    @pl.when(c == 0)
    def _():
        for p in range(PAIRS):
            arrived(ent.at[p], misc_send.at[BACK + p])
            for i in range(3):
                arrived(st2.at[p, y], link(YAXIS, p, i)[0])

    @pl.when(c == 1)
    def _():
        for p in range(PAIRS):
            arrived(st3.at[p, z], misc_send.at[TOTAL + p])
            arrived(pre.at[p], misc_send.at[PREFIX + p])
            for i in range(3):
                arrived(st3.at[p, z], link(ZAXIS, p, i)[0])

    for i in range(3):
        arrived(sq_s.at[x], misc_send.at[SQUARES + i])


def shards(
    tokens,
    input_norm_gain,
    query_weight,
    key_weight,
    value_weight,
    decay_first_map,
    decay_second_map,
    channel_decay_offset,
    position_decay_offset,
    extra_log_decay,
    rate_first_map,
    rate_second_map,
    channel_rate_offset,
    own_term_weight,
    head_norm_gain,
    starting_state,
    outer_gate_weight,
    inner_gate_weight,
    signal_weight,
    convolution_taps,
    convolution_gain,
):
    far = pl.BlockSpec(memory_space=pl.ANY)
    near = pl.BlockSpec(memory_space=pltpu.VMEM)

    def line(v):
        return v.reshape(1, -1)

    pair = pltpu.VMEM((PAIRS, TOK, 128), F32)
    dma = pltpu.SemaphoreType.DMA
    out = jax.ShapeDtypeStruct((TOK, 512), BF16)
    return pl.pallas_call(
        kernel,
        name="mixer",
        out_shape=(out, out),
        in_specs=[far, near, far, far, far, far, near, near, near, near, far]
        + [near] * 5
        + [far, far, far, near, near],
        out_specs=(near, near),
        scratch_shapes=[
            pltpu.VMEM((2, 32, 128, 768), BF16),
            pltpu.VMEM((2, 32, 128, 768), BF16),
            pltpu.VMEM((4, TOK, 1024), BF16),
            pltpu.VMEM((16, TOK + HALO, 256), BF16),
            pltpu.VMEM((FEATS, 128), BF16),
            pltpu.VMEM((FEATS, 128), BF16),
            pltpu.VMEM((2, TOK + HALO, 768), F32),
        ]
        + [pair] * 8
        + [
            pltpu.VMEM((PAIRS, 2, 2, 64, 128), BF16),
            pltpu.VMEM((PAIRS, 4, 2, 64, 128), BF16),
            pltpu.VMEM((PAIRS, 4, 2, 64, 128), BF16),
            pltpu.VMEM((PAIRS, 2, 64, 128), F32),
            pltpu.VMEM((PAIRS, 64, 128), F32),
            pltpu.VMEM((4, 8, TOK), F32),
            dma((11,)),
            dma((4,)),
            dma((4,)),
            dma((2,)),
            dma((44,)),
            dma((2,)),
            dma((34,)),
            dma((56,)),
            dma((56,)),
        ],
        compiler_params=pltpu.CompilerParams(
            collective_id=0, has_side_effects=True, vmem_limit_bytes=60 * 1024 * 1024
        ),
    )(
        tokens,
        line(input_norm_gain),
        query_weight,
        key_weight,
        value_weight,
        decay_first_map,
        decay_second_map,
        line(channel_decay_offset),
        line(position_decay_offset),
        extra_log_decay.T,
        rate_first_map,
        rate_second_map,
        line(channel_rate_offset),
        line(own_term_weight),
        line(head_norm_gain),
        starting_state,
        outer_gate_weight,
        inner_gate_weight,
        signal_weight,
        convolution_taps,
        line(convolution_gain),
    )


def solution(mesh):
    torus = Mesh(mesh.devices.reshape(4, 4, 2, mesh.shape["tp"]), (*SP, "tp"))
    return jax.shard_map(
        shards,
        mesh=torus,
        in_specs=(
            P(SP, "tp"),
            P(),
            P(SP, "tp"),
            P(SP, "tp"),
            P(SP, "tp"),
            P(),
            P(None, "tp"),
            P("tp"),
            P(SP),
            P(SP, "tp"),
            P(),
            P(None, "tp"),
            P("tp"),
            P("tp"),
            P("tp"),
            P("tp", None, None),
            P(SP, "tp"),
            P(SP, "tp"),
            P(SP, "tp"),
            P(None, "tp"),
            P("tp"),
        ),
        out_specs=(P(SP, "tp"), P(SP, "tp")),
        check_vma=False,
    )
```

```python
import jax
import jax.numpy as jnp
from jax import lax
from jax.experimental import pallas as pl
from jax.experimental.pallas import tpu as pltpu
from jax.sharding import Mesh
from jax.sharding import PartitionSpec as P

SP = ("sp_0", "sp_1", "sp_2")
MESH_IDS = pl.DeviceIdType.MESH
F32 = jnp.float32
BF16 = jnp.bfloat16

DECAY_FACTOR = 0.606531
NORM_EPS = 1e-06
GROUP_EPS = 0.00064
KEY_EPS = 1e-06

TOK = 256
HALO = 16
FEATS = 4096
BLK = 64
PAIRS = 4
OFFSETS = (0, -1, 1, 2)


def dot_nn(a, b):
    return lax.dot_general(a, b, (((1,), (0,)), ((), ())), preferred_element_type=F32)


def dot_nt(a, b):
    return lax.dot_general(a, b, (((1,), (1,)), ((), ())), preferred_element_type=F32)


def parts(a):
    high = a.astype(BF16)
    return high, (a - high.astype(F32)).astype(BF16)


def dot_tn(a, b):
    return lax.dot_general(a, b, (((0,), (0,)), ((), ())), preferred_element_type=F32)


def fine(dot, a, b):
    ah, al = parts(a)
    bh, bl = parts(b)
    a_dim = 0 if dot is dot_tn else 1
    b_dim = 1 if dot is dot_nt else 0
    return dot(
        jnp.concatenate([ah, al, ah], axis=a_dim), jnp.concatenate([bh, bh, bl], axis=b_dim)
    )


def exact_left(a, b):
    high, rest = parts(b)
    mid = (b - high.astype(F32) - rest.astype(F32)).astype(BF16)
    return dot_nn(a, high) + (dot_nn(a, rest) + dot_nn(a, mid))


def iota(shape, dim):
    return lax.broadcasted_iota(jnp.int32, shape, dim)


def same_head():
    return (iota((128, 128), 0) // 64) == (iota((128, 128), 1) // 64)


def diagonal_blocks(compact):
    return jnp.where(same_head(), jnp.concatenate([compact, compact], axis=0), 0.0)


def head_sums(values):
    ones = same_head().astype(F32).astype(BF16)
    high, rest = parts(values)
    return dot_nn(high, ones) + dot_nn(rest, ones)


def spread_heads(values):
    both = jnp.concatenate([values, values], axis=0)
    return jnp.where(same_head(), both, jnp.zeros_like(both))


def pair_local(q, k, v, decay, rate, cum):
    chunks = range(TOK // BLK)
    rows = [slice(BLK * n, BLK * (n + 1)) for n in chunks]
    later, earlier = iota((BLK, 128), 0), lax.rem(iota((BLK, 128), 1), BLK)
    strict, inclusive = later > earlier, later >= earlier
    unit = k * lax.rsqrt(head_sums(k * k) + KEY_EPS)
    grow = jnp.exp(-cum)
    a = -unit * jnp.exp(cum - decay)
    b = unit * rate
    r = q * jnp.exp(cum)
    a16, r16, v16 = a.astype(BF16), r.astype(BF16), v.astype(BF16)
    b16, k16 = (b * grow).astype(BF16), (k * grow).astype(BF16)
    grams = [
        dot_nt(
            jnp.concatenate([a16[t], r16[t]], axis=0),
            jnp.concatenate([spread_heads(b16[t]), spread_heads(k16[t])], axis=0),
        )
        for t in rows
    ]
    power = [jnp.where(strict, g[:BLK, :128], 0.0).astype(BF16) for g in grams]
    writes = [jnp.where(strict, g[:BLK, 128:], 0.0).astype(BF16) for g in grams]
    reads = [
        jnp.concatenate(
            [
                jnp.where(inclusive, g[BLK:, :128], 0.0).astype(BF16),
                jnp.where(inclusive, g[BLK:, 128:], 0.0).astype(BF16),
            ],
            axis=1,
        )
        for g in grams
    ]
    values = [spread_heads(v16[t]) for t in rows]
    keys_solved = [a[t] for t in rows]
    free_solved = [dot_nn(writes[n], values[n]) for n in chunks]
    for level in range(6):
        for n in chunks:
            right = [spread_heads(keys_solved[n].astype(BF16))]
            right.append(spread_heads(free_solved[n].astype(BF16)))
            if level < 5:
                right.append(spread_heads(power[n]))
            product = dot_nn(power[n], jnp.concatenate(right, axis=1))
            keys_solved[n] = keys_solved[n] + product[:, :128]
            free_solved[n] = free_solved[n] + product[:, 128:256]
            if level < 5:
                power[n] = product[:, 256:].astype(BF16)
    read = []
    for n in chunks:
        top = [spread_heads(keys_solved[n].astype(BF16)), spread_heads(free_solved[n].astype(BF16))]
        low = [jnp.zeros((128, 128), BF16), values[n]]
        right = jnp.concatenate([jnp.concatenate(t, axis=1) for t in (top, low)], axis=0)
        read.append(dot_nn(reads[n], right))
    eye = iota((128, 128), 0) == iota((128, 128), 1)
    steps, gains = [], []
    for n in chunks:
        last = cum[BLK * (n + 1) - 1 : BLK * (n + 1), :]
        fade = jnp.exp(last - cum[rows[n]])
        b_end, k_end = b[rows[n]] * fade, k[rows[n]] * fade
        solved = jnp.concatenate([keys_solved[n], free_solved[n]], axis=1)
        both = fine(dot_tn, solved, b_end)
        step = jnp.where(same_head(), both[:128], 0.0)
        steps.append(step + jnp.where(eye, jnp.broadcast_to(jnp.exp(last), (128, 128)), 0.0))
        gain = both[128:] + fine(dot_tn, v[rows[n]], k_end)
        gains.append(jnp.where(same_head(), gain, 0.0))
    state, chain = gains[0], steps[0]
    recalled, probes = [read[0][:, 128:]], [r[rows[0]] + read[0][:, :128]]
    for n in chunks[1:]:
        carried = jnp.concatenate([state, chain], axis=0)
        both = fine(dot_nt, r[rows[n]] + read[n][:, :128], carried)
        recalled.append(read[n][:, 128:] + both[:, :128])
        probes.append(both[:, 128:])
        both = fine(dot_nn, carried, steps[n])
        state, chain = both[:128] + gains[n], both[128:]
    return (
        jnp.concatenate(recalled, axis=0),
        jnp.concatenate(probes, axis=0),
        state[:64] + state[64:],
        chain[:64] + chain[64:],
    )


def compose(earlier, later):
    both = fine(dot_nn, jnp.concatenate(earlier, axis=0), diagonal_blocks(later[0]))
    return both[:64], both[64:] + later[1]


def advance(state, later):
    return fine(dot_nn, state, diagonal_blocks(later[0])) + later[1]


def kernel(
    tokens,
    gain_hbm,
    wq,
    wk,
    wv,
    decay_first,
    decay_second_hbm,
    channel_decay_hbm,
    position_decay_hbm,
    extra_decay_hbm,
    rate_first,
    rate_second_hbm,
    channel_rate_hbm,
    own_weight_hbm,
    norm_gain_hbm,
    start_state_hbm,
    wo,
    wi,
    wsig,
    taps_hbm,
    conv_gain_hbm,
    lin_hbm,
    conv_hbm,
    gain,
    decay_second,
    channel_decay,
    position_decay,
    extra_decay,
    rate_second,
    channel_rate,
    own_weight,
    norm_gain,
    start_state,
    taps,
    conv_gain,
    small_sem,
    lin_out,
    conv_out,
    out_sem,
    gat_q,
    gat_c,
    raw,
    xn,
    low_d,
    low_r,
    acc,
    q_s,
    k_s,
    v_s,
    decay_s,
    rate_s,
    cum_s,
    rec_s,
    probe_s,
    st1,
    st2,
    st3,
    pre,
    ent,
    ent_out,
    sq_s,
    load_sem,
    tok_send,
    tok_recv,
    ici_send,
    ici_recv,
    d2d_send,
    d2d_recv,
    misc_send,
    misc_recv,
):
    z, y, c = (lax.axis_index(n) for n in SP)
    x = lax.axis_index("tp")

    def up(pos, offset):
        return lax.rem(pos + (offset + 4), 4)

    def at_x(o):
        return {"tp": up(x, o)}

    def at_y(o):
        return {"sp_1": up(y, o), "sp_2": 1 - c}

    def at_z(o):
        return {"sp_0": up(z, o), "sp_2": 1 - c}

    def along(o):
        return {"sp_0": up(z, (1 - c) * o), "sp_1": up(y, c * o)}

    sibling = {"sp_2": 1 - c}
    rank = z * 8 + y * 2 + c
    after, before = lax.rem(rank + 1, 32), lax.rem(rank + 31, 32)

    def at_rank(r):
        return {"sp_0": r // 8, "sp_1": lax.rem(r // 2, 4), "sp_2": lax.rem(r, 2)}

    def push(src, dst, send, recv, device):
        copy = pltpu.make_async_remote_copy(
            src_ref=src,
            dst_ref=dst,
            send_sem=send,
            recv_sem=recv,
            device_id=device,
            device_id_type=MESH_IDS,
        )
        copy.start()
        return copy

    def arrived(region, recv):
        pltpu.make_async_copy(region, region, recv).wait()

    loads = [pltpu.make_async_copy(tokens, raw.at[x], load_sem.at[0])]
    for n, (buf, weights) in enumerate(((gat_q, (wq, wk, wv)), (gat_c, (wo, wi, wsig)))):
        for i, (w, first, count, half, at) in enumerate(
            (
                (weights[0], 0, 512, 0, 0),
                (weights[1], 0, 256, 0, 512),
                (weights[1], 256, 256, 1, 0),
                (weights[2], 0, 512, 1, 256),
            )
        ):
            src, dst = w.at[:, pl.ds(first, count)], buf.at[half, rank, :, pl.ds(at, count)]
            loads.append(pltpu.make_async_copy(src, dst, load_sem.at[1 + 4 * n + i]))
    loads.append(pltpu.make_async_copy(decay_first, low_d, load_sem.at[9]))
    loads.append(pltpu.make_async_copy(rate_first, low_r, load_sem.at[10]))
    small = [
        (gain_hbm, gain),
        (decay_second_hbm, decay_second),
        (channel_decay_hbm, channel_decay),
        (position_decay_hbm, position_decay),
        (extra_decay_hbm, extra_decay),
        (rate_second_hbm, rate_second),
        (channel_rate_hbm, channel_rate),
        (own_weight_hbm, own_weight),
        (norm_gain_hbm, norm_gain),
        (start_state_hbm, start_state),
        (taps_hbm, taps),
        (conv_gain_hbm, conv_gain),
    ]
    small = [
        pltpu.make_async_copy(src, dst, small_sem.at[i]) for i, (src, dst) in enumerate(small)
    ]
    for load in loads + small:
        load.start()

    barrier = pltpu.get_barrier_semaphore()
    partners = [f(o) for f in (at_x, at_y, at_z) for o in OFFSETS[1:]] + [along(1), along(-1)]
    partners += [{"sp_1": up(y, o)} for o in OFFSETS[1:]]
    partners += [sibling, at_rank(after), at_rank(before)]
    for partner in partners:
        pl.semaphore_signal(barrier, inc=1, device_id=partner, device_id_type=MESH_IDS)
    pl.semaphore_wait(barrier, len(partners))

    loads[0].wait()
    tok_copies = [
        push(raw.at[x], raw.at[x], tok_send.at[0], tok_recv.at[0], at_x(1)),
        push(raw.at[x], raw.at[x], tok_send.at[1], tok_recv.at[1], at_x(-1)),
    ]

    def token_forward():
        left, right = up(x, -1), up(x, 1)
        arrived(raw.at[left], tok_recv.at[0])
        part = raw.at[left, pl.ds(0, 128)]
        tok_copies.append(push(part, part, tok_send.at[2], tok_recv.at[2], at_x(1)))
        arrived(raw.at[right], tok_recv.at[1])
        part = raw.at[right, pl.ds(128, 128)]
        tok_copies.append(push(part, part, tok_send.at[3], tok_recv.at[3], at_x(-1)))

    def token_rest():
        far = up(x, 2)
        arrived(raw.at[far, pl.ds(0, 128)], tok_recv.at[2])
        arrived(raw.at[far, pl.ds(128, 128)], tok_recv.at[3])

    class Gather:
        def __init__(self, which, buf):
            self.g, self.buf = which, buf
            self.first, self.second = 1 - c, c

        def chip(self, ahead, across):
            zz = up(z, (1 - c) * ahead + c * across)
            return zz * 4 + up(y, c * ahead + (1 - c) * across)

        def piece(self, half, ahead, across, part=None):
            blocks = pl.ds(2 * self.chip(ahead, across), 2)
            if part is None:
                return self.buf.at[half, blocks]
            return self.buf.at[half, blocks, pl.ds(64 * part, 64)]

        def recv(self, index):
            return ici_recv.at[self.g * 22 + index]

        def shared(self, index):
            return d2d_recv.at[self.g * 17 + index]

        def send(self, region, direction, index):
            push(region, region, ici_send.at[self.g], self.recv(index), along(direction))

        def share(self, region, index):
            push(region, region, d2d_send.at[self.g], self.shared(index), sibling)

        def share_own(self):
            self.share(self.buf.at[self.second, rank], 0)
            self.share(self.buf.at[self.first, rank], 1)

        def start(self):
            own = self.buf.at[self.first, rank]
            self.send(own, 1, 0)
            self.send(own, -1, 2)

        def start_sibling(self):
            other = rank + 1 - 2 * c
            region = self.buf.at[self.first, other]
            arrived(region, self.shared(0))
            self.send(region, 1, 1)
            self.send(region, -1, 3)
            arrived(self.buf.at[self.second, other], self.shared(1))
            self.spread(0)

        def spread(self, mi):
            region = self.piece(self.second, 0, OFFSETS[mi])
            self.send(region, 1, 6 + 4 * mi)
            self.send(region, -1, 7 + 4 * mi)

        def first_near(self, j):
            offset = (-1, 1)[j]
            for core in range(2):
                block = 2 * self.chip(offset, 0) + (c if core == 0 else 1 - c)
                arrived(self.buf.at[self.first, block], self.recv(2 * j + core))
            self.send(self.piece(self.first, offset, 0, j), -offset, 4 + j)
            self.share(self.piece(self.first, offset, 0), 2 + j)

        def first_far(self):
            for j in range(2):
                arrived(self.piece(self.first, 2, 0, j), self.recv(4 + j))
            self.share(self.piece(self.first, 2, 0), 4)

        def second_start(self, mi):
            arrived(self.piece(self.second, 0, OFFSETS[mi]), self.shared(1 + mi))
            self.spread(mi)

        def second_near(self, mi, j):
            offset = (-1, 1)[j]
            arrived(self.piece(self.second, offset, OFFSETS[mi]), self.recv(6 + 4 * mi + j))
            part = self.piece(self.second, offset, OFFSETS[mi], j)
            self.send(part, -offset, 8 + 4 * mi + j)
            self.share(self.piece(self.second, offset, OFFSETS[mi]), 5 + 3 * mi + j)

        def second_far(self, mi):
            for j in range(2):
                part = self.piece(self.second, 2, OFFSETS[mi], j)
                arrived(part, self.recv(8 + 4 * mi + j))
            self.share(self.piece(self.second, 2, OFFSETS[mi]), 7 + 3 * mi)

        def complete(self, ahead, across):
            if across != 0:
                index = 5 + 3 * OFFSETS.index(ahead) + OFFSETS.index(across) - 1
                arrived(self.piece(self.first, ahead, across), self.shared(index))

        def steps(self):
            def near(mi):
                return [lambda j=j: self.second_near(mi, j) for j in range(2)]

            return [
                [lambda: self.first_near(0), lambda: self.first_near(1)],
                [lambda: self.second_start(1), lambda: self.second_start(2)],
                near(0),
                [self.first_far],
                [lambda: self.second_start(3)],
                near(1),
                near(2),
                [lambda: self.second_far(0)],
                near(3),
                [lambda: self.second_far(1), lambda: self.second_far(2)],
                [lambda: self.second_far(3)],
            ]

        def finish(self):
            arrived(self.buf.at[0, pl.ds(0, 30)], ici_send.at[self.g])
            arrived(self.buf.at[0], d2d_send.at[self.g])

    def run(group):
        for step in group:
            step()

    near = [(a, b) for a in (0, -1, 1) for b in (0, -1, 1)]
    axis_far = [(2, 0), (0, 2)]
    side_far = [(-1, 2), (1, 2), (2, -1), (2, 1)]

    def multiply(gather, chips, first_row, fresh=False):
        rows = pl.ds(first_row, TOK + HALO - first_row)
        for n, (ahead, across) in enumerate(chips):
            gather.complete(ahead, across)
            chip = gather.chip(ahead, across)
            left = xn[chip, rows]
            for half in range(2):
                right = gather.buf[half, pl.ds(chip * 2, 2)].reshape(256, 768)
                part = dot_nn(left, right)
                if fresh and n == 0:
                    acc[half, rows] = part
                else:
                    acc[half, rows] += part

    def projection(i, p):
        at = 512 * i + 128 * p
        return at // 768, slice(at % 768, at % 768 + 128)

    gather_q, gather_c = Gather(0, gat_q), Gather(1, gat_c)
    for load in loads[1:5]:
        load.wait()
    gather_q.share_own()
    gather_q.start()
    steps_q = gather_q.steps()
    gather_q.start_sibling()
    for n in range(3):
        run(steps_q[n])
    token_forward()
    for n in range(3, 6):
        run(steps_q[n])
    token_rest()

    for load in small:
        load.wait()
    total = jnp.zeros((TOK, 1), F32)
    for i in range(4):
        wide = raw[i].astype(F32)
        total = total + jnp.sum(wide * wide, axis=1, keepdims=True)
    inverse = lax.rsqrt(total / FEATS + NORM_EPS)
    for i in range(4):
        for j in range(4):
            lanes = slice(256 * j, 256 * (j + 1))
            wide = raw[i, :, lanes].astype(F32) * inverse * gain[:, 1024 * i + 256 * j :][:, :256]
            xn[4 * i + j, pl.ds(HALO, TOK)] = wide.astype(BF16)
    run(steps_q[6])
    run(steps_q[7])
    edge = pl.ds(TOK, HALO)
    halo_copy = push(
        xn.at[:, edge], xn.at[:, pl.ds(0, HALO)], misc_send.at[0], misc_recv.at[0], at_rank(after)
    )

    loads[9].wait()
    loads[10].wait()
    low = jnp.zeros((TOK, 256), F32)
    for i in range(16):
        rows = pl.ds(256 * i, 256)
        both = jnp.concatenate([low_d[rows], low_r[rows]], axis=1)
        low = low + dot_nn(xn[i, pl.ds(HALO, TOK)], both)
    decay_low = jnp.tanh(low[:, :128]).astype(BF16)
    rate_low = low[:, 128:].astype(BF16)
    by_position = jnp.broadcast_to(position_decay[...], (128, TOK)).T
    for p in range(PAIRS):
        lanes = slice(128 * p, 128 * (p + 1))
        logits = channel_decay[:, lanes] + dot_nn(decay_low, decay_second[:, lanes]) + by_position
        heads = [jnp.broadcast_to(extra_decay[h : h + 1], (64, TOK)) for h in (2 * p, 2 * p + 1)]
        extra = jnp.concatenate(heads, axis=0).T
        decay_s[p] = -DECAY_FACTOR * jax.nn.sigmoid(logits) + extra
        rate_s[p] = jax.nn.sigmoid(
            channel_rate[:, lanes] + dot_nn(rate_low, rate_second[:, lanes])
        )
    row, col = iota((TOK, TOK), 0), iota((TOK, TOK), 1)
    summing = (((row // BLK) == (col // BLK)) & (row >= col)).astype(F32).astype(BF16)
    for p in range(PAIRS):
        cum_s[p] = exact_left(summing, decay_s[p])

    for load in loads[5:9]:
        load.wait()
    gather_c.share_own()
    multiply(gather_q, near[:6], HALO, True)
    run(steps_q[8])
    gather_c.start()
    gather_c.start_sibling()
    multiply(gather_q, near[6:], HALO)
    multiply(gather_q, axis_far, HALO)
    run(steps_q[9])
    multiply(gather_q, side_far, HALO)
    run(steps_q[10])
    multiply(gather_q, [(2, 2)], HALO)
    body = pl.ds(HALO, TOK)
    for p in range(PAIRS):
        for i, dst in enumerate((q_s, k_s, v_s)):
            half, lanes = projection(i, p)
            dst[p] = acc[half, body, lanes].astype(BF16).astype(F32)

    steps_c = gather_c.steps()
    CORE, Y_MAPS, Z_MAPS, TOTAL, PREFIX, ENTER, SQUARES = 1, 5, 9, 13, 14, 15, 19
    Y_SENT, Z_SENT, BACK_SENT = 24, 28, 32

    def held(ref, *index):
        return ref[(*index, 0)].astype(F32), ref[(*index, 1)].astype(F32)

    def core_send(p):
        part = st1.at[p, c]
        push(part, part, misc_send.at[CORE + p], misc_recv.at[CORE + p], sibling)

    def y_send(p):
        arrived(st1.at[p, 1 - c], misc_recv.at[CORE + p])

        @pl.when((c == 0) | (p == y))
        def _():
            maps = compose(held(st1, p, 0), held(st1, p, 1))
            slot = (1 - c) * (4 + p) + c * y
            for i in range(2):
                st2[slot, i] = maps[i].astype(BF16)

        @pl.when((c == 0) & (p != y))
        def _():
            push(
                st2.at[4 + p],
                st2.at[y],
                misc_send.at[Y_SENT + p],
                misc_recv.at[Y_MAPS + y],
                {"sp_1": p, "sp_2": 1},
            )

    def z_send():
        for o in OFFSETS[1:]:
            arrived(st2.at[up(y, o)], misc_recv.at[Y_MAPS + up(y, o)])
        total_map = held(st2, 0)
        for k in range(1, 4):
            for i in range(2):
                pre[k - 1, i] = total_map[i]
            total_map = compose(total_map, held(st2, k))
        for i in range(2):
            st3[z, i] = total_map[i].astype(BF16)
        part = st3.at[z]
        for i, o in enumerate(OFFSETS[1:]):
            push(part, part, misc_send.at[Z_SENT + i], misc_recv.at[Z_MAPS + i], at_z(o))
        push(part, part, misc_send.at[TOTAL], misc_recv.at[TOTAL], sibling)
        push(pre, pre, misc_send.at[PREFIX], misc_recv.at[PREFIX], sibling)

    def back_send():
        for i, o in enumerate(OFFSETS[1:]):
            arrived(st3.at[up(z, -o)], misc_recv.at[Z_MAPS + i])
        arrived(st3.at[z], misc_recv.at[TOTAL])
        state = jnp.concatenate([start_state[2 * y], start_state[2 * y + 1]], axis=1)
        for k in range(3):
            state = jnp.where(z > k, advance(state, held(st3, k)), state)
        arrived(pre, misc_recv.at[PREFIX])
        ent_out[0] = state.astype(BF16)
        for k in range(3):
            ent_out[k + 1] = advance(state, (pre[k, 0], pre[k, 1])).astype(BF16)
        ent[y] = ent_out[y]
        for i, o in enumerate(OFFSETS[1:]):
            for core in range(2):
                push(
                    ent_out.at[up(y, o)],
                    ent.at[y],
                    misc_send.at[BACK_SENT + 2 * i + core],
                    misc_recv.at[ENTER + y],
                    {"sp_1": up(y, o), "sp_2": core},
                )
        push(ent_out.at[y], ent.at[y], misc_send.at[BACK_SENT + 6], misc_recv.at[ENTER + y], sibling)

    during = dict(enumerate(steps_c[:4]))

    def one_pair(p, carry):
        for at, group in during.items():
            pl.when(p == at)(lambda group=group: run(group))
        recalled, probe, state, chain = pair_local(
            q_s[p], k_s[p], v_s[p], decay_s[p], rate_s[p], cum_s[p]
        )
        rec_s[p] = recalled
        probe_s[p] = probe
        st1[p, c, 0] = chain.astype(BF16)
        st1[p, c, 1] = state.astype(BF16)
        core_send(p)
        pl.when(p >= 1)(lambda: y_send(p - 1))
        return carry

    lax.fori_loop(0, PAIRS, one_pair, 0)
    y_send(3)

    run(steps_c[4])
    run(steps_c[5])
    pl.when(c == 1)(z_send)
    run(steps_c[6])
    pl.when(c == 0)(back_send)
    run(steps_c[7])
    arrived(xn.at[:, pl.ds(0, HALO)], misc_recv.at[0])
    halo = xn[:, pl.ds(0, HALO)]
    xn[:, pl.ds(0, HALO)] = jnp.where(rank == 0, jnp.zeros_like(halo), halo)

    def finish_pair(p, carry):
        pl.when((c == 1) | (p != y))(lambda: arrived(ent.at[p], misc_recv.at[ENTER + p]))
        state = ent[p].astype(F32)
        state = jnp.where(c == 1, advance(state, held(st1, p, 0)), state)
        recalled = rec_s[p] + fine(dot_nt, probe_s[p], diagonal_blocks(state))
        center = recalled - head_sums(recalled) * (1.0 / 64)
        variance = head_sums(center * center) * (1.0 / 64)
        lanes = pl.ds(pl.multiple_of(128 * p, 128), 128)
        normed = center * lax.rsqrt(variance + GROUP_EPS) * norm_gain[:, lanes]
        own = head_sums(q_s[p] * k_s[p] * own_weight[:, lanes]) * v_s[p]
        lin_out[:, lanes] = (normed + own).astype(BF16)
        return carry

    multiply(gather_c, near[:5], 0, True)
    run(steps_c[8])
    multiply(gather_c, near[5:], 0)
    lax.fori_loop(0, PAIRS, finish_pair, 0)

    lin_copy = pltpu.make_async_copy(lin_out, lin_hbm, out_sem.at[0])
    lin_copy.start()
    multiply(gather_c, axis_far, 0)
    run(steps_c[9])
    multiply(gather_c, side_far, 0)
    run(steps_c[10])
    multiply(gather_c, [(2, 2)], 0)
    squares = jnp.zeros((TOK, 128), F32)
    for p in range(PAIRS):
        lanes = slice(128 * p, 128 * (p + 1))
        sums = [acc[projection(i, p)[0], :, projection(i, p)[1]] for i in range(3)]
        outer, inner, signal = (t.astype(BF16).astype(F32) for t in sums)
        mixed = (inner * signal).astype(BF16).astype(F32)
        tap = taps[:, lanes].astype(F32)
        gated = outer[HALO:] * (
            tap[0:1] * pltpu.roll(mixed, 2, 0)[HALO:]
            + tap[1:2] * pltpu.roll(mixed, 1, 0)[HALO:]
            + tap[2:3] * mixed[HALO:]
        )
        q_s[p] = gated
        squares = squares + gated * gated
    column = jnp.broadcast_to(jnp.sum(squares, axis=1, keepdims=True), (TOK, 128))
    sq_s[x] = column.T[:8]
    for i, o in enumerate(OFFSETS[1:]):
        push(sq_s.at[x], sq_s.at[x], misc_send.at[SQUARES + i], misc_recv.at[SQUARES + i], at_x(o))
    gather_q.finish()
    gather_c.finish()
    for copy in tok_copies:
        copy.wait_send()
    halo_copy.wait_send()
    for i, o in enumerate(OFFSETS[1:]):
        arrived(sq_s.at[up(x, -o)], misc_recv.at[SQUARES + i])
    summed = sq_s[0] + sq_s[1] + sq_s[2] + sq_s[3]
    column = jnp.concatenate([summed] * 16, axis=0).T
    scale = lax.rsqrt(column / 2048 + NORM_EPS)
    for p in range(PAIRS):
        lanes = slice(128 * p, 128 * (p + 1))
        conv_out[:, lanes] = (q_s[p] * scale * conv_gain[:, lanes]).astype(BF16)
    conv_copy = pltpu.make_async_copy(conv_out, conv_hbm, out_sem.at[1])
    conv_copy.start()
    for p in range(PAIRS):
        arrived(st1.at[p, c], misc_send.at[CORE + p])

    @pl.when(c == 0)
    def _():
        for p in range(PAIRS):
            pl.when(y != p)(lambda p=p: arrived(st2.at[4 + p], misc_send.at[Y_SENT + p]))
        for i in range(7):
            arrived(ent_out.at[0], misc_send.at[BACK_SENT + i])

    @pl.when(c == 1)
    def _():
        for i in range(3):
            arrived(st3.at[z], misc_send.at[Z_SENT + i])
        arrived(st3.at[z], misc_send.at[TOTAL])
        arrived(pre, misc_send.at[PREFIX])

    for i in range(3):
        arrived(sq_s.at[x], misc_send.at[SQUARES + i])
    lin_copy.wait()
    conv_copy.wait()


def shards(
    tokens,
    input_norm_gain,
    query_weight,
    key_weight,
    value_weight,
    decay_first_map,
    decay_second_map,
    channel_decay_offset,
    position_decay_offset,
    extra_log_decay,
    rate_first_map,
    rate_second_map,
    channel_rate_offset,
    own_term_weight,
    head_norm_gain,
    starting_state,
    outer_gate_weight,
    inner_gate_weight,
    signal_weight,
    convolution_taps,
    convolution_gain,
):
    far = pl.BlockSpec(memory_space=pl.ANY)

    def line(v):
        return v.reshape(1, -1)

    pair = pltpu.VMEM((PAIRS, TOK, 128), F32)
    dma = pltpu.SemaphoreType.DMA
    out = jax.ShapeDtypeStruct((TOK, 512), BF16)
    return pl.pallas_call(
        kernel,
        name="mixer",
        out_shape=(out, out),
        in_specs=[far] * 21,
        out_specs=(far, far),
        scratch_shapes=[
            pltpu.VMEM((1, FEATS), F32),
            pltpu.VMEM((128, 512), BF16),
            pltpu.VMEM((1, 512), F32),
            pltpu.VMEM((1, TOK), F32),
            pltpu.VMEM((8, TOK), F32),
            pltpu.VMEM((128, 512), BF16),
            pltpu.VMEM((1, 512), F32),
            pltpu.VMEM((1, 512), F32),
            pltpu.VMEM((1, 512), F32),
            pltpu.VMEM((8, 64, 64), F32),
            pltpu.VMEM((3, 512), BF16),
            pltpu.VMEM((1, 512), F32),
            dma((12,)),
            pltpu.VMEM((TOK, 512), BF16),
            pltpu.VMEM((TOK, 512), BF16),
            dma((2,)),
            pltpu.VMEM((2, 32, 128, 768), BF16),
            pltpu.VMEM((2, 32, 128, 768), BF16),
            pltpu.VMEM((4, TOK, 1024), BF16),
            pltpu.VMEM((16, TOK + HALO, 256), BF16),
            pltpu.VMEM((FEATS, 128), BF16),
            pltpu.VMEM((FEATS, 128), BF16),
            pltpu.VMEM((2, TOK + HALO, 768), F32),
        ]
        + [pair] * 8
        + [
            pltpu.VMEM((PAIRS, 2, 2, 64, 128), BF16),
            pltpu.VMEM((8, 2, 64, 128), BF16),
            pltpu.VMEM((4, 2, 64, 128), BF16),
            pltpu.VMEM((3, 2, 64, 128), F32),
            pltpu.VMEM((PAIRS, 64, 128), BF16),
            pltpu.VMEM((4, 64, 128), BF16),
            pltpu.VMEM((4, 8, TOK), F32),
            dma((11,)),
            dma((4,)),
            dma((4,)),
            dma((2,)),
            dma((44,)),
            dma((2,)),
            dma((34,)),
            dma((56,)),
            dma((56,)),
        ],
        compiler_params=pltpu.CompilerParams(
            collective_id=0, has_side_effects=True, vmem_limit_bytes=60 * 1024 * 1024
        ),
    )(
        tokens,
        line(input_norm_gain),
        query_weight,
        key_weight,
        value_weight,
        decay_first_map,
        decay_second_map,
        line(channel_decay_offset),
        line(position_decay_offset),
        extra_log_decay.T,
        rate_first_map,
        rate_second_map,
        line(channel_rate_offset),
        line(own_term_weight),
        line(head_norm_gain),
        starting_state,
        outer_gate_weight,
        inner_gate_weight,
        signal_weight,
        convolution_taps,
        line(convolution_gain),
    )


def solution(mesh):
    torus = Mesh(mesh.devices.reshape(4, 4, 2, mesh.shape["tp"]), (*SP, "tp"))
    return jax.shard_map(
        shards,
        mesh=torus,
        in_specs=(
            P(SP, "tp"),
            P(),
            P(SP, "tp"),
            P(SP, "tp"),
            P(SP, "tp"),
            P(),
            P(None, "tp"),
            P("tp"),
            P(SP),
            P(SP, "tp"),
            P(),
            P(None, "tp"),
            P("tp"),
            P("tp"),
            P("tp"),
            P("tp", None, None),
            P(SP, "tp"),
            P(SP, "tp"),
            P(SP, "tp"),
            P(None, "tp"),
            P("tp"),
        ),
        out_specs=(P(SP, "tp"), P(SP, "tp")),
        check_vma=False,
    )
```

```python
import jax
import jax.numpy as jnp
from jax import lax
from jax.experimental import pallas as pl
from jax.experimental.pallas import tpu as pltpu
from jax.sharding import Mesh
from jax.sharding import PartitionSpec as P

SP = ("sp_0", "sp_1", "sp_2")
MESH_IDS = pl.DeviceIdType.MESH
F32 = jnp.float32
BF16 = jnp.bfloat16

DECAY_FACTOR = 0.606531
NORM_EPS = 1e-06
GROUP_EPS = 0.00064
KEY_EPS = 1e-06

TOK = 256
HALO = 16
FEATS = 4096
BLK = 64
PAIRS = 4
OFFSETS = (0, -1, 1, 2)


def dot_nn(a, b):
    return lax.dot_general(a, b, (((1,), (0,)), ((), ())), preferred_element_type=F32)


def dot_nt(a, b):
    return lax.dot_general(a, b, (((1,), (1,)), ((), ())), preferred_element_type=F32)


def parts(a):
    high = a.astype(BF16)
    return high, (a - high.astype(F32)).astype(BF16)


def dot_tn(a, b):
    return lax.dot_general(a, b, (((0,), (0,)), ((), ())), preferred_element_type=F32)


def fine(dot, a, b):
    ah, al = parts(a)
    bh, bl = parts(b)
    a_dim = 0 if dot is dot_tn else 1
    b_dim = 1 if dot is dot_nt else 0
    return dot(
        jnp.concatenate([ah, al, ah], axis=a_dim), jnp.concatenate([bh, bh, bl], axis=b_dim)
    )


def exact_left(a, b):
    high, rest = parts(b)
    mid = (b - high.astype(F32) - rest.astype(F32)).astype(BF16)
    return dot_nn(a, high) + (dot_nn(a, rest) + dot_nn(a, mid))


def iota(shape, dim):
    return lax.broadcasted_iota(jnp.int32, shape, dim)


def same_head():
    return (iota((128, 128), 0) // 64) == (iota((128, 128), 1) // 64)


def diagonal_blocks(compact):
    return jnp.where(same_head(), jnp.concatenate([compact, compact], axis=0), 0.0)


def head_sums(values):
    ones = same_head().astype(F32).astype(BF16)
    high, rest = parts(values)
    return dot_nn(high, ones) + dot_nn(rest, ones)


def spread_heads(values):
    both = jnp.concatenate([values, values], axis=0)
    return jnp.where(same_head(), both, jnp.zeros_like(both))


def pair_local(q, k, v, decay, rate, cum):
    chunks = range(TOK // BLK)
    rows = [slice(BLK * n, BLK * (n + 1)) for n in chunks]
    later, earlier = iota((BLK, 128), 0), lax.rem(iota((BLK, 128), 1), BLK)
    strict, inclusive = later > earlier, later >= earlier
    unit = k * lax.rsqrt(head_sums(k * k) + KEY_EPS)
    grow = jnp.exp(-cum)
    a = -unit * jnp.exp(cum - decay)
    b = unit * rate
    r = q * jnp.exp(cum)
    a16, r16, v16 = a.astype(BF16), r.astype(BF16), v.astype(BF16)
    b16, k16 = (b * grow).astype(BF16), (k * grow).astype(BF16)
    grams = [
        dot_nt(
            jnp.concatenate([a16[t], r16[t]], axis=0),
            jnp.concatenate([spread_heads(b16[t]), spread_heads(k16[t])], axis=0),
        )
        for t in rows
    ]
    power = [jnp.where(strict, g[:BLK, :128], 0.0).astype(BF16) for g in grams]
    writes = [jnp.where(strict, g[:BLK, 128:], 0.0).astype(BF16) for g in grams]
    reads = [
        jnp.concatenate(
            [
                jnp.where(inclusive, g[BLK:, :128], 0.0).astype(BF16),
                jnp.where(inclusive, g[BLK:, 128:], 0.0).astype(BF16),
            ],
            axis=1,
        )
        for g in grams
    ]
    values = [spread_heads(v16[t]) for t in rows]
    keys_solved = [a[t] for t in rows]
    free_solved = [dot_nn(writes[n], values[n]) for n in chunks]
    for level in range(6):
        for n in chunks:
            right = [spread_heads(keys_solved[n].astype(BF16))]
            right.append(spread_heads(free_solved[n].astype(BF16)))
            if level < 5:
                right.append(spread_heads(power[n]))
            product = dot_nn(power[n], jnp.concatenate(right, axis=1))
            keys_solved[n] = keys_solved[n] + product[:, :128]
            free_solved[n] = free_solved[n] + product[:, 128:256]
            if level < 5:
                power[n] = product[:, 256:].astype(BF16)
    read = []
    for n in chunks:
        top = [spread_heads(keys_solved[n].astype(BF16)), spread_heads(free_solved[n].astype(BF16))]
        low = [jnp.zeros((128, 128), BF16), values[n]]
        right = jnp.concatenate([jnp.concatenate(t, axis=1) for t in (top, low)], axis=0)
        read.append(dot_nn(reads[n], right))
    eye = iota((128, 128), 0) == iota((128, 128), 1)
    steps, gains = [], []
    for n in chunks:
        last = cum[BLK * (n + 1) - 1 : BLK * (n + 1), :]
        fade = jnp.exp(last - cum[rows[n]])
        b_end, k_end = b[rows[n]] * fade, k[rows[n]] * fade
        solved = jnp.concatenate([keys_solved[n], free_solved[n]], axis=1)
        both = fine(dot_tn, solved, b_end)
        step = jnp.where(same_head(), both[:128], 0.0)
        steps.append(step + jnp.where(eye, jnp.broadcast_to(jnp.exp(last), (128, 128)), 0.0))
        gain = both[128:] + fine(dot_tn, v[rows[n]], k_end)
        gains.append(jnp.where(same_head(), gain, 0.0))
    state, chain = gains[0], steps[0]
    recalled, probes = [read[0][:, 128:]], [r[rows[0]] + read[0][:, :128]]
    for n in chunks[1:]:
        carried = jnp.concatenate([state, chain], axis=0)
        both = fine(dot_nt, r[rows[n]] + read[n][:, :128], carried)
        recalled.append(read[n][:, 128:] + both[:, :128])
        probes.append(both[:, 128:])
        both = fine(dot_nn, carried, steps[n])
        state, chain = both[:128] + gains[n], both[128:]
    return (
        jnp.concatenate(recalled, axis=0),
        jnp.concatenate(probes, axis=0),
        state[:64] + state[64:],
        chain[:64] + chain[64:],
    )


def compose(earlier, later):
    both = fine(dot_nn, jnp.concatenate(earlier, axis=0), diagonal_blocks(later[0]))
    return both[:64], both[64:] + later[1]


def advance(state, later):
    return fine(dot_nn, state, diagonal_blocks(later[0])) + later[1]


def kernel(
    tokens,
    gain_hbm,
    wq,
    wk,
    wv,
    decay_first,
    decay_second_hbm,
    channel_decay_hbm,
    position_decay_hbm,
    extra_decay_hbm,
    rate_first,
    rate_second_hbm,
    channel_rate_hbm,
    own_weight_hbm,
    norm_gain_hbm,
    start_state_hbm,
    wo,
    wi,
    wsig,
    taps_hbm,
    conv_gain_hbm,
    lin_hbm,
    conv_hbm,
    gain,
    decay_second,
    channel_decay,
    position_decay,
    extra_decay,
    rate_second,
    channel_rate,
    own_weight,
    norm_gain,
    start_state,
    taps,
    conv_gain,
    small_sem,
    lin_out,
    conv_out,
    out_sem,
    gat_q,
    gat_c,
    raw,
    xn,
    low_d,
    low_r,
    acc,
    q_s,
    k_s,
    v_s,
    decay_s,
    rate_s,
    cum_s,
    rec_s,
    probe_s,
    st1,
    st2,
    st3,
    pre,
    ent,
    ent_out,
    sq_s,
    load_sem,
    tok_send,
    tok_recv,
    ici_send,
    ici_recv,
    d2d_send,
    d2d_recv,
    misc_send,
    misc_recv,
):
    z, y, c = (lax.axis_index(n) for n in SP)
    x = lax.axis_index("tp")

    def up(pos, offset):
        return lax.rem(pos + (offset + 4), 4)

    def at_x(o):
        return {"tp": up(x, o)}

    def at_y(o):
        return {"sp_1": up(y, o), "sp_2": 1 - c}

    def at_z(o):
        return {"sp_0": up(z, o), "sp_2": 1 - c}

    def along(o):
        return {"sp_0": up(z, (1 - c) * o), "sp_1": up(y, c * o)}

    sibling = {"sp_2": 1 - c}
    rank = z * 8 + y * 2 + c
    after, before = lax.rem(rank + 1, 32), lax.rem(rank + 31, 32)

    def at_rank(r):
        return {"sp_0": r // 8, "sp_1": lax.rem(r // 2, 4), "sp_2": lax.rem(r, 2)}

    def push(src, dst, send, recv, device):
        copy = pltpu.make_async_remote_copy(
            src_ref=src,
            dst_ref=dst,
            send_sem=send,
            recv_sem=recv,
            device_id=device,
            device_id_type=MESH_IDS,
        )
        copy.start()
        return copy

    def arrived(region, recv):
        pltpu.make_async_copy(region, region, recv).wait()

    loads = [pltpu.make_async_copy(tokens, raw.at[x], load_sem.at[0])]
    for n, (buf, weights) in enumerate(((gat_q, (wq, wk, wv)), (gat_c, (wo, wi, wsig)))):
        for i, (w, first, count, half, at) in enumerate(
            (
                (weights[0], 0, 512, 0, 0),
                (weights[1], 0, 256, 0, 512),
                (weights[1], 256, 256, 1, 0),
                (weights[2], 0, 512, 1, 256),
            )
        ):
            src, dst = w.at[:, pl.ds(first, count)], buf.at[half, rank, :, pl.ds(at, count)]
            loads.append(pltpu.make_async_copy(src, dst, load_sem.at[1 + 4 * n + i]))
    loads.append(pltpu.make_async_copy(decay_first, low_d, load_sem.at[9]))
    loads.append(pltpu.make_async_copy(rate_first, low_r, load_sem.at[10]))
    small = [
        (gain_hbm, gain),
        (decay_second_hbm, decay_second),
        (channel_decay_hbm, channel_decay),
        (position_decay_hbm, position_decay),
        (extra_decay_hbm, extra_decay),
        (rate_second_hbm, rate_second),
        (channel_rate_hbm, channel_rate),
        (own_weight_hbm, own_weight),
        (norm_gain_hbm, norm_gain),
        (start_state_hbm, start_state),
        (taps_hbm, taps),
        (conv_gain_hbm, conv_gain),
    ]
    small = [
        pltpu.make_async_copy(src, dst, small_sem.at[i]) for i, (src, dst) in enumerate(small)
    ]
    for load in loads + small:
        load.start()

    barrier = pltpu.get_barrier_semaphore()
    partners = [f(o) for f in (at_x, at_y, at_z) for o in OFFSETS[1:]] + [along(1), along(-1)]
    partners += [{"sp_1": up(y, o)} for o in OFFSETS[1:]]
    partners += [sibling, at_rank(after), at_rank(before)]
    for partner in partners:
        pl.semaphore_signal(barrier, inc=1, device_id=partner, device_id_type=MESH_IDS)
    pl.semaphore_wait(barrier, len(partners))

    loads[0].wait()
    tok_copies = [
        push(raw.at[x], raw.at[x], tok_send.at[0], tok_recv.at[0], at_x(1)),
        push(raw.at[x], raw.at[x], tok_send.at[1], tok_recv.at[1], at_x(-1)),
    ]

    def token_forward():
        left, right = up(x, -1), up(x, 1)
        arrived(raw.at[left], tok_recv.at[0])
        part = raw.at[left, pl.ds(0, 128)]
        tok_copies.append(push(part, part, tok_send.at[2], tok_recv.at[2], at_x(1)))
        arrived(raw.at[right], tok_recv.at[1])
        part = raw.at[right, pl.ds(128, 128)]
        tok_copies.append(push(part, part, tok_send.at[3], tok_recv.at[3], at_x(-1)))

    def token_rest():
        far = up(x, 2)
        arrived(raw.at[far, pl.ds(0, 128)], tok_recv.at[2])
        arrived(raw.at[far, pl.ds(128, 128)], tok_recv.at[3])

    class Gather:
        def __init__(self, which, buf):
            self.g, self.buf = which, buf
            self.first, self.second = 1 - c, c

        def chip(self, ahead, across):
            zz = up(z, (1 - c) * ahead + c * across)
            return zz * 4 + up(y, c * ahead + (1 - c) * across)

        def piece(self, half, ahead, across, part=None, cut=64):
            blocks = pl.ds(2 * self.chip(ahead, across), 2)
            if part is None:
                return self.buf.at[half, blocks]
            return self.buf.at[half, blocks, pl.ds(cut * part, (cut, 128 - cut)[part])]

        def cut(self, mi):
            return 48 if self.g == 1 and mi == 1 else 64

        def recv(self, index):
            return ici_recv.at[self.g * 22 + index]

        def shared(self, index):
            return d2d_recv.at[self.g * 17 + index]

        def send(self, region, direction, index):
            push(region, region, ici_send.at[self.g], self.recv(index), along(direction))

        def share(self, region, index):
            push(region, region, d2d_send.at[self.g], self.shared(index), sibling)

        def share_own(self):
            self.share(self.buf.at[self.second, rank], 0)
            self.share(self.buf.at[self.first, rank], 1)

        def start(self):
            own = self.buf.at[self.first, rank]
            self.send(own, 1, 0)
            self.send(own, -1, 2)

        def start_sibling(self):
            other = rank + 1 - 2 * c
            region = self.buf.at[self.first, other]
            arrived(region, self.shared(0))
            self.send(region, 1, 1)
            self.send(region, -1, 3)
            arrived(self.buf.at[self.second, other], self.shared(1))
            self.spread(0)

        def spread(self, mi):
            region = self.piece(self.second, 0, OFFSETS[mi])
            self.send(region, 1, 6 + 4 * mi)
            self.send(region, -1, 7 + 4 * mi)

        def first_near(self, j):
            offset = (-1, 1)[j]
            for core in range(2):
                block = 2 * self.chip(offset, 0) + (c if core == 0 else 1 - c)
                arrived(self.buf.at[self.first, block], self.recv(2 * j + core))
            self.send(self.piece(self.first, offset, 0, j), -offset, 4 + j)
            self.share(self.piece(self.first, offset, 0), 2 + j)

        def first_far(self):
            for j in range(2):
                arrived(self.piece(self.first, 2, 0, j), self.recv(4 + j))
            self.share(self.piece(self.first, 2, 0), 4)

        def second_start(self, mi):
            arrived(self.piece(self.second, 0, OFFSETS[mi]), self.shared(1 + mi))
            self.spread(mi)

        def second_near(self, mi, j):
            offset = (-1, 1)[j]
            arrived(self.piece(self.second, offset, OFFSETS[mi]), self.recv(6 + 4 * mi + j))
            part = self.piece(self.second, offset, OFFSETS[mi], j, self.cut(mi))
            self.send(part, -offset, 8 + 4 * mi + j)
            self.share(self.piece(self.second, offset, OFFSETS[mi]), 5 + 3 * mi + j)

        def second_far(self, mi):
            for j in range(2):
                part = self.piece(self.second, 2, OFFSETS[mi], j, self.cut(mi))
                arrived(part, self.recv(8 + 4 * mi + j))
            self.share(self.piece(self.second, 2, OFFSETS[mi]), 7 + 3 * mi)

        def complete(self, ahead, across):
            if across != 0:
                index = 5 + 3 * OFFSETS.index(ahead) + OFFSETS.index(across) - 1
                arrived(self.piece(self.first, ahead, across), self.shared(index))

        def steps(self):
            def near(mi):
                return [lambda j=j: self.second_near(mi, j) for j in range(2)]

            return [
                [lambda: self.first_near(0), lambda: self.first_near(1)],
                [lambda: self.second_start(1), lambda: self.second_start(2)],
                near(0),
                [self.first_far],
                [lambda: self.second_start(3)],
                near(1),
                near(2),
                [lambda: self.second_far(0)],
                near(3),
                [lambda: self.second_far(1), lambda: self.second_far(2)],
                [lambda: self.second_far(3)],
            ]

        def finish(self):
            arrived(self.buf.at[0, pl.ds(0, 30)], ici_send.at[self.g])
            arrived(self.buf.at[0], d2d_send.at[self.g])

    def run(group):
        for step in group:
            step()

    near = [(a, b) for a in (0, -1, 1) for b in (0, -1, 1)]
    axis_far = [(2, 0), (0, 2)]
    side_far = [(-1, 2), (1, 2), (2, -1), (2, 1)]

    def multiply(gather, chips, first_row, fresh=False):
        rows = pl.ds(first_row, TOK + HALO - first_row)
        for n, (ahead, across) in enumerate(chips):
            gather.complete(ahead, across)
            chip = gather.chip(ahead, across)
            left = xn[chip, rows]
            for half in range(2):
                right = gather.buf[half, pl.ds(chip * 2, 2)].reshape(256, 768)
                part = dot_nn(left, right)
                if fresh and n == 0:
                    acc[half, rows] = part
                else:
                    acc[half, rows] += part

    def projection(i, p):
        at = 512 * i + 128 * p
        return at // 768, slice(at % 768, at % 768 + 128)

    gather_q, gather_c = Gather(0, gat_q), Gather(1, gat_c)
    for load in loads[1:5]:
        load.wait()
    gather_q.share_own()
    gather_q.start()
    steps_q = gather_q.steps()
    gather_q.start_sibling()
    for n in range(3):
        run(steps_q[n])
    token_forward()
    for n in range(3, 6):
        run(steps_q[n])
    token_rest()

    for load in small:
        load.wait()
    total = jnp.zeros((TOK, 1), F32)
    for i in range(4):
        wide = raw[i].astype(F32)
        total = total + jnp.sum(wide * wide, axis=1, keepdims=True)
    inverse = lax.rsqrt(total / FEATS + NORM_EPS)
    for i in range(4):
        for j in range(4):
            lanes = slice(256 * j, 256 * (j + 1))
            wide = raw[i, :, lanes].astype(F32) * inverse * gain[:, 1024 * i + 256 * j :][:, :256]
            xn[4 * i + j, pl.ds(HALO, TOK)] = wide.astype(BF16)
    run(steps_q[6])
    run(steps_q[7])
    edge = pl.ds(TOK, HALO)
    halo_copy = push(
        xn.at[:, edge], xn.at[:, pl.ds(0, HALO)], misc_send.at[0], misc_recv.at[0], at_rank(after)
    )

    loads[9].wait()
    loads[10].wait()
    low = jnp.zeros((TOK, 256), F32)
    for i in range(16):
        rows = pl.ds(256 * i, 256)
        both = jnp.concatenate([low_d[rows], low_r[rows]], axis=1)
        low = low + dot_nn(xn[i, pl.ds(HALO, TOK)], both)
    decay_low = jnp.tanh(low[:, :128]).astype(BF16)
    rate_low = low[:, 128:].astype(BF16)
    by_position = jnp.broadcast_to(position_decay[...], (128, TOK)).T
    for p in range(PAIRS):
        lanes = slice(128 * p, 128 * (p + 1))
        logits = channel_decay[:, lanes] + dot_nn(decay_low, decay_second[:, lanes]) + by_position
        heads = [jnp.broadcast_to(extra_decay[h : h + 1], (64, TOK)) for h in (2 * p, 2 * p + 1)]
        extra = jnp.concatenate(heads, axis=0).T
        decay_s[p] = -DECAY_FACTOR * jax.nn.sigmoid(logits) + extra
        rate_s[p] = jax.nn.sigmoid(
            channel_rate[:, lanes] + dot_nn(rate_low, rate_second[:, lanes])
        )
    row, col = iota((TOK, TOK), 0), iota((TOK, TOK), 1)
    summing = (((row // BLK) == (col // BLK)) & (row >= col)).astype(F32).astype(BF16)
    for p in range(PAIRS):
        cum_s[p] = exact_left(summing, decay_s[p])

    for load in loads[5:9]:
        load.wait()
    gather_c.share_own()
    multiply(gather_q, near[:6], HALO, True)
    run(steps_q[8])
    gather_c.start()
    gather_c.start_sibling()
    multiply(gather_q, near[6:], HALO)
    multiply(gather_q, axis_far, HALO)
    run(steps_q[9])
    run(steps_q[10])
    multiply(gather_q, side_far, HALO)
    multiply(gather_q, [(2, 2)], HALO)
    body = pl.ds(HALO, TOK)
    for p in range(PAIRS):
        for i, dst in enumerate((q_s, k_s, v_s)):
            half, lanes = projection(i, p)
            dst[p] = acc[half, body, lanes].astype(BF16).astype(F32)

    steps_c = gather_c.steps()
    CORE, Y_MAPS, Z_MAPS, TOTAL, PREFIX, ENTER, SQUARES = 1, 5, 9, 13, 14, 15, 19
    Y_SENT, Z_SENT, BACK_SENT = 24, 28, 32

    def held(ref, *index):
        return ref[(*index, 0)].astype(F32), ref[(*index, 1)].astype(F32)

    def core_send(p):
        part = st1.at[p, c]
        push(part, part, misc_send.at[CORE + p], misc_recv.at[CORE + p], sibling)

    def y_send(p):
        arrived(st1.at[p, 1 - c], misc_recv.at[CORE + p])

        @pl.when((c == 0) | (p == y))
        def _():
            maps = compose(held(st1, p, 0), held(st1, p, 1))
            slot = (1 - c) * (4 + p) + c * y
            for i in range(2):
                st2[slot, i] = maps[i].astype(BF16)

        @pl.when((c == 0) & (p != y))
        def _():
            push(
                st2.at[4 + p],
                st2.at[y],
                misc_send.at[Y_SENT + p],
                misc_recv.at[Y_MAPS + y],
                {"sp_1": p, "sp_2": 1},
            )

    def z_send():
        for o in OFFSETS[1:]:
            arrived(st2.at[up(y, o)], misc_recv.at[Y_MAPS + up(y, o)])
        total_map = held(st2, 0)
        for k in range(1, 4):
            for i in range(2):
                pre[k - 1, i] = total_map[i]
            total_map = compose(total_map, held(st2, k))
        for i in range(2):
            st3[z, i] = total_map[i].astype(BF16)
        part = st3.at[z]
        for i, o in enumerate(OFFSETS[1:]):
            push(part, part, misc_send.at[Z_SENT + i], misc_recv.at[Z_MAPS + i], at_z(o))
        push(part, part, misc_send.at[TOTAL], misc_recv.at[TOTAL], sibling)
        push(pre, pre, misc_send.at[PREFIX], misc_recv.at[PREFIX], sibling)

    def back_send():
        for i, o in enumerate(OFFSETS[1:]):
            arrived(st3.at[up(z, -o)], misc_recv.at[Z_MAPS + i])
        arrived(st3.at[z], misc_recv.at[TOTAL])
        state = jnp.concatenate([start_state[2 * y], start_state[2 * y + 1]], axis=1)
        for k in range(3):
            state = jnp.where(z > k, advance(state, held(st3, k)), state)
        arrived(pre, misc_recv.at[PREFIX])
        ent_out[0] = state.astype(BF16)
        for k in range(3):
            ent_out[k + 1] = advance(state, (pre[k, 0], pre[k, 1])).astype(BF16)
        ent[y] = ent_out[y]
        for i, o in enumerate(OFFSETS[1:]):
            for core in range(2):
                push(
                    ent_out.at[up(y, o)],
                    ent.at[y],
                    misc_send.at[BACK_SENT + 2 * i + core],
                    misc_recv.at[ENTER + y],
                    {"sp_1": up(y, o), "sp_2": core},
                )
        push(ent_out.at[y], ent.at[y], misc_send.at[BACK_SENT + 6], misc_recv.at[ENTER + y], sibling)

    during = dict(enumerate(steps_c[:4]))

    def one_pair(p, carry):
        for at, group in during.items():
            pl.when(p == at)(lambda group=group: run(group))
        recalled, probe, state, chain = pair_local(
            q_s[p], k_s[p], v_s[p], decay_s[p], rate_s[p], cum_s[p]
        )
        rec_s[p] = recalled
        probe_s[p] = probe
        st1[p, c, 0] = chain.astype(BF16)
        st1[p, c, 1] = state.astype(BF16)
        core_send(p)
        pl.when(p >= 1)(lambda: y_send(p - 1))
        return carry

    lax.fori_loop(0, PAIRS, one_pair, 0)
    y_send(3)

    run(steps_c[4])
    run(steps_c[5])
    pl.when(c == 1)(z_send)
    run(steps_c[6])
    pl.when(c == 0)(back_send)
    run(steps_c[7])
    arrived(xn.at[:, pl.ds(0, HALO)], misc_recv.at[0])
    halo = xn[:, pl.ds(0, HALO)]
    xn[:, pl.ds(0, HALO)] = jnp.where(rank == 0, jnp.zeros_like(halo), halo)

    def finish_pair(p, carry):
        pl.when((c == 1) | (p != y))(lambda: arrived(ent.at[p], misc_recv.at[ENTER + p]))
        state = ent[p].astype(F32)
        state = jnp.where(c == 1, advance(state, held(st1, p, 0)), state)
        recalled = rec_s[p] + fine(dot_nt, probe_s[p], diagonal_blocks(state))
        center = recalled - head_sums(recalled) * (1.0 / 64)
        variance = head_sums(center * center) * (1.0 / 64)
        lanes = pl.ds(pl.multiple_of(128 * p, 128), 128)
        normed = center * lax.rsqrt(variance + GROUP_EPS) * norm_gain[:, lanes]
        own = head_sums(q_s[p] * k_s[p] * own_weight[:, lanes]) * v_s[p]
        lin_out[:, lanes] = (normed + own).astype(BF16)
        return carry

    multiply(gather_c, near[:5], 0, True)
    run(steps_c[8])
    multiply(gather_c, near[5:], 0)
    lax.fori_loop(0, PAIRS, finish_pair, 0)

    lin_copy = pltpu.make_async_copy(lin_out, lin_hbm, out_sem.at[0])
    lin_copy.start()
    multiply(gather_c, axis_far, 0)
    run(steps_c[9])
    run(steps_c[10])
    multiply(gather_c, side_far, 0)
    multiply(gather_c, [(2, 2)], 0)
    squares = jnp.zeros((TOK, 128), F32)
    for p in range(PAIRS):
        lanes = slice(128 * p, 128 * (p + 1))
        sums = [acc[projection(i, p)[0], :, projection(i, p)[1]] for i in range(3)]
        outer, inner, signal = (t.astype(BF16).astype(F32) for t in sums)
        mixed = (inner * signal).astype(BF16).astype(F32)
        tap = taps[:, lanes].astype(F32)
        gated = outer[HALO:] * (
            tap[0:1] * pltpu.roll(mixed, 2, 0)[HALO:]
            + tap[1:2] * pltpu.roll(mixed, 1, 0)[HALO:]
            + tap[2:3] * mixed[HALO:]
        )
        q_s[p] = gated
        squares = squares + gated * gated
    column = jnp.broadcast_to(jnp.sum(squares, axis=1, keepdims=True), (TOK, 128))
    sq_s[x] = column.T[:8]
    for i, o in enumerate(OFFSETS[1:]):
        push(sq_s.at[x], sq_s.at[x], misc_send.at[SQUARES + i], misc_recv.at[SQUARES + i], at_x(o))
    gather_q.finish()
    gather_c.finish()
    for copy in tok_copies:
        copy.wait_send()
    halo_copy.wait_send()
    for i, o in enumerate(OFFSETS[1:]):
        arrived(sq_s.at[up(x, -o)], misc_recv.at[SQUARES + i])
    summed = sq_s[0] + sq_s[1] + sq_s[2] + sq_s[3]
    column = jnp.concatenate([summed] * 16, axis=0).T
    scale = lax.rsqrt(column / 2048 + NORM_EPS)
    for p in range(PAIRS):
        lanes = slice(128 * p, 128 * (p + 1))
        conv_out[:, lanes] = (q_s[p] * scale * conv_gain[:, lanes]).astype(BF16)
    conv_copy = pltpu.make_async_copy(conv_out, conv_hbm, out_sem.at[1])
    conv_copy.start()
    for p in range(PAIRS):
        arrived(st1.at[p, c], misc_send.at[CORE + p])

    @pl.when(c == 0)
    def _():
        for p in range(PAIRS):
            pl.when(y != p)(lambda p=p: arrived(st2.at[4 + p], misc_send.at[Y_SENT + p]))
        for i in range(7):
            arrived(ent_out.at[0], misc_send.at[BACK_SENT + i])

    @pl.when(c == 1)
    def _():
        for i in range(3):
            arrived(st3.at[z], misc_send.at[Z_SENT + i])
        arrived(st3.at[z], misc_send.at[TOTAL])
        arrived(pre, misc_send.at[PREFIX])

    for i in range(3):
        arrived(sq_s.at[x], misc_send.at[SQUARES + i])
    lin_copy.wait()
    conv_copy.wait()


def shards(
    tokens,
    input_norm_gain,
    query_weight,
    key_weight,
    value_weight,
    decay_first_map,
    decay_second_map,
    channel_decay_offset,
    position_decay_offset,
    extra_log_decay,
    rate_first_map,
    rate_second_map,
    channel_rate_offset,
    own_term_weight,
    head_norm_gain,
    starting_state,
    outer_gate_weight,
    inner_gate_weight,
    signal_weight,
    convolution_taps,
    convolution_gain,
):
    far = pl.BlockSpec(memory_space=pl.ANY)

    def line(v):
        return v.reshape(1, -1)

    pair = pltpu.VMEM((PAIRS, TOK, 128), F32)
    dma = pltpu.SemaphoreType.DMA
    out = jax.ShapeDtypeStruct((TOK, 512), BF16)
    return pl.pallas_call(
        kernel,
        name="mixer",
        out_shape=(out, out),
        in_specs=[far] * 21,
        out_specs=(far, far),
        scratch_shapes=[
            pltpu.VMEM((1, FEATS), F32),
            pltpu.VMEM((128, 512), BF16),
            pltpu.VMEM((1, 512), F32),
            pltpu.VMEM((1, TOK), F32),
            pltpu.VMEM((8, TOK), F32),
            pltpu.VMEM((128, 512), BF16),
            pltpu.VMEM((1, 512), F32),
            pltpu.VMEM((1, 512), F32),
            pltpu.VMEM((1, 512), F32),
            pltpu.VMEM((8, 64, 64), F32),
            pltpu.VMEM((3, 512), BF16),
            pltpu.VMEM((1, 512), F32),
            dma((12,)),
            pltpu.VMEM((TOK, 512), BF16),
            pltpu.VMEM((TOK, 512), BF16),
            dma((2,)),
            pltpu.VMEM((2, 32, 128, 768), BF16),
            pltpu.VMEM((2, 32, 128, 768), BF16),
            pltpu.VMEM((4, TOK, 1024), BF16),
            pltpu.VMEM((16, TOK + HALO, 256), BF16),
            pltpu.VMEM((FEATS, 128), BF16),
            pltpu.VMEM((FEATS, 128), BF16),
            pltpu.VMEM((2, TOK + HALO, 768), F32),
        ]
        + [pair] * 8
        + [
            pltpu.VMEM((PAIRS, 2, 2, 64, 128), BF16),
            pltpu.VMEM((8, 2, 64, 128), BF16),
            pltpu.VMEM((4, 2, 64, 128), BF16),
            pltpu.VMEM((3, 2, 64, 128), F32),
            pltpu.VMEM((PAIRS, 64, 128), BF16),
            pltpu.VMEM((4, 64, 128), BF16),
            pltpu.VMEM((4, 8, TOK), F32),
            dma((11,)),
            dma((4,)),
            dma((4,)),
            dma((2,)),
            dma((44,)),
            dma((2,)),
            dma((34,)),
            dma((56,)),
            dma((56,)),
        ],
        compiler_params=pltpu.CompilerParams(
            collective_id=0, has_side_effects=True, vmem_limit_bytes=60 * 1024 * 1024
        ),
    )(
        tokens,
        line(input_norm_gain),
        query_weight,
        key_weight,
        value_weight,
        decay_first_map,
        decay_second_map,
        line(channel_decay_offset),
        line(position_decay_offset),
        extra_log_decay.T,
        rate_first_map,
        rate_second_map,
        line(channel_rate_offset),
        line(own_term_weight),
        line(head_norm_gain),
        starting_state,
        outer_gate_weight,
        inner_gate_weight,
        signal_weight,
        convolution_taps,
        line(convolution_gain),
    )


def solution(mesh):
    torus = Mesh(mesh.devices.reshape(4, 4, 2, mesh.shape["tp"]), (*SP, "tp"))
    return jax.shard_map(
        shards,
        mesh=torus,
        in_specs=(
            P(SP, "tp"),
            P(),
            P(SP, "tp"),
            P(SP, "tp"),
            P(SP, "tp"),
            P(),
            P(None, "tp"),
            P("tp"),
            P(SP),
            P(SP, "tp"),
            P(),
            P(None, "tp"),
            P("tp"),
            P("tp"),
            P("tp"),
            P("tp", None, None),
            P(SP, "tp"),
            P(SP, "tp"),
            P(SP, "tp"),
            P(None, "tp"),
            P("tp"),
        ),
        out_specs=(P(SP, "tp"), P(SP, "tp")),
        check_vma=False,
    )
```

```python
import jax
import jax.numpy as jnp
from jax import lax
from jax.experimental import pallas as pl
from jax.experimental.pallas import tpu as pltpu
from jax.sharding import Mesh
from jax.sharding import PartitionSpec as P

SP = ("sp_0", "sp_1", "sp_2")
MESH_IDS = pl.DeviceIdType.MESH
F32 = jnp.float32
BF16 = jnp.bfloat16

DECAY_FACTOR = 0.606531
NORM_EPS = 1e-06
GROUP_EPS = 0.00064
KEY_EPS = 1e-06

TOK = 256
HALO = 16
FEATS = 4096
BLK = 64
PAIRS = 4
OFFSETS = (0, -1, 1, 2)


def dot_nn(a, b):
    return lax.dot_general(a, b, (((1,), (0,)), ((), ())), preferred_element_type=F32)


def dot_nt(a, b):
    return lax.dot_general(a, b, (((1,), (1,)), ((), ())), preferred_element_type=F32)


def parts(a):
    high = a.astype(BF16)
    return high, (a - high.astype(F32)).astype(BF16)


def dot_tn(a, b):
    return lax.dot_general(a, b, (((0,), (0,)), ((), ())), preferred_element_type=F32)


def fine(dot, a, b):
    ah, al = parts(a)
    bh, bl = parts(b)
    a_dim = 0 if dot is dot_tn else 1
    b_dim = 1 if dot is dot_nt else 0
    return dot(
        jnp.concatenate([ah, al, ah], axis=a_dim), jnp.concatenate([bh, bh, bl], axis=b_dim)
    )


def exact_left(a, b):
    high, rest = parts(b)
    mid = (b - high.astype(F32) - rest.astype(F32)).astype(BF16)
    return dot_nn(a, high) + (dot_nn(a, rest) + dot_nn(a, mid))


def iota(shape, dim):
    return lax.broadcasted_iota(jnp.int32, shape, dim)


def same_head():
    return (iota((128, 128), 0) // 64) == (iota((128, 128), 1) // 64)


def diagonal_blocks(compact):
    return jnp.where(same_head(), jnp.concatenate([compact, compact], axis=0), 0.0)


def head_sums(values):
    ones = same_head().astype(F32).astype(BF16)
    high, rest = parts(values)
    return dot_nn(high, ones) + dot_nn(rest, ones)


def spread_heads(values):
    both = jnp.concatenate([values, values], axis=0)
    return jnp.where(same_head(), both, jnp.zeros_like(both))


def pair_local(q, k, v, decay, rate, cum):
    chunks = range(TOK // BLK)
    rows = [slice(BLK * n, BLK * (n + 1)) for n in chunks]
    later, earlier = iota((BLK, 128), 0), lax.rem(iota((BLK, 128), 1), BLK)
    strict, inclusive = later > earlier, later >= earlier
    unit = k * lax.rsqrt(head_sums(k * k) + KEY_EPS)
    grow = jnp.exp(-cum)
    a = -unit * jnp.exp(cum - decay)
    b = unit * rate
    r = q * jnp.exp(cum)
    a16, r16, v16 = a.astype(BF16), r.astype(BF16), v.astype(BF16)
    b16, k16 = (b * grow).astype(BF16), (k * grow).astype(BF16)
    grams = [
        dot_nt(
            jnp.concatenate([a16[t], r16[t]], axis=0),
            jnp.concatenate([spread_heads(b16[t]), spread_heads(k16[t])], axis=0),
        )
        for t in rows
    ]
    power = [jnp.where(strict, g[:BLK, :128], 0.0).astype(BF16) for g in grams]
    writes = [jnp.where(strict, g[:BLK, 128:], 0.0).astype(BF16) for g in grams]
    reads = [
        jnp.concatenate(
            [
                jnp.where(inclusive, g[BLK:, :128], 0.0).astype(BF16),
                jnp.where(inclusive, g[BLK:, 128:], 0.0).astype(BF16),
            ],
            axis=1,
        )
        for g in grams
    ]
    values = [spread_heads(v16[t]) for t in rows]
    keys_solved = [a[t] for t in rows]
    free_solved = [dot_nn(writes[n], values[n]) for n in chunks]
    for level in range(6):
        for n in chunks:
            right = [spread_heads(keys_solved[n].astype(BF16))]
            right.append(spread_heads(free_solved[n].astype(BF16)))
            if level < 5:
                right.append(spread_heads(power[n]))
            product = dot_nn(power[n], jnp.concatenate(right, axis=1))
            keys_solved[n] = keys_solved[n] + product[:, :128]
            free_solved[n] = free_solved[n] + product[:, 128:256]
            if level < 5:
                power[n] = product[:, 256:].astype(BF16)
    read = []
    for n in chunks:
        top = [spread_heads(keys_solved[n].astype(BF16)), spread_heads(free_solved[n].astype(BF16))]
        low = [jnp.zeros((128, 128), BF16), values[n]]
        right = jnp.concatenate([jnp.concatenate(t, axis=1) for t in (top, low)], axis=0)
        read.append(dot_nn(reads[n], right))
    eye = iota((128, 128), 0) == iota((128, 128), 1)
    steps, gains = [], []
    for n in chunks:
        last = cum[BLK * (n + 1) - 1 : BLK * (n + 1), :]
        fade = jnp.exp(last - cum[rows[n]])
        b_end, k_end = b[rows[n]] * fade, k[rows[n]] * fade
        solved = jnp.concatenate([keys_solved[n], free_solved[n]], axis=1)
        both = fine(dot_tn, solved, b_end)
        step = jnp.where(same_head(), both[:128], 0.0)
        steps.append(step + jnp.where(eye, jnp.broadcast_to(jnp.exp(last), (128, 128)), 0.0))
        gain = both[128:] + fine(dot_tn, v[rows[n]], k_end)
        gains.append(jnp.where(same_head(), gain, 0.0))
    state, chain = gains[0], steps[0]
    recalled, probes = [read[0][:, 128:]], [r[rows[0]] + read[0][:, :128]]
    for n in chunks[1:]:
        carried = jnp.concatenate([state, chain], axis=0)
        both = fine(dot_nt, r[rows[n]] + read[n][:, :128], carried)
        recalled.append(read[n][:, 128:] + both[:, :128])
        probes.append(both[:, 128:])
        both = fine(dot_nn, carried, steps[n])
        state, chain = both[:128] + gains[n], both[128:]
    return (
        jnp.concatenate(recalled, axis=0),
        jnp.concatenate(probes, axis=0),
        state[:64] + state[64:],
        chain[:64] + chain[64:],
    )


def compose(earlier, later):
    both = fine(dot_nn, jnp.concatenate(earlier, axis=0), diagonal_blocks(later[0]))
    return both[:64], both[64:] + later[1]


def advance(state, later):
    return fine(dot_nn, state, diagonal_blocks(later[0])) + later[1]


def kernel(
    tokens,
    gain_hbm,
    wq,
    wk,
    wv,
    decay_first,
    decay_second_hbm,
    channel_decay_hbm,
    position_decay_hbm,
    extra_decay_hbm,
    rate_first,
    rate_second_hbm,
    channel_rate_hbm,
    own_weight_hbm,
    norm_gain_hbm,
    start_state_hbm,
    wo,
    wi,
    wsig,
    taps_hbm,
    lin_hbm,
    gated_hbm,
    total_hbm,
    gain,
    decay_second,
    channel_decay,
    position_decay,
    extra_decay,
    rate_second,
    channel_rate,
    own_weight,
    norm_gain,
    start_state,
    taps,
    small_sem,
    lin_out,
    total_out,
    out_sem,
    gat_q,
    gat_c,
    raw,
    xn,
    low_d,
    low_r,
    acc,
    q_s,
    k_s,
    v_s,
    decay_s,
    rate_s,
    cum_s,
    rec_s,
    probe_s,
    st1,
    st2,
    st3,
    pre,
    ent,
    ent_out,
    sq_s,
    load_sem,
    tok_send,
    tok_recv,
    ici_send,
    ici_recv,
    d2d_send,
    d2d_recv,
    misc_send,
    misc_recv,
):
    z, y, c = (lax.axis_index(n) for n in SP)
    x = lax.axis_index("tp")

    def up(pos, offset):
        return lax.rem(pos + (offset + 4), 4)

    def at_x(o):
        return {"tp": up(x, o)}

    def at_y(o):
        return {"sp_1": up(y, o), "sp_2": 1 - c}

    def at_z(o):
        return {"sp_0": up(z, o), "sp_2": 1 - c}

    def along(o):
        return {"sp_0": up(z, (1 - c) * o), "sp_1": up(y, c * o)}

    sibling = {"sp_2": 1 - c}
    rank = z * 8 + y * 2 + c
    after, before = lax.rem(rank + 1, 32), lax.rem(rank + 31, 32)

    def at_rank(r):
        return {"sp_0": r // 8, "sp_1": lax.rem(r // 2, 4), "sp_2": lax.rem(r, 2)}

    def push(src, dst, send, recv, device):
        copy = pltpu.make_async_remote_copy(
            src_ref=src,
            dst_ref=dst,
            send_sem=send,
            recv_sem=recv,
            device_id=device,
            device_id_type=MESH_IDS,
        )
        copy.start()
        return copy

    def arrived(region, recv):
        pltpu.make_async_copy(region, region, recv).wait()

    loads = [pltpu.make_async_copy(tokens, raw.at[x], load_sem.at[0])]
    for n, (buf, weights) in enumerate(((gat_q, (wq, wk, wv)), (gat_c, (wo, wi, wsig)))):
        for i, (w, first, count, half, at) in enumerate(
            (
                (weights[0], 0, 512, 0, 0),
                (weights[1], 0, 256, 0, 512),
                (weights[1], 256, 256, 1, 0),
                (weights[2], 0, 512, 1, 256),
            )
        ):
            src, dst = w.at[:, pl.ds(first, count)], buf.at[half, rank, :, pl.ds(at, count)]
            loads.append(pltpu.make_async_copy(src, dst, load_sem.at[1 + 4 * n + i]))
    loads.append(pltpu.make_async_copy(decay_first, low_d, load_sem.at[9]))
    loads.append(pltpu.make_async_copy(rate_first, low_r, load_sem.at[10]))
    small = [
        (gain_hbm, gain),
        (decay_second_hbm, decay_second),
        (channel_decay_hbm, channel_decay),
        (position_decay_hbm, position_decay),
        (extra_decay_hbm, extra_decay),
        (rate_second_hbm, rate_second),
        (channel_rate_hbm, channel_rate),
        (own_weight_hbm, own_weight),
        (norm_gain_hbm, norm_gain),
        (start_state_hbm, start_state),
        (taps_hbm, taps),
    ]
    small = [
        pltpu.make_async_copy(src, dst, small_sem.at[i]) for i, (src, dst) in enumerate(small)
    ]
    for load in loads + small:
        load.start()

    barrier = pltpu.get_barrier_semaphore()
    partners = [f(o) for f in (at_x, at_y, at_z) for o in OFFSETS[1:]] + [along(1), along(-1)]
    partners += [{"sp_1": up(y, o)} for o in OFFSETS[1:]]
    partners += [sibling, at_rank(after), at_rank(before)]
    for partner in partners:
        pl.semaphore_signal(barrier, inc=1, device_id=partner, device_id_type=MESH_IDS)
    pl.semaphore_wait(barrier, len(partners))

    loads[0].wait()
    tok_copies = [
        push(raw.at[x], raw.at[x], tok_send.at[0], tok_recv.at[0], at_x(1)),
        push(raw.at[x], raw.at[x], tok_send.at[1], tok_recv.at[1], at_x(-1)),
    ]

    def token_forward():
        left, right = up(x, -1), up(x, 1)
        arrived(raw.at[left], tok_recv.at[0])
        part = raw.at[left, pl.ds(0, 128)]
        tok_copies.append(push(part, part, tok_send.at[2], tok_recv.at[2], at_x(1)))
        arrived(raw.at[right], tok_recv.at[1])
        part = raw.at[right, pl.ds(128, 128)]
        tok_copies.append(push(part, part, tok_send.at[3], tok_recv.at[3], at_x(-1)))

    def token_rest():
        far = up(x, 2)
        arrived(raw.at[far, pl.ds(0, 128)], tok_recv.at[2])
        arrived(raw.at[far, pl.ds(128, 128)], tok_recv.at[3])

    class Gather:
        def __init__(self, which, buf):
            self.g, self.buf = which, buf
            self.first, self.second = 1 - c, c

        def chip(self, ahead, across):
            zz = up(z, (1 - c) * ahead + c * across)
            return zz * 4 + up(y, c * ahead + (1 - c) * across)

        def piece(self, half, ahead, across, part=None, cut=64):
            blocks = pl.ds(2 * self.chip(ahead, across), 2)
            if part is None:
                return self.buf.at[half, blocks]
            return self.buf.at[half, blocks, pl.ds(cut * part, (cut, 128 - cut)[part])]

        def cut(self, mi):
            return 48 if self.g == 1 and mi == 1 else 64

        def recv(self, index):
            return ici_recv.at[self.g * 22 + index]

        def shared(self, index):
            return d2d_recv.at[self.g * 18 + index]

        def send(self, region, direction, index):
            push(region, region, ici_send.at[self.g], self.recv(index), along(direction))

        def share(self, region, index):
            push(region, region, d2d_send.at[self.g], self.shared(index), sibling)

        def share_own(self):
            self.share(self.buf.at[self.second, rank], 0)
            self.share(self.buf.at[self.first, rank], 1)

        def start(self):
            own = self.buf.at[self.first, rank]
            self.send(own, 1, 0)
            self.send(own, -1, 2)

        def start_sibling(self):
            other = rank + 1 - 2 * c
            region = self.buf.at[self.first, other]
            arrived(region, self.shared(0))
            self.send(region, 1, 1)
            self.send(region, -1, 3)
            arrived(self.buf.at[self.second, other], self.shared(1))
            self.spread(0)

        def spread(self, mi):
            region = self.piece(self.second, 0, OFFSETS[mi])
            self.send(region, 1, 6 + 4 * mi)
            self.send(region, -1, 7 + 4 * mi)

        def first_near(self, j):
            offset = (-1, 1)[j]
            for core in range(2):
                block = 2 * self.chip(offset, 0) + (c if core == 0 else 1 - c)
                arrived(self.buf.at[self.first, block], self.recv(2 * j + core))
            self.send(self.piece(self.first, offset, 0, j), -offset, 4 + j)
            self.share(self.piece(self.first, offset, 0), 2 + j)

        def first_far(self):
            for j in range(2):
                arrived(self.piece(self.first, 2, 0, j), self.recv(4 + j))
            self.share(self.piece(self.first, 2, 0), 4)

        def second_start(self, mi):
            arrived(self.piece(self.second, 0, OFFSETS[mi]), self.shared(1 + mi))
            self.spread(mi)

        def second_near(self, mi, j):
            offset = (-1, 1)[j]
            arrived(self.piece(self.second, offset, OFFSETS[mi]), self.recv(6 + 4 * mi + j))
            part = self.piece(self.second, offset, OFFSETS[mi], j, self.cut(mi))
            self.send(part, -offset, 8 + 4 * mi + j)
            self.share(self.piece(self.second, offset, OFFSETS[mi]), 5 + 3 * mi + j)

        def second_far(self, mi):
            for j in range(2):
                part = self.piece(self.second, 2, OFFSETS[mi], j, self.cut(mi))
                arrived(part, self.recv(8 + 4 * mi + j))
                if mi == 3:
                    self.share(part, 16 + j)
            if mi < 3:
                self.share(self.piece(self.second, 2, OFFSETS[mi]), 7 + 3 * mi)

        def complete(self, ahead, across):
            if (ahead, across) == (2, 2):
                for j in range(2):
                    arrived(self.piece(self.first, 2, 2, j), self.shared(16 + j))
            elif across != 0:
                index = 5 + 3 * OFFSETS.index(ahead) + OFFSETS.index(across) - 1
                arrived(self.piece(self.first, ahead, across), self.shared(index))

        def steps(self):
            def near(mi):
                return [lambda j=j: self.second_near(mi, j) for j in range(2)]

            return [
                [lambda: self.first_near(0), lambda: self.first_near(1)],
                [lambda: self.second_start(1), lambda: self.second_start(2)],
                near(0),
                [self.first_far],
                [lambda: self.second_start(3)],
                near(1),
                near(2),
                [lambda: self.second_far(0)],
                near(3),
                [lambda: self.second_far(1)],
                [lambda: self.second_far(2)],
                [lambda: self.second_far(3)],
            ]

        def finish(self):
            arrived(self.buf.at[0, pl.ds(0, 30)], ici_send.at[self.g])
            arrived(self.buf.at[0], d2d_send.at[self.g])

    def run(group):
        for step in group:
            step()

    near = [(a, b) for a in (0, -1, 1) for b in (0, -1, 1)]
    axis_far = [(2, 0), (0, 2)]
    side_far = [(-1, 2), (1, 2), (2, -1), (2, 1)]

    def multiply(gather, chips, first_row, fresh=False):
        rows = pl.ds(first_row, TOK + HALO - first_row)
        for n, (ahead, across) in enumerate(chips):
            gather.complete(ahead, across)
            chip = gather.chip(ahead, across)
            left = xn[chip, rows]
            for half in range(2):
                right = gather.buf[half, pl.ds(chip * 2, 2)].reshape(256, 768)
                part = dot_nn(left, right)
                if fresh and n == 0:
                    acc[half, rows] = part
                else:
                    acc[half, rows] += part

    def projection(i, p):
        at = 512 * i + 128 * p
        return at // 768, slice(at % 768, at % 768 + 128)

    gather_q, gather_c = Gather(0, gat_q), Gather(1, gat_c)
    for load in loads[1:5]:
        load.wait()
    gather_q.share_own()
    gather_q.start()
    steps_q = gather_q.steps()
    gather_q.start_sibling()
    for n in range(3):
        run(steps_q[n])
    token_forward()
    for n in range(3, 6):
        run(steps_q[n])
    token_rest()

    for load in small:
        load.wait()
    total = jnp.zeros((TOK, 1), F32)
    for i in range(4):
        wide = raw[i].astype(F32)
        total = total + jnp.sum(wide * wide, axis=1, keepdims=True)
    inverse = lax.rsqrt(total / FEATS + NORM_EPS)
    for i in range(4):
        for j in range(4):
            lanes = slice(256 * j, 256 * (j + 1))
            wide = raw[i, :, lanes].astype(F32) * inverse * gain[:, 1024 * i + 256 * j :][:, :256]
            xn[4 * i + j, pl.ds(HALO, TOK)] = wide.astype(BF16)
    run(steps_q[6])
    run(steps_q[7])
    edge = pl.ds(TOK, HALO)
    halo_copy = push(
        xn.at[:, edge], xn.at[:, pl.ds(0, HALO)], misc_send.at[0], misc_recv.at[0], at_rank(after)
    )

    loads[9].wait()
    loads[10].wait()
    low = jnp.zeros((TOK, 256), F32)
    for i in range(16):
        rows = pl.ds(256 * i, 256)
        both = jnp.concatenate([low_d[rows], low_r[rows]], axis=1)
        low = low + dot_nn(xn[i, pl.ds(HALO, TOK)], both)
    decay_low = jnp.tanh(low[:, :128]).astype(BF16)
    rate_low = low[:, 128:].astype(BF16)
    by_position = jnp.broadcast_to(position_decay[...], (128, TOK)).T
    for p in range(PAIRS):
        lanes = slice(128 * p, 128 * (p + 1))
        logits = channel_decay[:, lanes] + dot_nn(decay_low, decay_second[:, lanes]) + by_position
        heads = [jnp.broadcast_to(extra_decay[h : h + 1], (64, TOK)) for h in (2 * p, 2 * p + 1)]
        extra = jnp.concatenate(heads, axis=0).T
        decay_s[p] = -DECAY_FACTOR * jax.nn.sigmoid(logits) + extra
        rate_s[p] = jax.nn.sigmoid(
            channel_rate[:, lanes] + dot_nn(rate_low, rate_second[:, lanes])
        )
    row, col = iota((TOK, TOK), 0), iota((TOK, TOK), 1)
    summing = (((row // BLK) == (col // BLK)) & (row >= col)).astype(F32).astype(BF16)
    for p in range(PAIRS):
        cum_s[p] = exact_left(summing, decay_s[p])

    for load in loads[5:9]:
        load.wait()
    gather_c.share_own()
    multiply(gather_q, near[:6], HALO, True)
    run(steps_q[8])
    gather_c.start()
    gather_c.start_sibling()
    multiply(gather_q, near[6:], HALO)
    multiply(gather_q, axis_far, HALO)
    run(steps_q[9])
    run(steps_q[10])
    multiply(gather_q, side_far[2:], HALO)
    run(steps_q[11])
    multiply(gather_q, side_far[:2], HALO)
    multiply(gather_q, [(2, 2)], HALO)
    body = pl.ds(HALO, TOK)
    for p in range(PAIRS):
        for i, dst in enumerate((q_s, k_s, v_s)):
            half, lanes = projection(i, p)
            dst[p] = acc[half, body, lanes].astype(BF16).astype(F32)

    steps_c = gather_c.steps()
    CORE, Y_MAPS, Z_MAPS, TOTAL, PREFIX, ENTER, SQUARES = 1, 5, 9, 13, 14, 15, 19
    Y_SENT, Z_SENT, BACK_SENT = 24, 28, 32

    def held(ref, *index):
        return ref[(*index, 0)].astype(F32), ref[(*index, 1)].astype(F32)

    def core_send(p):
        part = st1.at[p, c]
        push(part, part, misc_send.at[CORE + p], misc_recv.at[CORE + p], sibling)

    def y_send(p):
        arrived(st1.at[p, 1 - c], misc_recv.at[CORE + p])

        @pl.when((c == 0) | (p == y))
        def _():
            maps = compose(held(st1, p, 0), held(st1, p, 1))
            slot = (1 - c) * (4 + p) + c * y
            for i in range(2):
                st2[slot, i] = maps[i].astype(BF16)

        @pl.when((c == 0) & (p != y))
        def _():
            push(
                st2.at[4 + p],
                st2.at[y],
                misc_send.at[Y_SENT + p],
                misc_recv.at[Y_MAPS + y],
                {"sp_1": p, "sp_2": 1},
            )

    def z_send():
        for o in OFFSETS[1:]:
            arrived(st2.at[up(y, o)], misc_recv.at[Y_MAPS + up(y, o)])
        total_map = held(st2, 0)
        for k in range(1, 4):
            for i in range(2):
                pre[k - 1, i] = total_map[i]
            total_map = compose(total_map, held(st2, k))
        for i in range(2):
            st3[z, i] = total_map[i].astype(BF16)
        part = st3.at[z]
        for i, o in enumerate(OFFSETS[1:]):
            push(part, part, misc_send.at[Z_SENT + i], misc_recv.at[Z_MAPS + i], at_z(o))
        push(part, part, misc_send.at[TOTAL], misc_recv.at[TOTAL], sibling)
        push(pre, pre, misc_send.at[PREFIX], misc_recv.at[PREFIX], sibling)

    def back_send():
        for i, o in enumerate(OFFSETS[1:]):
            arrived(st3.at[up(z, -o)], misc_recv.at[Z_MAPS + i])
        arrived(st3.at[z], misc_recv.at[TOTAL])
        state = jnp.concatenate([start_state[2 * y], start_state[2 * y + 1]], axis=1)
        for k in range(3):
            state = jnp.where(z > k, advance(state, held(st3, k)), state)
        arrived(pre, misc_recv.at[PREFIX])
        ent_out[0] = state.astype(BF16)
        for k in range(3):
            ent_out[k + 1] = advance(state, (pre[k, 0], pre[k, 1])).astype(BF16)
        ent[y] = ent_out[y]
        for i, o in enumerate(OFFSETS[1:]):
            for core in range(2):
                push(
                    ent_out.at[up(y, o)],
                    ent.at[y],
                    misc_send.at[BACK_SENT + 2 * i + core],
                    misc_recv.at[ENTER + y],
                    {"sp_1": up(y, o), "sp_2": core},
                )
        push(ent_out.at[y], ent.at[y], misc_send.at[BACK_SENT + 6], misc_recv.at[ENTER + y], sibling)

    during = dict(enumerate(steps_c[:4]))

    def one_pair(p, carry):
        for at, group in during.items():
            pl.when(p == at)(lambda group=group: run(group))
        recalled, probe, state, chain = pair_local(
            q_s[p], k_s[p], v_s[p], decay_s[p], rate_s[p], cum_s[p]
        )
        rec_s[p] = recalled
        probe_s[p] = probe
        st1[p, c, 0] = chain.astype(BF16)
        st1[p, c, 1] = state.astype(BF16)
        core_send(p)
        pl.when(p >= 1)(lambda: y_send(p - 1))
        return carry

    lax.fori_loop(0, PAIRS, one_pair, 0)
    y_send(3)

    run(steps_c[4])
    run(steps_c[5])
    pl.when(c == 1)(z_send)
    run(steps_c[6])
    pl.when(c == 0)(back_send)
    run(steps_c[7])
    arrived(xn.at[:, pl.ds(0, HALO)], misc_recv.at[0])
    halo = xn[:, pl.ds(0, HALO)]
    xn[:, pl.ds(0, HALO)] = jnp.where(rank == 0, jnp.zeros_like(halo), halo)

    def finish_pair(p, carry):
        pl.when((c == 1) | (p != y))(lambda: arrived(ent.at[p], misc_recv.at[ENTER + p]))
        state = ent[p].astype(F32)
        state = jnp.where(c == 1, advance(state, held(st1, p, 0)), state)
        recalled = rec_s[p] + fine(dot_nt, probe_s[p], diagonal_blocks(state))
        center = recalled - head_sums(recalled) * (1.0 / 64)
        variance = head_sums(center * center) * (1.0 / 64)
        lanes = pl.ds(pl.multiple_of(128 * p, 128), 128)
        normed = center * lax.rsqrt(variance + GROUP_EPS) * norm_gain[:, lanes]
        own = head_sums(q_s[p] * k_s[p] * own_weight[:, lanes]) * v_s[p]
        lin_out[:, lanes] = (normed + own).astype(BF16)
        return carry

    multiply(gather_c, near, 0, True)
    lax.fori_loop(0, 2, finish_pair, 0)
    run(steps_c[8])
    lax.fori_loop(2, PAIRS, finish_pair, 0)
    lin_copy = pltpu.make_async_copy(lin_out, lin_hbm, out_sem.at[0])
    lin_copy.start()
    multiply(gather_c, axis_far, 0)
    run(steps_c[9])
    run(steps_c[10])
    multiply(gather_c, side_far[2:], 0)
    run(steps_c[11])
    multiply(gather_c, side_far[:2], 0)
    multiply(gather_c, [(2, 2)], 0)
    squares = jnp.zeros((TOK, 128), F32)
    for p in range(PAIRS):
        lanes = slice(128 * p, 128 * (p + 1))
        sums = [acc[projection(i, p)[0], :, projection(i, p)[1]] for i in range(3)]
        outer, inner, signal = (t.astype(BF16).astype(F32) for t in sums)
        mixed = (inner * signal).astype(BF16).astype(F32)
        tap = taps[:, lanes].astype(F32)
        gated = outer[HALO:] * (
            tap[0:1] * pltpu.roll(mixed, 2, 0)[HALO:]
            + tap[1:2] * pltpu.roll(mixed, 1, 0)[HALO:]
            + tap[2:3] * mixed[HALO:]
        )
        q_s[p] = gated
        squares = squares + gated * gated
    column = jnp.broadcast_to(jnp.sum(squares, axis=1, keepdims=True), (TOK, 128))
    gated_copy = pltpu.make_async_copy(q_s, gated_hbm, out_sem.at[2])
    sq_s[x] = column.T[:8]
    for i, o in enumerate(OFFSETS[1:]):
        push(sq_s.at[x], sq_s.at[x], misc_send.at[SQUARES + i], misc_recv.at[SQUARES + i], at_x(o))
    gated_copy.start()
    gather_q.finish()
    gather_c.finish()
    for copy in tok_copies:
        copy.wait_send()
    halo_copy.wait_send()
    for i, o in enumerate(OFFSETS[1:]):
        arrived(sq_s.at[up(x, -o)], misc_recv.at[SQUARES + i])
    total_out[...] = sq_s[0] + sq_s[1] + sq_s[2] + sq_s[3]
    total_copy = pltpu.make_async_copy(total_out, total_hbm, out_sem.at[1])
    total_copy.start()
    for p in range(PAIRS):
        arrived(st1.at[p, c], misc_send.at[CORE + p])

    @pl.when(c == 0)
    def _():
        for p in range(PAIRS):
            pl.when(y != p)(lambda p=p: arrived(st2.at[4 + p], misc_send.at[Y_SENT + p]))
        for i in range(7):
            arrived(ent_out.at[0], misc_send.at[BACK_SENT + i])

    @pl.when(c == 1)
    def _():
        for i in range(3):
            arrived(st3.at[z], misc_send.at[Z_SENT + i])
        arrived(st3.at[z], misc_send.at[TOTAL])
        arrived(pre, misc_send.at[PREFIX])

    for i in range(3):
        arrived(sq_s.at[x], misc_send.at[SQUARES + i])
    lin_copy.wait()
    gated_copy.wait()
    total_copy.wait()


def finish(linear, gated, total, gain, lin_out, conv_out):
    lin_out[...] = linear[...]
    column = jnp.concatenate([total[...]] * 16, axis=0).T
    scale = lax.rsqrt(column / 2048 + NORM_EPS)
    for p in range(PAIRS):
        lanes = slice(128 * p, 128 * (p + 1))
        conv_out[:, lanes] = (gated[p] * scale * gain[:, lanes]).astype(BF16)


def shards(
    tokens,
    input_norm_gain,
    query_weight,
    key_weight,
    value_weight,
    decay_first_map,
    decay_second_map,
    channel_decay_offset,
    position_decay_offset,
    extra_log_decay,
    rate_first_map,
    rate_second_map,
    channel_rate_offset,
    own_term_weight,
    head_norm_gain,
    starting_state,
    outer_gate_weight,
    inner_gate_weight,
    signal_weight,
    convolution_taps,
    convolution_gain,
):
    far = pl.BlockSpec(memory_space=pl.ANY)

    def line(v):
        return v.reshape(1, -1)

    pair = pltpu.VMEM((PAIRS, TOK, 128), F32)
    dma = pltpu.SemaphoreType.DMA
    out = jax.ShapeDtypeStruct((TOK, 512), BF16)
    linear, gated, total = pl.pallas_call(
        kernel,
        name="mixer",
        out_shape=(
            out,
            jax.ShapeDtypeStruct((PAIRS, TOK, 128), F32),
            jax.ShapeDtypeStruct((8, TOK), F32),
        ),
        in_specs=[far] * 20,
        out_specs=(far, far, far),
        scratch_shapes=[
            pltpu.VMEM((1, FEATS), F32),
            pltpu.VMEM((128, 512), BF16),
            pltpu.VMEM((1, 512), F32),
            pltpu.VMEM((1, TOK), F32),
            pltpu.VMEM((8, TOK), F32),
            pltpu.VMEM((128, 512), BF16),
            pltpu.VMEM((1, 512), F32),
            pltpu.VMEM((1, 512), F32),
            pltpu.VMEM((1, 512), F32),
            pltpu.VMEM((8, 64, 64), F32),
            pltpu.VMEM((3, 512), BF16),
            dma((11,)),
            pltpu.VMEM((TOK, 512), BF16),
            pltpu.VMEM((8, TOK), F32),
            dma((3,)),
            pltpu.VMEM((2, 32, 128, 768), BF16),
            pltpu.VMEM((2, 32, 128, 768), BF16),
            pltpu.VMEM((4, TOK, 1024), BF16),
            pltpu.VMEM((16, TOK + HALO, 256), BF16),
            pltpu.VMEM((FEATS, 128), BF16),
            pltpu.VMEM((FEATS, 128), BF16),
            pltpu.VMEM((2, TOK + HALO, 768), F32),
        ]
        + [pair] * 8
        + [
            pltpu.VMEM((PAIRS, 2, 2, 64, 128), BF16),
            pltpu.VMEM((8, 2, 64, 128), BF16),
            pltpu.VMEM((4, 2, 64, 128), BF16),
            pltpu.VMEM((3, 2, 64, 128), F32),
            pltpu.VMEM((PAIRS, 64, 128), BF16),
            pltpu.VMEM((4, 64, 128), BF16),
            pltpu.VMEM((4, 8, TOK), F32),
            dma((11,)),
            dma((4,)),
            dma((4,)),
            dma((2,)),
            dma((44,)),
            dma((2,)),
            dma((36,)),
            dma((56,)),
            dma((56,)),
        ],
        compiler_params=pltpu.CompilerParams(
            collective_id=0, has_side_effects=True, vmem_limit_bytes=60 * 1024 * 1024
        ),
    )(
        tokens,
        line(input_norm_gain),
        query_weight,
        key_weight,
        value_weight,
        decay_first_map,
        decay_second_map,
        line(channel_decay_offset),
        line(position_decay_offset),
        extra_log_decay.T,
        rate_first_map,
        rate_second_map,
        line(channel_rate_offset),
        line(own_term_weight),
        line(head_norm_gain),
        starting_state,
        outer_gate_weight,
        inner_gate_weight,
        signal_weight,
        convolution_taps,
    )
    return pl.pallas_call(finish, name="finish", out_shape=(out, out))(
        linear, gated, total, line(convolution_gain)
    )


def solution(mesh):
    torus = Mesh(mesh.devices.reshape(4, 4, 2, mesh.shape["tp"]), (*SP, "tp"))
    return jax.shard_map(
        shards,
        mesh=torus,
        in_specs=(
            P(SP, "tp"),
            P(),
            P(SP, "tp"),
            P(SP, "tp"),
            P(SP, "tp"),
            P(),
            P(None, "tp"),
            P("tp"),
            P(SP),
            P(SP, "tp"),
            P(),
            P(None, "tp"),
            P("tp"),
            P("tp"),
            P("tp"),
            P("tp", None, None),
            P(SP, "tp"),
            P(SP, "tp"),
            P(SP, "tp"),
            P(None, "tp"),
            P("tp"),
        ),
        out_specs=(P(SP, "tp"), P(SP, "tp")),
        check_vma=False,
    )
```

```python
import jax
import jax.numpy as jnp
from jax import lax
from jax.experimental import pallas as pl
from jax.experimental.pallas import tpu as pltpu
from jax.sharding import Mesh
from jax.sharding import PartitionSpec as P

SP = ("sp_0", "sp_1", "sp_2")
MESH_IDS = pl.DeviceIdType.MESH
F32 = jnp.float32
BF16 = jnp.bfloat16

DECAY_FACTOR = 0.606531
NORM_EPS = 1e-06
GROUP_EPS = 0.00064
KEY_EPS = 1e-06

TOK = 256
HALO = 16
FEATS = 4096
BLK = 64
PAIRS = 4
OFFSETS = (0, -1, 1, 2)


def dot_nn(a, b):
    return lax.dot_general(a, b, (((1,), (0,)), ((), ())), preferred_element_type=F32)


def dot_nt(a, b):
    return lax.dot_general(a, b, (((1,), (1,)), ((), ())), preferred_element_type=F32)


def parts(a):
    high = a.astype(BF16)
    return high, (a - high.astype(F32)).astype(BF16)


def dot_tn(a, b):
    return lax.dot_general(a, b, (((0,), (0,)), ((), ())), preferred_element_type=F32)


def fine(dot, a, b):
    ah, al = parts(a)
    bh, bl = parts(b)
    a_dim = 0 if dot is dot_tn else 1
    b_dim = 1 if dot is dot_nt else 0
    return dot(
        jnp.concatenate([ah, al, ah], axis=a_dim), jnp.concatenate([bh, bh, bl], axis=b_dim)
    )


def exact_left(a, b):
    high, rest = parts(b)
    mid = (b - high.astype(F32) - rest.astype(F32)).astype(BF16)
    return dot_nn(a, high) + (dot_nn(a, rest) + dot_nn(a, mid))


def iota(shape, dim):
    return lax.broadcasted_iota(jnp.int32, shape, dim)


def same_head():
    return (iota((128, 128), 0) // 64) == (iota((128, 128), 1) // 64)


def diagonal_blocks(compact):
    return jnp.where(same_head(), jnp.concatenate([compact, compact], axis=0), 0.0)


def head_sums(values):
    ones = same_head().astype(F32).astype(BF16)
    high, rest = parts(values)
    return dot_nn(high, ones) + dot_nn(rest, ones)


def spread_heads(values):
    both = jnp.concatenate([values, values], axis=0)
    return jnp.where(same_head(), both, jnp.zeros_like(both))


def pair_local(q, k, v, decay, rate, cum):
    chunks = range(TOK // BLK)
    rows = [slice(BLK * n, BLK * (n + 1)) for n in chunks]
    later, earlier = iota((BLK, 128), 0), lax.rem(iota((BLK, 128), 1), BLK)
    strict, inclusive = later > earlier, later >= earlier
    unit = k * lax.rsqrt(head_sums(k * k) + KEY_EPS)
    middles = [cum[t.start + BLK // 2 - 1 : t.start + BLK // 2, :] for t in rows]
    middle = jnp.concatenate([jnp.broadcast_to(t, (BLK, 128)) for t in middles], axis=0)
    grow = jnp.exp(middle - cum)
    a = -unit * jnp.exp(cum - decay - middle)
    b = unit * rate
    r = q * jnp.exp(cum - middle)
    a16, r16, v16 = a.astype(BF16), r.astype(BF16), v.astype(BF16)
    b16, k16 = (b * grow).astype(BF16), (k * grow).astype(BF16)
    grams = [
        dot_nt(
            jnp.concatenate([a16[t], r16[t]], axis=0),
            jnp.concatenate([spread_heads(b16[t]), spread_heads(k16[t])], axis=0),
        )
        for t in rows
    ]
    power = [jnp.where(strict, g[:BLK, :128], 0.0).astype(BF16) for g in grams]
    writes = [jnp.where(strict, g[:BLK, 128:], 0.0).astype(BF16) for g in grams]
    reads = [
        jnp.concatenate(
            [
                jnp.where(inclusive, g[BLK:, :128], 0.0).astype(BF16),
                jnp.where(inclusive, g[BLK:, 128:], 0.0).astype(BF16),
            ],
            axis=1,
        )
        for g in grams
    ]
    values = [spread_heads(v16[t]) for t in rows]
    keys_solved = [a[t] for t in rows]
    free_solved = [dot_nn(writes[n], values[n]) for n in chunks]
    for level in range(6):
        for n in chunks:
            right = [spread_heads(keys_solved[n].astype(BF16))]
            right.append(spread_heads(free_solved[n].astype(BF16)))
            if level < 5:
                right.append(spread_heads(power[n]))
            product = dot_nn(power[n], jnp.concatenate(right, axis=1))
            keys_solved[n] = keys_solved[n] + product[:, :128]
            free_solved[n] = free_solved[n] + product[:, 128:256]
            if level < 5:
                power[n] = product[:, 256:].astype(BF16)
    read = []
    for n in chunks:
        top = [spread_heads(keys_solved[n].astype(BF16)), spread_heads(free_solved[n].astype(BF16))]
        low = [jnp.zeros((128, 128), BF16), values[n]]
        right = jnp.concatenate([jnp.concatenate(t, axis=1) for t in (top, low)], axis=0)
        read.append(dot_nn(reads[n], right))
    eye = iota((128, 128), 0) == iota((128, 128), 1)
    steps, gains = [], []
    for n in chunks:
        last = cum[BLK * (n + 1) - 1 : BLK * (n + 1), :]
        fade = jnp.exp(last - cum[rows[n]])
        b_end, k_end = b[rows[n]] * fade, k[rows[n]] * fade
        solved = [keys_solved[n] * jnp.exp(middles[n]), free_solved[n]]
        solved = jnp.concatenate(solved, axis=1)
        both = fine(dot_tn, solved, b_end)
        step = jnp.where(same_head(), both[:128], 0.0)
        steps.append(step + jnp.where(eye, jnp.broadcast_to(jnp.exp(last), (128, 128)), 0.0))
        gain = both[128:] + fine(dot_tn, v[rows[n]], k_end)
        gains.append(jnp.where(same_head(), gain, 0.0))
    state, chain = gains[0], steps[0]
    asked = [(r[rows[n]] + read[n][:, :128]) * jnp.exp(middles[n]) for n in chunks]
    recalled, probes = [read[0][:, 128:]], [asked[0]]
    for n in chunks[1:]:
        carried = jnp.concatenate([state, chain], axis=0)
        both = fine(dot_nt, asked[n], carried)
        recalled.append(read[n][:, 128:] + both[:, :128])
        probes.append(both[:, 128:])
        both = fine(dot_nn, carried, steps[n])
        state, chain = both[:128] + gains[n], both[128:]
    return (
        jnp.concatenate(recalled, axis=0),
        jnp.concatenate(probes, axis=0),
        state[:64] + state[64:],
        chain[:64] + chain[64:],
    )


def compose(earlier, later):
    both = fine(dot_nn, jnp.concatenate(earlier, axis=0), diagonal_blocks(later[0]))
    return both[:64], both[64:] + later[1]


def advance(state, later):
    return fine(dot_nn, state, diagonal_blocks(later[0])) + later[1]


def kernel(
    tokens,
    gain_hbm,
    wq,
    wk,
    wv,
    decay_first,
    decay_second_hbm,
    channel_decay_hbm,
    position_decay_hbm,
    extra_decay_hbm,
    rate_first,
    rate_second_hbm,
    channel_rate_hbm,
    own_weight_hbm,
    norm_gain_hbm,
    start_state_hbm,
    wo,
    wi,
    wsig,
    taps_hbm,
    lin_hbm,
    gated_hbm,
    total_hbm,
    gain,
    decay_second,
    channel_decay,
    position_decay,
    extra_decay,
    rate_second,
    channel_rate,
    own_weight,
    norm_gain,
    start_state,
    taps,
    small_sem,
    lin_out,
    total_out,
    out_sem,
    gat_q,
    gat_c,
    raw,
    xn,
    low_d,
    low_r,
    acc,
    q_s,
    k_s,
    v_s,
    decay_s,
    rate_s,
    cum_s,
    rec_s,
    probe_s,
    st1,
    st2,
    st3,
    pre,
    ent,
    ent_out,
    sq_s,
    load_sem,
    tok_send,
    tok_recv,
    ici_send,
    ici_recv,
    d2d_send,
    d2d_recv,
    misc_send,
    misc_recv,
):
    z, y, c = (lax.axis_index(n) for n in SP)
    x = lax.axis_index("tp")

    def up(pos, offset):
        return lax.rem(pos + (offset + 4), 4)

    def at_x(o):
        return {"tp": up(x, o)}

    def at_y(o):
        return {"sp_1": up(y, o), "sp_2": 1 - c}

    def at_z(o):
        return {"sp_0": up(z, o), "sp_2": 1 - c}

    def along(o):
        return {"sp_0": up(z, (1 - c) * o), "sp_1": up(y, c * o)}

    sibling = {"sp_2": 1 - c}
    rank = z * 8 + y * 2 + c
    after, before = lax.rem(rank + 1, 32), lax.rem(rank + 31, 32)

    def at_rank(r):
        return {"sp_0": r // 8, "sp_1": lax.rem(r // 2, 4), "sp_2": lax.rem(r, 2)}

    def push(src, dst, send, recv, device):
        copy = pltpu.make_async_remote_copy(
            src_ref=src,
            dst_ref=dst,
            send_sem=send,
            recv_sem=recv,
            device_id=device,
            device_id_type=MESH_IDS,
        )
        copy.start()
        return copy

    def arrived(region, recv):
        pltpu.make_async_copy(region, region, recv).wait()

    loads = [pltpu.make_async_copy(tokens, raw.at[x], load_sem.at[0])]
    for n, (buf, weights) in enumerate(((gat_q, (wq, wk, wv)), (gat_c, (wo, wi, wsig)))):
        for i, (w, first, count, half, at) in enumerate(
            (
                (weights[0], 0, 512, 0, 0),
                (weights[1], 0, 256, 0, 512),
                (weights[1], 256, 256, 1, 0),
                (weights[2], 0, 512, 1, 256),
            )
        ):
            src, dst = w.at[:, pl.ds(first, count)], buf.at[half, rank, :, pl.ds(at, count)]
            loads.append(pltpu.make_async_copy(src, dst, load_sem.at[1 + 4 * n + i]))
    loads.append(pltpu.make_async_copy(decay_first, low_d, load_sem.at[9]))
    loads.append(pltpu.make_async_copy(rate_first, low_r, load_sem.at[10]))
    small = [
        (gain_hbm, gain),
        (decay_second_hbm, decay_second),
        (channel_decay_hbm, channel_decay),
        (position_decay_hbm, position_decay),
        (extra_decay_hbm, extra_decay),
        (rate_second_hbm, rate_second),
        (channel_rate_hbm, channel_rate),
        (own_weight_hbm, own_weight),
        (norm_gain_hbm, norm_gain),
        (start_state_hbm, start_state),
        (taps_hbm, taps),
    ]
    small = [
        pltpu.make_async_copy(src, dst, small_sem.at[i]) for i, (src, dst) in enumerate(small)
    ]
    for load in loads + small:
        load.start()

    barrier = pltpu.get_barrier_semaphore()
    partners = [f(o) for f in (at_x, at_y, at_z) for o in OFFSETS[1:]] + [along(1), along(-1)]
    partners += [{"sp_1": up(y, o)} for o in OFFSETS[1:]]
    partners += [sibling, at_rank(after), at_rank(before)]
    for partner in partners:
        pl.semaphore_signal(barrier, inc=1, device_id=partner, device_id_type=MESH_IDS)
    pl.semaphore_wait(barrier, len(partners))

    loads[0].wait()
    tok_copies = [
        push(raw.at[x], raw.at[x], tok_send.at[0], tok_recv.at[0], at_x(1)),
        push(raw.at[x], raw.at[x], tok_send.at[1], tok_recv.at[1], at_x(-1)),
    ]

    def token_forward():
        left, right = up(x, -1), up(x, 1)
        arrived(raw.at[left], tok_recv.at[0])
        part = raw.at[left, pl.ds(0, 128)]
        tok_copies.append(push(part, part, tok_send.at[2], tok_recv.at[2], at_x(1)))
        arrived(raw.at[right], tok_recv.at[1])
        part = raw.at[right, pl.ds(128, 128)]
        tok_copies.append(push(part, part, tok_send.at[3], tok_recv.at[3], at_x(-1)))

    def token_rest():
        far = up(x, 2)
        arrived(raw.at[far, pl.ds(0, 128)], tok_recv.at[2])
        arrived(raw.at[far, pl.ds(128, 128)], tok_recv.at[3])

    class Gather:
        def __init__(self, which, buf):
            self.g, self.buf = which, buf
            self.first, self.second = 1 - c, c

        def chip(self, ahead, across):
            zz = up(z, (1 - c) * ahead + c * across)
            return zz * 4 + up(y, c * ahead + (1 - c) * across)

        def piece(self, half, ahead, across, part=None, cut=64):
            blocks = pl.ds(2 * self.chip(ahead, across), 2)
            if part is None:
                return self.buf.at[half, blocks]
            return self.buf.at[half, blocks, pl.ds(cut * part, (cut, 128 - cut)[part])]

        def cut(self, mi):
            return 48 if self.g == 1 and mi == 1 else 64

        def recv(self, index):
            return ici_recv.at[self.g * 22 + index]

        def shared(self, index):
            return d2d_recv.at[self.g * 18 + index]

        def send(self, region, direction, index):
            push(region, region, ici_send.at[self.g], self.recv(index), along(direction))

        def share(self, region, index):
            push(region, region, d2d_send.at[self.g], self.shared(index), sibling)

        def share_own(self):
            self.share(self.buf.at[self.second, rank], 0)
            self.share(self.buf.at[self.first, rank], 1)

        def start(self):
            own = self.buf.at[self.first, rank]
            self.send(own, 1, 0)
            self.send(own, -1, 2)

        def start_sibling(self):
            other = rank + 1 - 2 * c
            region = self.buf.at[self.first, other]
            arrived(region, self.shared(0))
            self.send(region, 1, 1)
            self.send(region, -1, 3)
            arrived(self.buf.at[self.second, other], self.shared(1))
            self.spread(0)

        def spread(self, mi):
            region = self.piece(self.second, 0, OFFSETS[mi])
            self.send(region, 1, 6 + 4 * mi)
            self.send(region, -1, 7 + 4 * mi)

        def first_near(self, j):
            offset = (-1, 1)[j]
            for core in range(2):
                block = 2 * self.chip(offset, 0) + (c if core == 0 else 1 - c)
                arrived(self.buf.at[self.first, block], self.recv(2 * j + core))
            self.send(self.piece(self.first, offset, 0, j), -offset, 4 + j)
            self.share(self.piece(self.first, offset, 0), 2 + j)

        def first_far(self):
            for j in range(2):
                arrived(self.piece(self.first, 2, 0, j), self.recv(4 + j))
            self.share(self.piece(self.first, 2, 0), 4)

        def second_start(self, mi):
            arrived(self.piece(self.second, 0, OFFSETS[mi]), self.shared(1 + mi))
            self.spread(mi)

        def second_near(self, mi, j):
            offset = (-1, 1)[j]
            arrived(self.piece(self.second, offset, OFFSETS[mi]), self.recv(6 + 4 * mi + j))
            part = self.piece(self.second, offset, OFFSETS[mi], j, self.cut(mi))
            self.send(part, -offset, 8 + 4 * mi + j)
            self.share(self.piece(self.second, offset, OFFSETS[mi]), 5 + 3 * mi + j)

        def second_far(self, mi):
            for j in range(2):
                part = self.piece(self.second, 2, OFFSETS[mi], j, self.cut(mi))
                arrived(part, self.recv(8 + 4 * mi + j))
                if mi == 3:
                    self.share(part, 16 + j)
            if mi < 3:
                self.share(self.piece(self.second, 2, OFFSETS[mi]), 7 + 3 * mi)

        def complete(self, ahead, across):
            if (ahead, across) == (2, 2):
                for j in range(2):
                    arrived(self.piece(self.first, 2, 2, j), self.shared(16 + j))
            elif across != 0:
                index = 5 + 3 * OFFSETS.index(ahead) + OFFSETS.index(across) - 1
                arrived(self.piece(self.first, ahead, across), self.shared(index))

        def steps(self):
            def near(mi):
                return [lambda j=j: self.second_near(mi, j) for j in range(2)]

            return [
                [lambda: self.first_near(0), lambda: self.first_near(1)],
                [lambda: self.second_start(1), lambda: self.second_start(2)],
                near(0),
                [self.first_far],
                [lambda: self.second_start(3)],
                near(1),
                near(2),
                [lambda: self.second_far(0)],
                near(3),
                [lambda: self.second_far(1)],
                [lambda: self.second_far(2)],
                [lambda: self.second_far(3)],
            ]

        def finish(self):
            arrived(self.buf.at[0, pl.ds(0, 30)], ici_send.at[self.g])
            arrived(self.buf.at[0], d2d_send.at[self.g])

    def run(group):
        for step in group:
            step()

    near = [(a, b) for a in (0, -1, 1) for b in (0, -1, 1)]
    axis_far = [(2, 0), (0, 2)]
    side_far = [(-1, 2), (1, 2), (2, -1), (2, 1)]

    def multiply(gather, chips, first_row, fresh=False):
        rows = pl.ds(first_row, TOK + HALO - first_row)
        for n, (ahead, across) in enumerate(chips):
            gather.complete(ahead, across)
            chip = gather.chip(ahead, across)
            left = xn[chip, rows]
            for half in range(2):
                right = gather.buf[half, pl.ds(chip * 2, 2)].reshape(256, 768)
                part = dot_nn(left, right)
                if fresh and n == 0:
                    acc[half, rows] = part
                else:
                    acc[half, rows] += part

    def projection(i, p):
        at = 512 * i + 128 * p
        return at // 768, slice(at % 768, at % 768 + 128)

    gather_q, gather_c = Gather(0, gat_q), Gather(1, gat_c)
    for load in loads[1:5]:
        load.wait()
    gather_q.share_own()
    gather_q.start()
    steps_q = gather_q.steps()
    gather_q.start_sibling()
    for n in range(3):
        run(steps_q[n])
    token_forward()
    for n in range(3, 6):
        run(steps_q[n])
    token_rest()

    for load in small:
        load.wait()
    total = jnp.zeros((TOK, 1), F32)
    for i in range(4):
        wide = raw[i].astype(F32)
        total = total + jnp.sum(wide * wide, axis=1, keepdims=True)
    inverse = lax.rsqrt(total / FEATS + NORM_EPS)
    for i in range(4):
        for j in range(4):
            lanes = slice(256 * j, 256 * (j + 1))
            wide = raw[i, :, lanes].astype(F32) * inverse * gain[:, 1024 * i + 256 * j :][:, :256]
            xn[4 * i + j, pl.ds(HALO, TOK)] = wide.astype(BF16)
    run(steps_q[6])
    run(steps_q[7])
    edge = pl.ds(TOK, HALO)
    halo_copy = push(
        xn.at[:, edge], xn.at[:, pl.ds(0, HALO)], misc_send.at[0], misc_recv.at[0], at_rank(after)
    )

    loads[9].wait()
    loads[10].wait()
    low = jnp.zeros((TOK, 256), F32)
    for i in range(16):
        rows = pl.ds(256 * i, 256)
        both = jnp.concatenate([low_d[rows], low_r[rows]], axis=1)
        low = low + dot_nn(xn[i, pl.ds(HALO, TOK)], both)
    decay_low = jnp.tanh(low[:, :128]).astype(BF16)
    rate_low = low[:, 128:].astype(BF16)
    by_position = jnp.broadcast_to(position_decay[...], (128, TOK)).T
    for p in range(PAIRS):
        lanes = slice(128 * p, 128 * (p + 1))
        logits = channel_decay[:, lanes] + dot_nn(decay_low, decay_second[:, lanes]) + by_position
        heads = [jnp.broadcast_to(extra_decay[h : h + 1], (64, TOK)) for h in (2 * p, 2 * p + 1)]
        extra = jnp.concatenate(heads, axis=0).T
        decay_s[p] = -DECAY_FACTOR * jax.nn.sigmoid(logits) + extra
        rate_s[p] = jax.nn.sigmoid(
            channel_rate[:, lanes] + dot_nn(rate_low, rate_second[:, lanes])
        )
    row, col = iota((TOK, TOK), 0), iota((TOK, TOK), 1)
    summing = (((row // BLK) == (col // BLK)) & (row >= col)).astype(F32).astype(BF16)
    for p in range(PAIRS):
        cum_s[p] = exact_left(summing, decay_s[p])

    for load in loads[5:9]:
        load.wait()
    gather_c.share_own()
    multiply(gather_q, near[:6], HALO, True)
    run(steps_q[8])
    gather_c.start()
    gather_c.start_sibling()
    multiply(gather_q, near[6:], HALO)
    multiply(gather_q, axis_far, HALO)
    run(steps_q[9])
    run(steps_q[10])
    multiply(gather_q, side_far[2:], HALO)
    run(steps_q[11])
    multiply(gather_q, side_far[:2], HALO)
    multiply(gather_q, [(2, 2)], HALO)
    body = pl.ds(HALO, TOK)
    for p in range(PAIRS):
        for i, dst in enumerate((q_s, k_s, v_s)):
            half, lanes = projection(i, p)
            dst[p] = acc[half, body, lanes].astype(BF16).astype(F32)

    steps_c = gather_c.steps()
    CORE, Y_MAPS, Z_MAPS, TOTAL, PREFIX, ENTER, SQUARES = 1, 5, 9, 13, 14, 15, 19
    Y_SENT, Z_SENT, BACK_SENT = 24, 28, 32

    def held(ref, *index):
        return ref[(*index, 0)].astype(F32), ref[(*index, 1)].astype(F32)

    def core_send(p):
        part = st1.at[p, c]
        push(part, part, misc_send.at[CORE + p], misc_recv.at[CORE + p], sibling)

    def y_send(p):
        arrived(st1.at[p, 1 - c], misc_recv.at[CORE + p])

        @pl.when((c == 0) | (p == y))
        def _():
            maps = compose(held(st1, p, 0), held(st1, p, 1))
            slot = (1 - c) * (4 + p) + c * y
            for i in range(2):
                st2[slot, i] = maps[i].astype(BF16)

        @pl.when((c == 0) & (p != y))
        def _():
            push(
                st2.at[4 + p],
                st2.at[y],
                misc_send.at[Y_SENT + p],
                misc_recv.at[Y_MAPS + y],
                {"sp_1": p, "sp_2": 1},
            )

    def z_send():
        for o in OFFSETS[1:]:
            arrived(st2.at[up(y, o)], misc_recv.at[Y_MAPS + up(y, o)])
        total_map = held(st2, 0)
        for k in range(1, 4):
            for i in range(2):
                pre[k - 1, i] = total_map[i]
            total_map = compose(total_map, held(st2, k))
        for i in range(2):
            st3[z, i] = total_map[i].astype(BF16)
        part = st3.at[z]
        for i, o in enumerate(OFFSETS[1:]):
            push(part, part, misc_send.at[Z_SENT + i], misc_recv.at[Z_MAPS + i], at_z(o))
        push(part, part, misc_send.at[TOTAL], misc_recv.at[TOTAL], sibling)
        push(pre, pre, misc_send.at[PREFIX], misc_recv.at[PREFIX], sibling)

    def back_send():
        for i, o in enumerate(OFFSETS[1:]):
            arrived(st3.at[up(z, -o)], misc_recv.at[Z_MAPS + i])
        arrived(st3.at[z], misc_recv.at[TOTAL])
        state = jnp.concatenate([start_state[2 * y], start_state[2 * y + 1]], axis=1)
        for k in range(3):
            state = jnp.where(z > k, advance(state, held(st3, k)), state)
        arrived(pre, misc_recv.at[PREFIX])
        ent_out[0] = state.astype(BF16)
        for k in range(3):
            ent_out[k + 1] = advance(state, (pre[k, 0], pre[k, 1])).astype(BF16)
        ent[y] = ent_out[y]
        for i, o in enumerate(OFFSETS[1:]):
            for core in range(2):
                push(
                    ent_out.at[up(y, o)],
                    ent.at[y],
                    misc_send.at[BACK_SENT + 2 * i + core],
                    misc_recv.at[ENTER + y],
                    {"sp_1": up(y, o), "sp_2": core},
                )
        push(ent_out.at[y], ent.at[y], misc_send.at[BACK_SENT + 6], misc_recv.at[ENTER + y], sibling)

    during = dict(enumerate(steps_c[:4]))

    def one_pair(p, carry):
        for at, group in during.items():
            pl.when(p == at)(lambda group=group: run(group))
        recalled, probe, state, chain = pair_local(
            q_s[p], k_s[p], v_s[p], decay_s[p], rate_s[p], cum_s[p]
        )
        rec_s[p] = recalled
        probe_s[p] = probe
        st1[p, c, 0] = chain.astype(BF16)
        st1[p, c, 1] = state.astype(BF16)
        core_send(p)
        pl.when(p >= 1)(lambda: y_send(p - 1))
        return carry

    lax.fori_loop(0, PAIRS, one_pair, 0)
    y_send(3)

    run(steps_c[4])
    run(steps_c[5])
    pl.when(c == 1)(z_send)
    run(steps_c[6])
    pl.when(c == 0)(back_send)
    run(steps_c[7])
    arrived(xn.at[:, pl.ds(0, HALO)], misc_recv.at[0])
    halo = xn[:, pl.ds(0, HALO)]
    xn[:, pl.ds(0, HALO)] = jnp.where(rank == 0, jnp.zeros_like(halo), halo)

    def finish_pair(p, carry):
        pl.when((c == 1) | (p != y))(lambda: arrived(ent.at[p], misc_recv.at[ENTER + p]))
        state = ent[p].astype(F32)
        state = jnp.where(c == 1, advance(state, held(st1, p, 0)), state)
        recalled = rec_s[p] + fine(dot_nt, probe_s[p], diagonal_blocks(state))
        center = recalled - head_sums(recalled) * (1.0 / 64)
        variance = head_sums(center * center) * (1.0 / 64)
        lanes = pl.ds(pl.multiple_of(128 * p, 128), 128)
        normed = center * lax.rsqrt(variance + GROUP_EPS) * norm_gain[:, lanes]
        own = head_sums(q_s[p] * k_s[p] * own_weight[:, lanes]) * v_s[p]
        lin_out[:, lanes] = (normed + own).astype(BF16)
        return carry

    multiply(gather_c, near, 0, True)
    lax.fori_loop(0, 2, finish_pair, 0)
    run(steps_c[8])
    lax.fori_loop(2, PAIRS, finish_pair, 0)
    lin_copy = pltpu.make_async_copy(lin_out, lin_hbm, out_sem.at[0])
    lin_copy.start()
    multiply(gather_c, axis_far, 0)
    run(steps_c[9])
    run(steps_c[10])
    multiply(gather_c, side_far[2:], 0)
    run(steps_c[11])
    multiply(gather_c, side_far[:2], 0)
    multiply(gather_c, [(2, 2)], 0)
    squares = jnp.zeros((TOK, 128), F32)
    for p in range(PAIRS):
        lanes = slice(128 * p, 128 * (p + 1))
        sums = [acc[projection(i, p)[0], :, projection(i, p)[1]] for i in range(3)]
        outer, inner, signal = (t.astype(BF16).astype(F32) for t in sums)
        mixed = (inner * signal).astype(BF16).astype(F32)
        tap = taps[:, lanes].astype(F32)
        gated = outer[HALO:] * (
            tap[0:1] * pltpu.roll(mixed, 2, 0)[HALO:]
            + tap[1:2] * pltpu.roll(mixed, 1, 0)[HALO:]
            + tap[2:3] * mixed[HALO:]
        )
        q_s[p] = gated
        squares = squares + gated * gated
    column = jnp.broadcast_to(jnp.sum(squares, axis=1, keepdims=True), (TOK, 128))
    gated_copy = pltpu.make_async_copy(q_s, gated_hbm, out_sem.at[2])
    sq_s[x] = column.T[:8]
    for i, o in enumerate(OFFSETS[1:]):
        push(sq_s.at[x], sq_s.at[x], misc_send.at[SQUARES + i], misc_recv.at[SQUARES + i], at_x(o))
    gated_copy.start()
    gather_q.finish()
    gather_c.finish()
    for copy in tok_copies:
        copy.wait_send()
    halo_copy.wait_send()
    for i, o in enumerate(OFFSETS[1:]):
        arrived(sq_s.at[up(x, -o)], misc_recv.at[SQUARES + i])
    total_out[...] = sq_s[0] + sq_s[1] + sq_s[2] + sq_s[3]
    total_copy = pltpu.make_async_copy(total_out, total_hbm, out_sem.at[1])
    total_copy.start()
    for p in range(PAIRS):
        arrived(st1.at[p, c], misc_send.at[CORE + p])

    @pl.when(c == 0)
    def _():
        for p in range(PAIRS):
            pl.when(y != p)(lambda p=p: arrived(st2.at[4 + p], misc_send.at[Y_SENT + p]))
        for i in range(7):
            arrived(ent_out.at[0], misc_send.at[BACK_SENT + i])

    @pl.when(c == 1)
    def _():
        for i in range(3):
            arrived(st3.at[z], misc_send.at[Z_SENT + i])
        arrived(st3.at[z], misc_send.at[TOTAL])
        arrived(pre, misc_send.at[PREFIX])

    for i in range(3):
        arrived(sq_s.at[x], misc_send.at[SQUARES + i])
    lin_copy.wait()
    gated_copy.wait()
    total_copy.wait()


def finish(linear, gated, total, gain, lin_out, conv_out):
    lin_out[...] = linear[...]
    column = jnp.concatenate([total[...]] * 16, axis=0).T
    scale = lax.rsqrt(column / 2048 + NORM_EPS)
    for p in range(PAIRS):
        lanes = slice(128 * p, 128 * (p + 1))
        conv_out[:, lanes] = (gated[p] * scale * gain[:, lanes]).astype(BF16)


def shards(
    tokens,
    input_norm_gain,
    query_weight,
    key_weight,
    value_weight,
    decay_first_map,
    decay_second_map,
    channel_decay_offset,
    position_decay_offset,
    extra_log_decay,
    rate_first_map,
    rate_second_map,
    channel_rate_offset,
    own_term_weight,
    head_norm_gain,
    starting_state,
    outer_gate_weight,
    inner_gate_weight,
    signal_weight,
    convolution_taps,
    convolution_gain,
):
    far = pl.BlockSpec(memory_space=pl.ANY)

    def line(v):
        return v.reshape(1, -1)

    pair = pltpu.VMEM((PAIRS, TOK, 128), F32)
    dma = pltpu.SemaphoreType.DMA
    out = jax.ShapeDtypeStruct((TOK, 512), BF16)
    linear, gated, total = pl.pallas_call(
        kernel,
        name="mixer",
        out_shape=(
            out,
            jax.ShapeDtypeStruct((PAIRS, TOK, 128), F32),
            jax.ShapeDtypeStruct((8, TOK), F32),
        ),
        in_specs=[far] * 20,
        out_specs=(far, far, far),
        scratch_shapes=[
            pltpu.VMEM((1, FEATS), F32),
            pltpu.VMEM((128, 512), BF16),
            pltpu.VMEM((1, 512), F32),
            pltpu.VMEM((1, TOK), F32),
            pltpu.VMEM((8, TOK), F32),
            pltpu.VMEM((128, 512), BF16),
            pltpu.VMEM((1, 512), F32),
            pltpu.VMEM((1, 512), F32),
            pltpu.VMEM((1, 512), F32),
            pltpu.VMEM((8, 64, 64), F32),
            pltpu.VMEM((3, 512), BF16),
            dma((11,)),
            pltpu.VMEM((TOK, 512), BF16),
            pltpu.VMEM((8, TOK), F32),
            dma((3,)),
            pltpu.VMEM((2, 32, 128, 768), BF16),
            pltpu.VMEM((2, 32, 128, 768), BF16),
            pltpu.VMEM((4, TOK, 1024), BF16),
            pltpu.VMEM((16, TOK + HALO, 256), BF16),
            pltpu.VMEM((FEATS, 128), BF16),
            pltpu.VMEM((FEATS, 128), BF16),
            pltpu.VMEM((2, TOK + HALO, 768), F32),
        ]
        + [pair] * 8
        + [
            pltpu.VMEM((PAIRS, 2, 2, 64, 128), BF16),
            pltpu.VMEM((8, 2, 64, 128), BF16),
            pltpu.VMEM((4, 2, 64, 128), BF16),
            pltpu.VMEM((3, 2, 64, 128), F32),
            pltpu.VMEM((PAIRS, 64, 128), BF16),
            pltpu.VMEM((4, 64, 128), BF16),
            pltpu.VMEM((4, 8, TOK), F32),
            dma((11,)),
            dma((4,)),
            dma((4,)),
            dma((2,)),
            dma((44,)),
            dma((2,)),
            dma((36,)),
            dma((56,)),
            dma((56,)),
        ],
        compiler_params=pltpu.CompilerParams(
            collective_id=0, has_side_effects=True, vmem_limit_bytes=60 * 1024 * 1024
        ),
    )(
        tokens,
        line(input_norm_gain),
        query_weight,
        key_weight,
        value_weight,
        decay_first_map,
        decay_second_map,
        line(channel_decay_offset),
        line(position_decay_offset),
        extra_log_decay.T,
        rate_first_map,
        rate_second_map,
        line(channel_rate_offset),
        line(own_term_weight),
        line(head_norm_gain),
        starting_state,
        outer_gate_weight,
        inner_gate_weight,
        signal_weight,
        convolution_taps,
    )
    return pl.pallas_call(finish, name="finish", out_shape=(out, out))(
        linear, gated, total, line(convolution_gain)
    )


def solution(mesh):
    torus = Mesh(mesh.devices.reshape(4, 4, 2, mesh.shape["tp"]), (*SP, "tp"))
    return jax.shard_map(
        shards,
        mesh=torus,
        in_specs=(
            P(SP, "tp"),
            P(),
            P(SP, "tp"),
            P(SP, "tp"),
            P(SP, "tp"),
            P(),
            P(None, "tp"),
            P("tp"),
            P(SP),
            P(SP, "tp"),
            P(),
            P(None, "tp"),
            P("tp"),
            P("tp"),
            P("tp"),
            P("tp", None, None),
            P(SP, "tp"),
            P(SP, "tp"),
            P(SP, "tp"),
            P(None, "tp"),
            P("tp"),
        ),
        out_specs=(P(SP, "tp"), P(SP, "tp")),
        check_vma=False,
    )
```

```python
import jax
import jax.numpy as jnp
from jax import lax
from jax.experimental import pallas as pl
from jax.experimental.pallas import tpu as pltpu
from jax.sharding import Mesh
from jax.sharding import PartitionSpec as P

SP = ("sp_0", "sp_1", "sp_2")
MESH_IDS = pl.DeviceIdType.MESH
F32 = jnp.float32
BF16 = jnp.bfloat16

DECAY_FACTOR = 0.606531
NORM_EPS = 1e-06
GROUP_EPS = 0.00064
KEY_EPS = 1e-06

TOK = 256
HALO = 16
FEATS = 4096
BLK = 64
PAIRS = 4
OFFSETS = (0, -1, 1, 2)


def dot_nn(a, b):
    return lax.dot_general(a, b, (((1,), (0,)), ((), ())), preferred_element_type=F32)


def dot_nt(a, b):
    return lax.dot_general(a, b, (((1,), (1,)), ((), ())), preferred_element_type=F32)


def parts(a):
    high = a.astype(BF16)
    return high, (a - high.astype(F32)).astype(BF16)


def dot_tn(a, b):
    return lax.dot_general(a, b, (((0,), (0,)), ((), ())), preferred_element_type=F32)


def fine(dot, a, b):
    ah, al = parts(a)
    bh, bl = parts(b)
    a_dim = 0 if dot is dot_tn else 1
    b_dim = 1 if dot is dot_nt else 0
    return dot(
        jnp.concatenate([ah, al, ah], axis=a_dim), jnp.concatenate([bh, bh, bl], axis=b_dim)
    )


def exact_left(a, b):
    high, rest = parts(b)
    mid = (b - high.astype(F32) - rest.astype(F32)).astype(BF16)
    return dot_nn(a, high) + (dot_nn(a, rest) + dot_nn(a, mid))


def iota(shape, dim):
    return lax.broadcasted_iota(jnp.int32, shape, dim)


def same_head():
    return (iota((128, 128), 0) // 64) == (iota((128, 128), 1) // 64)


def diagonal_blocks(compact):
    return jnp.where(same_head(), jnp.concatenate([compact, compact], axis=0), 0.0)


def head_sums(values):
    ones = same_head().astype(F32).astype(BF16)
    high, rest = parts(values)
    return dot_nn(high, ones) + dot_nn(rest, ones)


def spread_heads(values):
    both = jnp.concatenate([values, values], axis=0)
    return jnp.where(same_head(), both, jnp.zeros_like(both))


def pair_local(q, k, v, decay, rate, cum):
    chunks = range(TOK // BLK)
    rows = [slice(BLK * n, BLK * (n + 1)) for n in chunks]
    later, earlier = iota((BLK, 128), 0), lax.rem(iota((BLK, 128), 1), BLK)
    strict, inclusive = later > earlier, later >= earlier
    unit = k * lax.rsqrt(head_sums(k * k) + KEY_EPS)
    middles = [cum[t.start + BLK // 2 - 1 : t.start + BLK // 2, :] for t in rows]
    middle = jnp.concatenate([jnp.broadcast_to(t, (BLK, 128)) for t in middles], axis=0)
    grow = jnp.exp(middle - cum)
    a = -unit * jnp.exp(cum - decay - middle)
    b = unit * rate
    r = q * jnp.exp(cum - middle)
    a16, r16, v16 = a.astype(BF16), r.astype(BF16), v.astype(BF16)
    b16, k16 = (b * grow).astype(BF16), (k * grow).astype(BF16)
    grams = [
        dot_nt(
            jnp.concatenate([a16[t], r16[t]], axis=0),
            jnp.concatenate([spread_heads(b16[t]), spread_heads(k16[t])], axis=0),
        )
        for t in rows
    ]
    power = [jnp.where(strict, g[:BLK, :128], 0.0).astype(BF16) for g in grams]
    writes = [jnp.where(strict, g[:BLK, 128:], 0.0).astype(BF16) for g in grams]
    reads = [
        jnp.concatenate(
            [
                jnp.where(inclusive, g[BLK:, :128], 0.0).astype(BF16),
                jnp.where(inclusive, g[BLK:, 128:], 0.0).astype(BF16),
            ],
            axis=1,
        )
        for g in grams
    ]
    values = [spread_heads(v16[t]) for t in rows]
    keys_solved = [a[t] for t in rows]
    free_solved = [dot_nn(writes[n], values[n]) for n in chunks]
    for level in range(6):
        for n in chunks:
            right = [spread_heads(keys_solved[n].astype(BF16))]
            right.append(spread_heads(free_solved[n].astype(BF16)))
            if level < 5:
                right.append(spread_heads(power[n]))
            product = dot_nn(power[n], jnp.concatenate(right, axis=1))
            keys_solved[n] = keys_solved[n] + product[:, :128]
            free_solved[n] = free_solved[n] + product[:, 128:256]
            if level < 5:
                power[n] = product[:, 256:].astype(BF16)
    read = []
    for n in chunks:
        top = [spread_heads(keys_solved[n].astype(BF16)), spread_heads(free_solved[n].astype(BF16))]
        low = [jnp.zeros((128, 128), BF16), values[n]]
        right = jnp.concatenate([jnp.concatenate(t, axis=1) for t in (top, low)], axis=0)
        read.append(dot_nn(reads[n], right))
    eye = iota((128, 128), 0) == iota((128, 128), 1)
    steps, gains = [], []
    for n in chunks:
        last = cum[BLK * (n + 1) - 1 : BLK * (n + 1), :]
        fade = jnp.exp(last - cum[rows[n]])
        b_end, k_end = b[rows[n]] * fade, k[rows[n]] * fade
        solved = [keys_solved[n] * jnp.exp(middles[n]), free_solved[n]]
        solved = jnp.concatenate(solved, axis=1)
        both = fine(dot_tn, solved, b_end)
        step = jnp.where(same_head(), both[:128], 0.0)
        steps.append(step + jnp.where(eye, jnp.broadcast_to(jnp.exp(last), (128, 128)), 0.0))
        gain = both[128:] + fine(dot_tn, v[rows[n]], k_end)
        gains.append(jnp.where(same_head(), gain, 0.0))
    state, chain = gains[0], steps[0]
    asked = [(r[rows[n]] + read[n][:, :128]) * jnp.exp(middles[n]) for n in chunks]
    recalled, probes = [read[0][:, 128:]], [asked[0]]
    for n in chunks[1:]:
        carried = jnp.concatenate([state, chain], axis=0)
        both = fine(dot_nt, asked[n], carried)
        recalled.append(read[n][:, 128:] + both[:, :128])
        probes.append(both[:, 128:])
        both = fine(dot_nn, carried, steps[n])
        state, chain = both[:128] + gains[n], both[128:]
    return (
        jnp.concatenate(recalled, axis=0),
        jnp.concatenate(probes, axis=0),
        state[:64] + state[64:],
        chain[:64] + chain[64:],
    )


def compose(earlier, later):
    both = fine(dot_nn, jnp.concatenate(earlier, axis=0), diagonal_blocks(later[0]))
    return both[:64], both[64:] + later[1]


def advance(state, later):
    return fine(dot_nn, state, diagonal_blocks(later[0])) + later[1]


def kernel(
    tokens,
    gain_hbm,
    wq,
    wk,
    wv,
    decay_first,
    decay_second_hbm,
    channel_decay_hbm,
    position_decay_hbm,
    extra_decay_hbm,
    rate_first,
    rate_second_hbm,
    channel_rate_hbm,
    own_weight_hbm,
    norm_gain_hbm,
    start_state_hbm,
    wo,
    wi,
    wsig,
    taps_hbm,
    lin_hbm,
    gated_hbm,
    total_hbm,
    gain,
    decay_second,
    channel_decay,
    position_decay,
    extra_decay,
    rate_second,
    channel_rate,
    own_weight,
    norm_gain,
    start_state,
    taps,
    small_sem,
    lin_out,
    total_out,
    out_sem,
    gat_q,
    gat_c,
    raw,
    xn,
    low_d,
    low_r,
    acc,
    q_s,
    k_s,
    v_s,
    decay_s,
    rate_s,
    cum_s,
    rec_s,
    probe_s,
    st1,
    st2,
    st3,
    pre,
    ent,
    ent_out,
    sq_s,
    load_sem,
    tok_send,
    tok_recv,
    ici_send,
    ici_recv,
    d2d_send,
    d2d_recv,
    misc_send,
    misc_recv,
):
    z, y, c = (lax.axis_index(n) for n in SP)
    x = lax.axis_index("tp")

    def up(pos, offset):
        return lax.rem(pos + (offset + 4), 4)

    def at_x(o):
        return {"tp": up(x, o)}

    def at_y(o):
        return {"sp_1": up(y, o), "sp_2": 1 - c}

    def at_z(o):
        return {"sp_0": up(z, o), "sp_2": 1 - c}

    def along(o):
        return {"sp_0": up(z, (1 - c) * o), "sp_1": up(y, c * o)}

    sibling = {"sp_2": 1 - c}
    rank = z * 8 + y * 2 + c
    after, before = lax.rem(rank + 1, 32), lax.rem(rank + 31, 32)

    def at_rank(r):
        return {"sp_0": r // 8, "sp_1": lax.rem(r // 2, 4), "sp_2": lax.rem(r, 2)}

    def push(src, dst, send, recv, device):
        copy = pltpu.make_async_remote_copy(
            src_ref=src,
            dst_ref=dst,
            send_sem=send,
            recv_sem=recv,
            device_id=device,
            device_id_type=MESH_IDS,
        )
        copy.start()
        return copy

    def arrived(region, recv):
        pltpu.make_async_copy(region, region, recv).wait()

    loads = [pltpu.make_async_copy(tokens, raw.at[x], load_sem.at[0])]
    for n, (buf, weights) in enumerate(((gat_q, (wq, wk, wv)), (gat_c, (wo, wi, wsig)))):
        for i, (w, first, count, half, at) in enumerate(
            (
                (weights[0], 0, 512, 0, 0),
                (weights[1], 0, 256, 0, 512),
                (weights[1], 256, 256, 1, 0),
                (weights[2], 0, 512, 1, 256),
            )
        ):
            src, dst = w.at[:, pl.ds(first, count)], buf.at[half, rank, :, pl.ds(at, count)]
            loads.append(pltpu.make_async_copy(src, dst, load_sem.at[1 + 4 * n + i]))
    loads.append(pltpu.make_async_copy(decay_first, low_d, load_sem.at[9]))
    loads.append(pltpu.make_async_copy(rate_first, low_r, load_sem.at[10]))
    small = [
        (gain_hbm, gain),
        (decay_second_hbm, decay_second),
        (channel_decay_hbm, channel_decay),
        (position_decay_hbm, position_decay),
        (extra_decay_hbm, extra_decay),
        (rate_second_hbm, rate_second),
        (channel_rate_hbm, channel_rate),
        (own_weight_hbm, own_weight),
        (norm_gain_hbm, norm_gain),
        (start_state_hbm, start_state),
        (taps_hbm, taps),
    ]
    small = [
        pltpu.make_async_copy(src, dst, small_sem.at[i]) for i, (src, dst) in enumerate(small)
    ]
    for load in loads + small:
        load.start()

    barrier = pltpu.get_barrier_semaphore()
    partners = [at_x(1), at_x(-1), along(1), along(-1), sibling]
    for partner in partners:
        pl.semaphore_signal(barrier, inc=1, device_id=partner, device_id_type=MESH_IDS)
    pl.semaphore_wait(barrier, len(partners))

    loads[0].wait()
    tok_copies = [
        push(raw.at[x], raw.at[x], tok_send.at[0], tok_recv.at[0], at_x(1)),
        push(raw.at[x], raw.at[x], tok_send.at[1], tok_recv.at[1], at_x(-1)),
    ]

    def token_forward():
        left, right = up(x, -1), up(x, 1)
        arrived(raw.at[left], tok_recv.at[0])
        part = raw.at[left, pl.ds(0, 128)]
        tok_copies.append(push(part, part, tok_send.at[2], tok_recv.at[2], at_x(1)))
        arrived(raw.at[right], tok_recv.at[1])
        part = raw.at[right, pl.ds(128, 128)]
        tok_copies.append(push(part, part, tok_send.at[3], tok_recv.at[3], at_x(-1)))

    def token_rest():
        far = up(x, 2)
        arrived(raw.at[far, pl.ds(0, 128)], tok_recv.at[2])
        arrived(raw.at[far, pl.ds(128, 128)], tok_recv.at[3])

    class Gather:
        def __init__(self, which, buf):
            self.g, self.buf = which, buf
            self.first, self.second = 1 - c, c

        def chip(self, ahead, across):
            zz = up(z, (1 - c) * ahead + c * across)
            return zz * 4 + up(y, c * ahead + (1 - c) * across)

        def piece(self, half, ahead, across, part=None, cut=64):
            blocks = pl.ds(2 * self.chip(ahead, across), 2)
            if part is None:
                return self.buf.at[half, blocks]
            return self.buf.at[half, blocks, pl.ds(cut * part, (cut, 128 - cut)[part])]

        def cut(self, mi):
            return 48 if self.g == 1 and mi == 1 else 64

        def recv(self, index):
            return ici_recv.at[self.g * 22 + index]

        def shared(self, index):
            return d2d_recv.at[self.g * 18 + index]

        def send(self, region, direction, index):
            push(region, region, ici_send.at[self.g], self.recv(index), along(direction))

        def share(self, region, index):
            push(region, region, d2d_send.at[self.g], self.shared(index), sibling)

        def share_own(self):
            self.share(self.buf.at[self.second, rank], 0)
            self.share(self.buf.at[self.first, rank], 1)

        def start(self):
            own = self.buf.at[self.first, rank]
            self.send(own, 1, 0)
            self.send(own, -1, 2)

        def start_sibling(self):
            other = rank + 1 - 2 * c
            region = self.buf.at[self.first, other]
            arrived(region, self.shared(0))
            self.send(region, 1, 1)
            self.send(region, -1, 3)
            arrived(self.buf.at[self.second, other], self.shared(1))
            self.spread(0)

        def spread(self, mi):
            region = self.piece(self.second, 0, OFFSETS[mi])
            self.send(region, 1, 6 + 4 * mi)
            self.send(region, -1, 7 + 4 * mi)

        def first_near(self, j):
            offset = (-1, 1)[j]
            for core in range(2):
                block = 2 * self.chip(offset, 0) + (c if core == 0 else 1 - c)
                arrived(self.buf.at[self.first, block], self.recv(2 * j + core))
            self.send(self.piece(self.first, offset, 0, j), -offset, 4 + j)
            self.share(self.piece(self.first, offset, 0), 2 + j)

        def first_far(self):
            for j in range(2):
                arrived(self.piece(self.first, 2, 0, j), self.recv(4 + j))
            self.share(self.piece(self.first, 2, 0), 4)

        def second_start(self, mi):
            arrived(self.piece(self.second, 0, OFFSETS[mi]), self.shared(1 + mi))
            self.spread(mi)

        def second_near(self, mi, j):
            offset = (-1, 1)[j]
            arrived(self.piece(self.second, offset, OFFSETS[mi]), self.recv(6 + 4 * mi + j))
            part = self.piece(self.second, offset, OFFSETS[mi], j, self.cut(mi))
            self.send(part, -offset, 8 + 4 * mi + j)
            self.share(self.piece(self.second, offset, OFFSETS[mi]), 5 + 3 * mi + j)

        def second_far(self, mi):
            for j in range(2):
                part = self.piece(self.second, 2, OFFSETS[mi], j, self.cut(mi))
                arrived(part, self.recv(8 + 4 * mi + j))
                if mi == 3:
                    self.share(part, 16 + j)
            if mi < 3:
                self.share(self.piece(self.second, 2, OFFSETS[mi]), 7 + 3 * mi)

        def complete(self, ahead, across):
            if (ahead, across) == (2, 2):
                for j in range(2):
                    arrived(self.piece(self.first, 2, 2, j), self.shared(16 + j))
            elif across != 0:
                index = 5 + 3 * OFFSETS.index(ahead) + OFFSETS.index(across) - 1
                arrived(self.piece(self.first, ahead, across), self.shared(index))

        def steps(self):
            def near(mi):
                return [lambda j=j: self.second_near(mi, j) for j in range(2)]

            return [
                [lambda: self.first_near(0), lambda: self.first_near(1)],
                [lambda: self.second_start(1), lambda: self.second_start(2)],
                near(0),
                [self.first_far],
                [lambda: self.second_start(3)],
                near(1),
                near(2),
                [lambda: self.second_far(0)],
                near(3),
                [lambda: self.second_far(1)],
                [lambda: self.second_far(2)],
                [lambda: self.second_far(3)],
            ]

        def finish(self):
            arrived(self.buf.at[0, pl.ds(0, 30)], ici_send.at[self.g])
            arrived(self.buf.at[0], d2d_send.at[self.g])

    def run(group):
        for step in group:
            step()

    near = [(a, b) for a in (0, -1, 1) for b in (0, -1, 1)]
    axis_far = [(2, 0), (0, 2)]
    side_far = [(-1, 2), (1, 2), (2, -1), (2, 1)]

    def multiply(gather, chips, first_row, fresh=False):
        rows = pl.ds(first_row, TOK + HALO - first_row)
        for n, (ahead, across) in enumerate(chips):
            gather.complete(ahead, across)
            chip = gather.chip(ahead, across)
            left = xn[chip, rows]
            for half in range(2):
                right = gather.buf[half, pl.ds(chip * 2, 2)].reshape(256, 768)
                part = dot_nn(left, right)
                if fresh and n == 0:
                    acc[half, rows] = part
                else:
                    acc[half, rows] += part

    def projection(i, p):
        at = 512 * i + 128 * p
        return at // 768, slice(at % 768, at % 768 + 128)

    gather_q, gather_c = Gather(0, gat_q), Gather(1, gat_c)
    for load in loads[1:5]:
        load.wait()
    gather_q.share_own()
    gather_q.start()
    steps_q = gather_q.steps()
    gather_q.start_sibling()
    for n in range(3):
        run(steps_q[n])
    token_forward()
    for n in range(3, 6):
        run(steps_q[n])
    token_rest()

    for load in small:
        load.wait()
    total = jnp.zeros((TOK, 1), F32)
    for i in range(4):
        wide = raw[i].astype(F32)
        total = total + jnp.sum(wide * wide, axis=1, keepdims=True)
    inverse = lax.rsqrt(total / FEATS + NORM_EPS)
    for i in range(4):
        for j in range(4):
            lanes = slice(256 * j, 256 * (j + 1))
            wide = raw[i, :, lanes].astype(F32) * inverse * gain[:, 1024 * i + 256 * j :][:, :256]
            xn[4 * i + j, pl.ds(HALO, TOK)] = wide.astype(BF16)
    run(steps_q[6])
    run(steps_q[7])
    edge = pl.ds(TOK, HALO)
    halo_copy = push(
        xn.at[:, edge], xn.at[:, pl.ds(0, HALO)], misc_send.at[0], misc_recv.at[0], at_rank(after)
    )

    loads[9].wait()
    loads[10].wait()
    low = jnp.zeros((TOK, 256), F32)
    for i in range(16):
        rows = pl.ds(256 * i, 256)
        both = jnp.concatenate([low_d[rows], low_r[rows]], axis=1)
        low = low + dot_nn(xn[i, pl.ds(HALO, TOK)], both)
    decay_low = jnp.tanh(low[:, :128]).astype(BF16)
    rate_low = low[:, 128:].astype(BF16)
    by_position = jnp.broadcast_to(position_decay[...], (128, TOK)).T
    for p in range(PAIRS):
        lanes = slice(128 * p, 128 * (p + 1))
        logits = channel_decay[:, lanes] + dot_nn(decay_low, decay_second[:, lanes]) + by_position
        heads = [jnp.broadcast_to(extra_decay[h : h + 1], (64, TOK)) for h in (2 * p, 2 * p + 1)]
        extra = jnp.concatenate(heads, axis=0).T
        decay_s[p] = -DECAY_FACTOR * jax.nn.sigmoid(logits) + extra
        rate_s[p] = jax.nn.sigmoid(
            channel_rate[:, lanes] + dot_nn(rate_low, rate_second[:, lanes])
        )
    row, col = iota((TOK, TOK), 0), iota((TOK, TOK), 1)
    summing = (((row // BLK) == (col // BLK)) & (row >= col)).astype(F32).astype(BF16)
    for p in range(PAIRS):
        cum_s[p] = exact_left(summing, decay_s[p])

    for load in loads[5:9]:
        load.wait()
    gather_c.share_own()
    multiply(gather_q, near[:6], HALO, True)
    run(steps_q[8])
    gather_c.start()
    gather_c.start_sibling()
    multiply(gather_q, near[6:], HALO)
    multiply(gather_q, axis_far, HALO)
    run(steps_q[9])
    run(steps_q[10])
    multiply(gather_q, side_far[2:], HALO)
    run(steps_q[11])
    multiply(gather_q, side_far[:2], HALO)
    multiply(gather_q, [(2, 2)], HALO)
    body = pl.ds(HALO, TOK)
    for p in range(PAIRS):
        for i, dst in enumerate((q_s, k_s, v_s)):
            half, lanes = projection(i, p)
            dst[p] = acc[half, body, lanes].astype(BF16).astype(F32)

    steps_c = gather_c.steps()
    CORE, Y_MAPS, Z_MAPS, TOTAL, PREFIX, ENTER, SQUARES = 1, 5, 9, 13, 14, 15, 19
    Y_SENT, Z_SENT, BACK_SENT = 24, 28, 32

    def held(ref, *index):
        return ref[(*index, 0)].astype(F32), ref[(*index, 1)].astype(F32)

    def core_send(p):
        part = st1.at[p, c]
        push(part, part, misc_send.at[CORE + p], misc_recv.at[CORE + p], sibling)

    def y_send(p):
        arrived(st1.at[p, 1 - c], misc_recv.at[CORE + p])

        @pl.when((c == 0) | (p == y))
        def _():
            maps = compose(held(st1, p, 0), held(st1, p, 1))
            slot = (1 - c) * (4 + p) + c * y
            for i in range(2):
                st2[slot, i] = maps[i].astype(BF16)

        @pl.when((c == 0) & (p != y))
        def _():
            push(
                st2.at[4 + p],
                st2.at[y],
                misc_send.at[Y_SENT + p],
                misc_recv.at[Y_MAPS + y],
                {"sp_1": p, "sp_2": 1},
            )

    def z_send():
        for o in OFFSETS[1:]:
            arrived(st2.at[up(y, o)], misc_recv.at[Y_MAPS + up(y, o)])
        total_map = held(st2, 0)
        for k in range(1, 4):
            for i in range(2):
                pre[k - 1, i] = total_map[i]
            total_map = compose(total_map, held(st2, k))
        for i in range(2):
            st3[z, i] = total_map[i].astype(BF16)
        part = st3.at[z]
        for i, o in enumerate(OFFSETS[1:]):
            push(part, part, misc_send.at[Z_SENT + i], misc_recv.at[Z_MAPS + i], at_z(o))
        push(part, part, misc_send.at[TOTAL], misc_recv.at[TOTAL], sibling)
        push(pre, pre, misc_send.at[PREFIX], misc_recv.at[PREFIX], sibling)

    def back_send():
        for i, o in enumerate(OFFSETS[1:]):
            arrived(st3.at[up(z, -o)], misc_recv.at[Z_MAPS + i])
        arrived(st3.at[z], misc_recv.at[TOTAL])
        state = jnp.concatenate([start_state[2 * y], start_state[2 * y + 1]], axis=1)
        for k in range(3):
            state = jnp.where(z > k, advance(state, held(st3, k)), state)
        arrived(pre, misc_recv.at[PREFIX])
        ent_out[0] = state.astype(BF16)
        for k in range(3):
            ent_out[k + 1] = advance(state, (pre[k, 0], pre[k, 1])).astype(BF16)
        ent[y] = ent_out[y]
        for i, o in enumerate(OFFSETS[1:]):
            for core in range(2):
                push(
                    ent_out.at[up(y, o)],
                    ent.at[y],
                    misc_send.at[BACK_SENT + 2 * i + core],
                    misc_recv.at[ENTER + y],
                    {"sp_1": up(y, o), "sp_2": core},
                )
        push(ent_out.at[y], ent.at[y], misc_send.at[BACK_SENT + 6], misc_recv.at[ENTER + y], sibling)

    during = dict(enumerate(steps_c[:4]))

    def one_pair(p, carry):
        for at, group in during.items():
            pl.when(p == at)(lambda group=group: run(group))
        recalled, probe, state, chain = pair_local(
            q_s[p], k_s[p], v_s[p], decay_s[p], rate_s[p], cum_s[p]
        )
        rec_s[p] = recalled
        probe_s[p] = probe
        st1[p, c, 0] = chain.astype(BF16)
        st1[p, c, 1] = state.astype(BF16)
        core_send(p)
        pl.when(p >= 1)(lambda: y_send(p - 1))
        return carry

    lax.fori_loop(0, PAIRS, one_pair, 0)
    y_send(3)

    run(steps_c[4])
    run(steps_c[5])
    pl.when(c == 1)(z_send)
    run(steps_c[6])
    pl.when(c == 0)(back_send)
    run(steps_c[7])
    arrived(xn.at[:, pl.ds(0, HALO)], misc_recv.at[0])
    halo = xn[:, pl.ds(0, HALO)]
    xn[:, pl.ds(0, HALO)] = jnp.where(rank == 0, jnp.zeros_like(halo), halo)

    def finish_pair(p, carry):
        pl.when((c == 1) | (p != y))(lambda: arrived(ent.at[p], misc_recv.at[ENTER + p]))
        state = ent[p].astype(F32)
        state = jnp.where(c == 1, advance(state, held(st1, p, 0)), state)
        recalled = rec_s[p] + fine(dot_nt, probe_s[p], diagonal_blocks(state))
        center = recalled - head_sums(recalled) * (1.0 / 64)
        variance = head_sums(center * center) * (1.0 / 64)
        lanes = pl.ds(pl.multiple_of(128 * p, 128), 128)
        normed = center * lax.rsqrt(variance + GROUP_EPS) * norm_gain[:, lanes]
        own = head_sums(q_s[p] * k_s[p] * own_weight[:, lanes]) * v_s[p]
        lin_out[:, lanes] = (normed + own).astype(BF16)
        return carry

    multiply(gather_c, near, 0, True)
    lax.fori_loop(0, 2, finish_pair, 0)
    run(steps_c[8])
    lax.fori_loop(2, PAIRS, finish_pair, 0)
    lin_copy = pltpu.make_async_copy(lin_out, lin_hbm, out_sem.at[0])
    lin_copy.start()
    multiply(gather_c, axis_far, 0)
    run(steps_c[9])
    run(steps_c[10])
    multiply(gather_c, side_far[2:], 0)
    run(steps_c[11])
    multiply(gather_c, side_far[:2], 0)
    multiply(gather_c, [(2, 2)], 0)
    squares = jnp.zeros((TOK, 128), F32)
    for p in range(PAIRS):
        lanes = slice(128 * p, 128 * (p + 1))
        sums = [acc[projection(i, p)[0], :, projection(i, p)[1]] for i in range(3)]
        outer, inner, signal = (t.astype(BF16).astype(F32) for t in sums)
        mixed = (inner * signal).astype(BF16).astype(F32)
        tap = taps[:, lanes].astype(F32)
        gated = outer[HALO:] * (
            tap[0:1] * pltpu.roll(mixed, 2, 0)[HALO:]
            + tap[1:2] * pltpu.roll(mixed, 1, 0)[HALO:]
            + tap[2:3] * mixed[HALO:]
        )
        q_s[p] = gated
        squares = squares + gated * gated
    column = jnp.broadcast_to(jnp.sum(squares, axis=1, keepdims=True), (TOK, 128))
    gated_copy = pltpu.make_async_copy(q_s, gated_hbm, out_sem.at[2])
    sq_s[x] = column.T[:8]
    for i, o in enumerate(OFFSETS[1:]):
        push(sq_s.at[x], sq_s.at[x], misc_send.at[SQUARES + i], misc_recv.at[SQUARES + i], at_x(o))
    gated_copy.start()
    gather_q.finish()
    gather_c.finish()
    for copy in tok_copies:
        copy.wait_send()
    halo_copy.wait_send()
    for i, o in enumerate(OFFSETS[1:]):
        arrived(sq_s.at[up(x, -o)], misc_recv.at[SQUARES + i])
    total_out[...] = sq_s[0] + sq_s[1] + sq_s[2] + sq_s[3]
    total_copy = pltpu.make_async_copy(total_out, total_hbm, out_sem.at[1])
    total_copy.start()
    for p in range(PAIRS):
        arrived(st1.at[p, c], misc_send.at[CORE + p])

    @pl.when(c == 0)
    def _():
        for p in range(PAIRS):
            pl.when(y != p)(lambda p=p: arrived(st2.at[4 + p], misc_send.at[Y_SENT + p]))
        for i in range(7):
            arrived(ent_out.at[0], misc_send.at[BACK_SENT + i])

    @pl.when(c == 1)
    def _():
        for i in range(3):
            arrived(st3.at[z], misc_send.at[Z_SENT + i])
        arrived(st3.at[z], misc_send.at[TOTAL])
        arrived(pre, misc_send.at[PREFIX])

    for i in range(3):
        arrived(sq_s.at[x], misc_send.at[SQUARES + i])
    lin_copy.wait()
    gated_copy.wait()
    total_copy.wait()


def finish(linear, gated, total, gain, lin_out, conv_out):
    lin_out[...] = linear[...]
    column = jnp.concatenate([total[...]] * 16, axis=0).T
    scale = lax.rsqrt(column / 2048 + NORM_EPS)
    for p in range(PAIRS):
        lanes = slice(128 * p, 128 * (p + 1))
        conv_out[:, lanes] = (gated[p] * scale * gain[:, lanes]).astype(BF16)


def shards(
    tokens,
    input_norm_gain,
    query_weight,
    key_weight,
    value_weight,
    decay_first_map,
    decay_second_map,
    channel_decay_offset,
    position_decay_offset,
    extra_log_decay,
    rate_first_map,
    rate_second_map,
    channel_rate_offset,
    own_term_weight,
    head_norm_gain,
    starting_state,
    outer_gate_weight,
    inner_gate_weight,
    signal_weight,
    convolution_taps,
    convolution_gain,
):
    far = pl.BlockSpec(memory_space=pl.ANY)

    def line(v):
        return v.reshape(1, -1)

    pair = pltpu.VMEM((PAIRS, TOK, 128), F32)
    dma = pltpu.SemaphoreType.DMA
    out = jax.ShapeDtypeStruct((TOK, 512), BF16)
    linear, gated, total = pl.pallas_call(
        kernel,
        name="mixer",
        out_shape=(
            out,
            jax.ShapeDtypeStruct((PAIRS, TOK, 128), F32),
            jax.ShapeDtypeStruct((8, TOK), F32),
        ),
        in_specs=[far] * 20,
        out_specs=(far, far, far),
        scratch_shapes=[
            pltpu.VMEM((1, FEATS), F32),
            pltpu.VMEM((128, 512), BF16),
            pltpu.VMEM((1, 512), F32),
            pltpu.VMEM((1, TOK), F32),
            pltpu.VMEM((8, TOK), F32),
            pltpu.VMEM((128, 512), BF16),
            pltpu.VMEM((1, 512), F32),
            pltpu.VMEM((1, 512), F32),
            pltpu.VMEM((1, 512), F32),
            pltpu.VMEM((8, 64, 64), F32),
            pltpu.VMEM((3, 512), BF16),
            dma((11,)),
            pltpu.VMEM((TOK, 512), BF16),
            pltpu.VMEM((8, TOK), F32),
            dma((3,)),
            pltpu.VMEM((2, 32, 128, 768), BF16),
            pltpu.VMEM((2, 32, 128, 768), BF16),
            pltpu.VMEM((4, TOK, 1024), BF16),
            pltpu.VMEM((16, TOK + HALO, 256), BF16),
            pltpu.VMEM((FEATS, 128), BF16),
            pltpu.VMEM((FEATS, 128), BF16),
            pltpu.VMEM((2, TOK + HALO, 768), F32),
        ]
        + [pair] * 8
        + [
            pltpu.VMEM((PAIRS, 2, 2, 64, 128), BF16),
            pltpu.VMEM((8, 2, 64, 128), BF16),
            pltpu.VMEM((4, 2, 64, 128), BF16),
            pltpu.VMEM((3, 2, 64, 128), F32),
            pltpu.VMEM((PAIRS, 64, 128), BF16),
            pltpu.VMEM((4, 64, 128), BF16),
            pltpu.VMEM((4, 8, TOK), F32),
            dma((11,)),
            dma((4,)),
            dma((4,)),
            dma((2,)),
            dma((44,)),
            dma((2,)),
            dma((36,)),
            dma((56,)),
            dma((56,)),
        ],
        compiler_params=pltpu.CompilerParams(
            collective_id=0, has_side_effects=True, vmem_limit_bytes=60 * 1024 * 1024
        ),
    )(
        tokens,
        line(input_norm_gain),
        query_weight,
        key_weight,
        value_weight,
        decay_first_map,
        decay_second_map,
        line(channel_decay_offset),
        line(position_decay_offset),
        extra_log_decay.T,
        rate_first_map,
        rate_second_map,
        line(channel_rate_offset),
        line(own_term_weight),
        line(head_norm_gain),
        starting_state,
        outer_gate_weight,
        inner_gate_weight,
        signal_weight,
        convolution_taps,
    )
    return pl.pallas_call(finish, name="finish", out_shape=(out, out))(
        linear, gated, total, line(convolution_gain)
    )


def solution(mesh):
    torus = Mesh(mesh.devices.reshape(4, 4, 2, mesh.shape["tp"]), (*SP, "tp"))
    return jax.shard_map(
        shards,
        mesh=torus,
        in_specs=(
            P(SP, "tp"),
            P(),
            P(SP, "tp"),
            P(SP, "tp"),
            P(SP, "tp"),
            P(),
            P(None, "tp"),
            P("tp"),
            P(SP),
            P(SP, "tp"),
            P(),
            P(None, "tp"),
            P("tp"),
            P("tp"),
            P("tp"),
            P("tp", None, None),
            P(SP, "tp"),
            P(SP, "tp"),
            P(SP, "tp"),
            P(None, "tp"),
            P("tp"),
        ),
        out_specs=(P(SP, "tp"), P(SP, "tp")),
        check_vma=False,
    )
```
